128 devices in a mesh: fs: 16 (over z, y), tp: 8 (over x, core).
Axes of the slice: x: 4, y: 4, z: 4, core: 2. Of those that a mesh axis runs over, the one named last changes fastest.
Arguments:
- resid: bfloat16 [16384, 2048], P(('fs', 'tp')), may hold values from -6 to 6
- mix_gain: float32 [2048], replicated, may hold values from 0.1 to 1.9
- w_query: bfloat16 [2048, 1024], P('fs', 'tp'), may hold values from -0.125 to 0.125
- w_key: bfloat16 [2048, 1024], P('fs', 'tp'), may hold values from -0.125 to 0.125
- w_value: bfloat16 [2048, 2048], P('fs', 'tp'), may hold values from -0.125 to 0.125
- w_gate: bfloat16 [2048, 2048], P('fs', 'tp'), may hold values from -0.125 to 0.125
- w_output: bfloat16 [2048, 2048], P('tp', 'fs'), may hold values from -0.125 to 0.125
- decay_rate: float32 [8], P('tp'), may hold values from 0.0008 to 0.034, as said below
- mlp_gain: float32 [2048], replicated, may hold values from 0.1 to 1.9
- w_up: bfloat16 [2048, 8192], P('fs', 'tp'), may hold values from -0.125 to 0.125
- w_down: bfloat16 [8192, 2048], P('tp', 'fs'), may hold values from -0.0625 to 0.0625
Outputs:
- layer_out: bfloat16 [16384, 2048], P(('fs', 'tp'))
The draws below stay inside these ranges and needn't reach their ends.
Inputs may be any that keep to these rules, and one draw needn't show every extreme that they name: `decay_rate`: decay rates per position, one for each head.
All inputs are finite; a program needn't handle non-finite values.
Results may differ from the reference program's by a relative error of at most 0.038.
Values may be sent and summed in bfloat16 or wider, within the bound.
A program may use at most 64 MiB of HBM per device.

```python
import jax
import jax.numpy as jnp
from jax import lax

D = 2048
HEADS = 8
DK = 128
DV = 256
FF = 8192
BLOCK = 128
LENGTH = 512
TOKENS = 16384
N_TP = 8


def draw_decay_rate(key, part):
    order_key, quick_key, slow_key = jax.random.split(key, 3)
    ranking = jax.random.permutation(order_key, HEADS)
    quick_rate = jnp.exp(jax.random.uniform(quick_key, (HEADS,), jnp.float32, jnp.log(1.0 / 50.0), jnp.log(1.0 / 30.0)))
    slow_rate = jax.random.uniform(slow_key, (HEADS,), jnp.float32, 0.2, 1.0) * (2.3 / LENGTH)
    return jnp.where(ranking < HEADS // 2, quick_rate, slow_rate)


def levels(rng, shape, cuts, low, largest):
    def one(position, shards_of):
        draws = jax.random.uniform(jax.random.fold_in(jax.random.fold_in(rng, 6), position), (shards_of,), jnp.float32, low / len(cuts), largest / len(cuts))
        return jnp.repeat(jnp.exp(draws), shape[position] // shards_of).reshape((-1,) + (1,) * (len(shape) - position - 1))

    level = one(*cuts[0])
    for cut in cuts[1:]:
        level = level * one(*cut)
    return level


def scatter_about(own_key, shape, scale, limit, pieces=(), held_as=jnp.bfloat16):
    drawn = jax.random.normal(own_key, shape, jnp.float32) * scale
    if len(pieces) > 0:
        drawn = levels(own_key, shape, pieces, -0.22, 0.18) * drawn
    return jnp.clip(drawn, min=-limit, max=limit).astype(held_as)


def setup_inputs(seed: int = 0) -> dict:
    key_list = jax.random.split(jax.random.key(seed), 12)
    resid = scatter_about(key_list[0], (TOKENS, D), 1.0, 6.0, ((0, 128),))
    mix_gain = jnp.clip(1.0 + 0.18 * jax.random.normal(key_list[1], (D,), jnp.float32), 0.1, 1.9)
    w_query = scatter_about(key_list[2], (D, HEADS * DK), D ** -0.5, 0.125, ((0, 16), (1, 8)))
    w_key = scatter_about(key_list[3], (D, HEADS * DK), D ** -0.5, 0.125, ((0, 16), (1, 8)))
    w_value = scatter_about(key_list[4], (D, HEADS * DV), D ** -0.5, 0.125, ((0, 16), (1, 8)))
    w_gate = scatter_about(key_list[5], (D, HEADS * DV), D ** -0.5, 0.125, ((0, 16), (1, 8)))
    w_output = scatter_about(key_list[6], (HEADS * DV, D), (HEADS * DV) ** -0.5, 0.125, ((0, 8), (1, 16)))
    decay_rate = draw_decay_rate(jax.random.fold_in(key_list[11], 71), 0)
    mlp_gain = jnp.clip(1.0 + 0.18 * jax.random.normal(key_list[8], (D,), jnp.float32), 0.1, 1.9)
    w_up = scatter_about(key_list[9], (D, FF), D ** -0.5, 0.125, ((0, 16), (1, 8)))
    w_down = scatter_about(key_list[10], (FF, D), FF ** -0.5, 0.0625, ((0, 8), (1, 16)))
    return dict(resid=resid, mix_gain=mix_gain, w_query=w_query, w_key=w_key, w_value=w_value, w_gate=w_gate, w_output=w_output, decay_rate=decay_rate, mlp_gain=mlp_gain, w_up=w_up, w_down=w_down)


epsilon = 1e-06

def rms_scale(source, gains):
    widened = source.astype(jnp.float32)
    scaled = widened * lax.rsqrt(lax.optimization_barrier(jnp.mean(widened * widened, axis=-1, keepdims=True)) + epsilon)
    return (scaled * gains).astype(jnp.bfloat16)

def retention(queries, key_rows, values, rates):
    seq_count, length, head_count, key_width = queries.shape
    value_width = values.shape[-1]
    block_count = length // BLOCK
    queries = queries.reshape(seq_count, block_count, BLOCK, head_count, key_width)
    key_rows = key_rows.reshape(seq_count, block_count, BLOCK, head_count, key_width) * key_width ** (-0.5)
    values = values.reshape(seq_count, block_count, BLOCK, head_count, value_width)
    places = jnp.arange(BLOCK, dtype=jnp.float32)
    offset = places[:, None] - places[None, :]
    causal = offset >= 0
    inner_decay = jnp.where(causal[None], jnp.exp(-rates[:, None, None] * jnp.where(causal, offset, 0.0)[None]), 0.0)
    scores = jnp.einsum('bnihd,bnjhd->bnhij', queries, key_rows) * inner_decay[None, None]
    within = jnp.einsum('bnhij,bnjhe->bnihe', scores, values)
    key_decayed = key_rows * jnp.exp(-rates[None, :] * (BLOCK - 1.0 - places)[:, None])[None, None, :, :, None]
    updates = jnp.einsum('bnjhd,bnjhe->nbhde', key_decayed, values)
    carry_decay = jnp.exp(-rates * BLOCK)[None, :, None, None]

    def advance(memory, update):
        return (carry_decay * memory + update, memory)
    _, before = lax.scan(advance, jnp.zeros((seq_count, head_count, key_width, value_width), jnp.float32), updates)
    query_decayed = queries * jnp.exp(-rates[None, :] * (places + 1.0)[:, None])[None, None, :, :, None]
    carried = jnp.einsum('bnihd,nbhde->bnihe', query_decayed, before)
    mixed = (within + carried).reshape(seq_count, length, head_count, value_width)
    centre = lax.optimization_barrier(jnp.mean(mixed, axis=-1, keepdims=True))
    spread = lax.optimization_barrier(jnp.mean(jnp.square(mixed - centre), axis=-1, keepdims=True))
    return (mixed - centre) * lax.rsqrt(spread + epsilon)

def heads_view(source, width):
    return source.astype(jnp.float32).reshape(-1, LENGTH, source.shape[1] // width, width)

def grouped_sum(left, right):
    group = left.shape[1] // N_TP
    result = jnp.zeros((left.shape[0], right.shape[1]), jnp.float32)
    for member in range(N_TP):
        partial_sum = jnp.dot(left[:, member * group:(member + 1) * group], right[member * group:(member + 1) * group], preferred_element_type=jnp.float32)
        result = result + lax.optimization_barrier(partial_sum.astype(jnp.bfloat16)).astype(jnp.float32)
    return result

def reference(resid, mix_gain, w_query, w_key, w_value, w_gate, w_output, decay_rate, mlp_gain, w_up, w_down):
    tokens = resid.shape[0]
    normed = rms_scale(resid, mix_gain)

    def project(weight):
        return jnp.dot(normed, weight, preferred_element_type=jnp.float32).astype(jnp.bfloat16)
    queries = project(w_query)
    key_rows = project(w_key)
    values = project(w_value)
    gate_rows = project(w_gate)
    grouped = retention(heads_view(queries, DK), heads_view(key_rows, DK), heads_view(values, DV), decay_rate)
    gated = (jax.nn.silu(gate_rows.astype(jnp.float32)) * grouped.reshape(tokens, -1)).astype(jnp.bfloat16)
    mix_sum = grouped_sum(gated, w_output)
    after_mix = (resid.astype(jnp.float32) + mix_sum).astype(jnp.bfloat16)
    normed_mlp = rms_scale(after_mix, mlp_gain)
    lifted = jnp.dot(normed_mlp, w_up, preferred_element_type=jnp.float32)
    hidden = jnp.square(jax.nn.relu(lifted)).astype(jnp.bfloat16)
    mlp_sum = grouped_sum(hidden, w_down)
    return (after_mix.astype(jnp.float32) + mlp_sum).astype(jnp.bfloat16)
```

```python
import jax
import jax.numpy as jnp
from jax import lax
from jax.experimental import pallas as pl
from jax.experimental.pallas import tpu as pltpu
from jax.sharding import PartitionSpec as P

D = 2048
DK = 128
DV = 256
LENGTH = 512
RING = 4
EPS = 1e-06
MESH = pl.DeviceIdType.MESH
F32 = jnp.float32
BF16 = jnp.bfloat16

STEP = {"y+": (1, 0), "y-": (-1, 0), "z+": (0, 1), "z-": (0, -1)}


def near(d):
    return {0: 0, 1: 1, 2: 2, 3: -1}[d % RING]


def arrived(message):
    dy, dz, part, way = message
    return near(dy - STEP[way][0]), near(dz - STEP[way][1]), part, way


def onward(message):
    dy, dz, part, way = arrived(message)
    half = "0" if way[1] == "+" else "1"
    across = ("z+", "z-") if way[0] == "y" else ("y+", "y-")
    first = "A" if way[0] == "y" else "B"
    if part == "full":
        return [(dy, dz, "h" + half, way)] + [(dy, dz, first, w) for w in across]
    if part in ("h0", "h1"):
        return [(dy, dz, first + part, w) for w in across]
    if part in ("A", "B"):
        return [(dy, dz, part + "h" + half, way)]
    far = dy if part[0] == "A" else dz
    last = dz if part[0] == "A" else dy
    if far == 2 and last != 2 and part[-1] == half:
        return [(dy, dz, part, way)]
    return []


def plan():
    rounds = [[(0, 0, "full", w) for w in ("y+", "y-", "z+", "z-")]]
    while rounds[-1]:
        rounds.append([m for sent in rounds[-1] for m in onward(sent)])
    return rounds[:-1]


ROUNDS = plan()
MESSAGES = [m for sent in ROUNDS for m in sent]
NUMBER = {m: i for i, m in enumerate(MESSAGES)}

GATHER = (
    [(0, h, w) for h in (0, 1) for w in ("x+", "x-", "d")]
    + [(-1, h, "d") for h in (0, 1)]
    + [(1, h, "d") for h in (0, 1)]
    + [(-1, 0, "x+"), (1, 1, "x-")]
    + [(2, h, "d") for h in (0, 1)]
)
GATHER_NUMBER = {m: i for i, m in enumerate(GATHER)}
TURN = {2: 0, 1: 1, -1: 2, 0: 3}


def kernel(
    resid, mix_gain, wq, wk, wv, wg, wo, rate, mlp_gain, wu, wd,
    out,
    w_in, w_out, w_up, w_down, xn, rbuf, after, proj, gated, hid, decay, kept,
    dout, din, sout, rin2, rin1,
    local_sem, w_send, w_recv, g_send, g_recv, d_send, d_recv, s_send, s_recv,
):
    fs, tp = lax.axis_index("fs"), lax.axis_index("tp")
    z, y, x, c = fs // RING, fs % RING, tp // 2, tp % 2

    def turn(v, d):
        return (v + d + RING) % RING

    device = {
        "y+": (z * RING + turn(y, 1), tp),
        "y-": (z * RING + turn(y, -1), tp),
        "z+": (turn(z, 1) * RING + y, tp),
        "z-": (turn(z, -1) * RING + y, tp),
        "x+": (fs, turn(x, 1) * 2 + c),
        "x-": (fs, turn(x, -1) * 2 + c),
        "d": (fs, x * 2 + 1 - c),
    }
    started = []

    def remote(src, dst, send, recv, way):
        return pltpu.make_async_remote_copy(
            src_ref=src, dst_ref=dst, send_sem=send, recv_sem=recv,
            device_id=device[way], device_id_type=MESH,
        )

    def send(*args):
        copy = remote(*args)
        copy.start()
        started.append(copy)

    weights = (w_in, w_out, w_up, w_down)

    def piece(t, dy, dz, part):
        ref = weights[t]
        f = turn(z, dz) * RING + turn(y, dy)
        if part == "full":
            return ref.at[f]
        if part in ("A", "B"):
            return ref.at[f, :, "AB".index(part)]
        if part in ("h0", "h1"):
            return ref.at[f, int(part[1])]
        return ref.at[f, int(part[2]), "AB".index(part[0])]

    def w_send_one(t, message):
        dy, dz, part, way = message
        n = NUMBER[message]
        ref = piece(t, dy, dz, part)
        send(ref, ref, w_send.at[t, n], w_recv.at[t, n], way)

    def w_first(t):
        for message in ROUNDS[0]:
            w_send_one(t, message)

    def pump(t, r):
        for message in ROUNDS[r - 1]:
            dy, dz, part, way = arrived(message)
            n = NUMBER[message]
            ref = piece(t, dy, dz, part)
            remote(ref, ref, w_send.at[t, n], w_recv.at[t, n], way).wait_recv()
            for following in onward(message):
                w_send_one(t, following)

    def g_piece(g, dx, h, core):
        return xn.at[g, turn(x, dx) * 2 + core, h]

    def g_send_one(g, message):
        dx, h, way = message
        n = GATHER_NUMBER[message]
        ref = g_piece(g, dx, h, c)
        send(ref, ref, g_send.at[g, n], g_recv.at[g, n], way)

    def g_wait(g, message):
        dx, h, way = message
        n = GATHER_NUMBER[message]
        if way == "d":
            ref = g_piece(g, dx, h, 1 - c)
        else:
            ref = g_piece(g, near(dx - (1 if way == "x+" else -1)), h, c)
        remote(ref, ref, g_send.at[g, n], g_recv.at[g, n], way).wait_recv()

    def g_first(g, h):
        for way in ("x+", "x-", "d"):
            g_send_one(g, (0, h, way))

    def g_near(g, h):
        g_wait(g, (0, h, "x+"))
        if h == 0:
            g_send_one(g, (-1, 0, "x+"))
        g_send_one(g, (-1, h, "d"))
        g_wait(g, (0, h, "x-"))
        if h == 1:
            g_send_one(g, (1, 1, "x-"))
        g_send_one(g, (1, h, "d"))

    def g_far(g):
        g_wait(g, (-1, 0, "x+"))
        g_send_one(g, (2, 0, "d"))
        g_wait(g, (1, 1, "x-"))
        g_send_one(g, (2, 1, "d"))

    def g_partner(g, dx):
        for h in (0, 1):
            g_wait(g, (dx, h, "d"))

    def rows16(body):
        def step(i, carry):
            body(pl.ds(pl.multiple_of(i * 16, 16), 16), i * 16)
            return carry

        lax.fori_loop(0, 4, step, 0)

    def d_copy(g, k):
        return (dout.at[g, k], din.at[g, k], d_send.at[g, k], d_recv.at[g, k], "d")

    def s_copy(g, n):
        if n == 0:
            src, dst, way = sout.at[g, 0, 0], rin2.at[g, 0], "x+"
        elif n == 1:
            src, dst, way = sout.at[g, 0, 1], rin2.at[g, 1], "x-"
        elif n < 4:
            src, dst, way = sout.at[g, 1, n - 2], rin1.at[g, 0, n - 2], "x+"
        else:
            src, dst, way = sout.at[g, 2, n - 4], rin1.at[g, 1, n - 4], "x-"
        return (src, dst, s_send.at[g, n], s_recv.at[g, n], way)

    def partial(g, dx, lhs, weight):
        k = TURN[dx]
        depth = weight.shape[1] * weight.shape[2] * weight.shape[3]

        def step(j, carry):
            w = jnp.concatenate([weight[4 * j + i].reshape(depth, 128) for i in range(4)], axis=1)
            o = jnp.dot(lhs(), w, preferred_element_type=F32)
            columns = pl.ds(pl.multiple_of(j * 512, 512), 512)
            dout[g, k, 0, :, columns] = o[:64].astype(BF16)
            dout[g, k, 1, :, columns] = o[64:128].astype(BF16)
            kept[k, :, columns] = o[128:]
            return carry

        lax.fori_loop(0, 4, step, 0)
        send(*d_copy(g, k))

    def add_half(g, k, h, extra=None):
        def body(rows, first):
            at = pl.ds(pl.multiple_of(h * 64 + first, 16), 16)
            total = kept[k, at, :] + din[g, k, h, rows, :].astype(F32)
            if extra is not None:
                total = total + rin2[g, extra, rows, :].astype(F32)
            sout[g, k, h, rows, :] = total.astype(BF16)

        rows16(body)

    def d_wait(g, k):
        remote(*d_copy(g, k)).wait_recv()

    def s_wait(g, n):
        remote(*s_copy(g, n)).wait_recv()

    def combine_far(g):
        d_wait(g, 0)
        add_half(g, 0, 0)
        send(*s_copy(g, 0))
        add_half(g, 0, 1)
        send(*s_copy(g, 1))

    def combine_free(g):
        d_wait(g, 1)
        add_half(g, 1, 1)
        send(*s_copy(g, 3))
        d_wait(g, 2)
        add_half(g, 2, 0)
        send(*s_copy(g, 4))

    def combine_near(g):
        s_wait(g, 0)
        add_half(g, 1, 0, 0)
        send(*s_copy(g, 2))
        s_wait(g, 1)
        add_half(g, 2, 1, 1)
        send(*s_copy(g, 5))

    def sum_rows(g, h, rows, first):
        at = pl.ds(pl.multiple_of(h * 64 + first, 16), 16)
        total = kept[3, at, :] + din[g, 3, h, rows, :].astype(F32)
        return total + rin1[g, 0, h, rows, :].astype(F32) + rin1[g, 1, h, rows, :].astype(F32)

    def normed(values, gain):
        scale = lax.rsqrt(jnp.mean(values * values, axis=-1, keepdims=True) + EPS)
        return (values * scale * gain).astype(BF16)

    loads = []

    def load(src, dst):
        copy = pltpu.make_async_copy(src, dst, local_sem.at[len(loads)])
        copy.start()
        loads.append(copy)

    for src, low, wide in ((wq, 0, 128), (wk, 128, 128), (wv, 256, 256), (wg, 512, 256)):
        load(src, w_in.at[fs, :, :, :, low : low + wide])
    load(resid, rbuf)
    load(wo, w_out.at[fs])
    load(wu, w_up.at[fs])
    load(wd, w_down.at[fs])
    barrier = pltpu.get_barrier_semaphore()
    for way in device:
        pl.semaphore_signal(barrier, inc=1, device_id=device[way], device_id_type=MESH)
    for copy in loads[:5]:
        copy.wait()
    for h in (0, 1):
        def first_norm(rows, first):
            xn[0, tp, h, rows, :] = normed(rbuf[h, rows, :].astype(F32), mix_gain[...])

        rows16(first_norm)
    pl.semaphore_wait(barrier, 7)
    w_first(0)
    g_first(0, 0)
    g_first(0, 1)
    loads[5].wait()
    w_first(1)

    r = rate[0]

    def decay_rows(i, carry):
        rows = pl.ds(pl.multiple_of(i * 64, 64), 64)
        t = lax.broadcasted_iota(jnp.int32, (64, LENGTH), 0) + i * 64
        s = lax.broadcasted_iota(jnp.int32, (64, LENGTH), 1)
        gap = (t - s).astype(F32)
        value = jnp.exp(-r * jnp.maximum(gap, 0.0)) * DK ** (-0.5)
        decay[rows, :] = jnp.where(gap >= 0.0, value, 0.0)
        return carry

    lax.fori_loop(0, LENGTH // 64, decay_rows, 0)

    def project(first_pair, step):
        rhs = lambda j: w_in[:, :, :, :, pl.ds(pl.multiple_of(j * 256, 256), 256)].reshape(D, 256)

        def body(n, carry):
            pair = first_pair + n // 3 * step
            j = n % 3
            lhs = xn[0, pl.ds(2 * pair, 2)].reshape(256, D)
            o = jnp.dot(lhs, rhs(j), preferred_element_type=F32).astype(BF16)
            columns = pl.ds(pl.multiple_of(j * 256, 256), 256)
            proj[pl.ds(2 * pair, 2), :, columns] = o.reshape(2, 128, 256)
            return carry

        lax.fori_loop(0, 6, body, 0)

    def retain(seq):
        for i in (0, 1):
            mine = pl.ds(seq * 4 + 2 * i, 2)
            upto = pl.ds(seq * 4, 2 * i + 2)
            wide = 256 * (i + 1)
            q = proj[mine, :, 0:128].reshape(256, DK)
            k = proj[upto, :, 128:256].reshape(wide, DK)
            v = proj[upto, :, 256:512].reshape(wide, DV)
            scores = lax.dot_general(q, k, (((1,), (1,)), ((), ())), preferred_element_type=F32)
            scores = (scores * decay[i * 256 : (i + 1) * 256, 0:wide]).astype(BF16)
            mixed = jnp.dot(scores, v, preferred_element_type=F32)
            mixed = mixed - jnp.mean(mixed, axis=-1, keepdims=True)
            spread = jnp.mean(mixed * mixed, axis=-1, keepdims=True)
            gate = proj[mine, :, 512:768].reshape(256, DV).astype(F32)
            value = gate / (1.0 + jnp.exp(-gate)) * (mixed * lax.rsqrt(spread + EPS))
            gated[mine] = value.astype(BF16).reshape(2, 128, DV)

    def gated_rows(dx):
        first = turn(x, dx) * 2
        return lambda: jnp.concatenate([gated[first + 1 - c], gated[first + c]], axis=0)

    pump(0, 1)
    pump(1, 1)
    g_near(0, 0)
    pump(0, 2)
    pump(1, 2)
    g_near(0, 1)
    pump(0, 3)
    pump(1, 3)
    loads[6].wait()
    w_first(2)
    g_far(0)
    pump(0, 4)
    for dx in (0, -1, 1, 2):
        g_partner(0, dx)
    other = 1 - x // 2
    project(other * 2, 1)
    retain(other)
    pump(1, 4)
    partial(0, 2, gated_rows(2), w_out)
    pump(2, 1)
    loads[7].wait()
    w_first(3)
    combine_far(0)
    project((1 - other) * 2, 1)
    retain(1 - other)
    partial(0, 1, gated_rows(1), w_out)
    partial(0, -1, gated_rows(-1), w_out)
    combine_free(0)
    pump(2, 2)
    partial(0, 0, gated_rows(0), w_out)
    combine_near(0)
    pump(2, 3)
    pump(3, 1)
    d_wait(0, 3)
    s_wait(0, 3)
    s_wait(0, 4)
    pump(2, 4)
    s_wait(0, 2)
    s_wait(0, 5)
    for h in (0, 1):
        def second_norm(rows, first):
            value = (rbuf[h, rows, :].astype(F32) + sum_rows(0, h, rows, first)).astype(BF16)
            after[h, rows, :] = value
            xn[1, tp, h, rows, :] = normed(value.astype(F32), mlp_gain[...])

        rows16(second_norm)
        g_first(1, h)

    def lift(dx):
        k = TURN[dx]
        first = turn(x, dx) * 2

        def body(j, carry):
            columns = pl.ds(pl.multiple_of(j * 256, 256), 256)
            lhs = jnp.concatenate(
                [xn[1, first + 1 - c].reshape(128, D), xn[1, first + c].reshape(128, D)], axis=0
            )
            rhs = w_up[:, :, :, :, columns].reshape(D, 256)
            o = jnp.maximum(jnp.dot(lhs, rhs, preferred_element_type=F32), 0.0)
            hid[k, :, columns] = (o * o).astype(BF16)
            return carry

        lax.fori_loop(0, w_up.shape[4] // 256, body, 0)

    def hidden_rows(dx):
        return lambda: hid[TURN[dx]]

    pump(3, 2)
    g_partner(1, 0)
    lift(0)
    g_near(1, 0)
    pump(3, 3)
    g_near(1, 1)
    g_partner(1, -1)
    lift(-1)
    g_partner(1, 1)
    lift(1)
    pump(3, 4)
    partial(1, 0, hidden_rows(0), w_down)
    g_far(1)
    g_partner(1, 2)
    lift(2)
    partial(1, 2, hidden_rows(2), w_down)
    combine_far(1)
    partial(1, 1, hidden_rows(1), w_down)
    partial(1, -1, hidden_rows(-1), w_down)
    combine_free(1)
    combine_near(1)
    d_wait(1, 3)
    s_wait(1, 3)
    s_wait(1, 4)
    s_wait(1, 2)
    s_wait(1, 5)
    for h in (0, 1):
        def last(rows, first):
            total = after[h, rows, :].astype(F32) + sum_rows(1, h, rows, first)
            out[h, rows, :] = total.astype(BF16)

        rows16(last)
    for copy in started:
        copy.wait_send()


def on_device(
    resid, mix_gain, w_query, w_key, w_value, w_gate, w_output, decay_rate, mlp_gain, w_up, w_down
):
    def cut(w):
        return w.reshape(2, 2, w.shape[0] // 4, w.shape[1])

    wide = w_query.shape[1] + w_key.shape[1] + w_value.shape[1] + w_gate.shape[1]
    count = RING * RING

    def held(rows, columns):
        return pltpu.VMEM((count, 2, 2, rows // 4, columns), BF16)

    dma = pltpu.SemaphoreType.DMA
    vmem = pl.BlockSpec(memory_space=pltpu.VMEM)
    hbm = pl.BlockSpec(memory_space=pl.ANY)
    tokens = (2, 64, D)
    number = len(MESSAGES)
    result = pl.pallas_call(
        kernel,
        out_shape=jax.ShapeDtypeStruct(tokens, BF16),
        in_specs=[
            hbm, vmem, hbm, hbm, hbm, hbm, hbm,
            pl.BlockSpec(memory_space=pltpu.SMEM), vmem, hbm, hbm,
        ],
        out_specs=vmem,
        scratch_shapes=[
            held(128, wide),
            held(w_output.shape[0], 128),
            held(128, w_up.shape[1]),
            held(w_down.shape[0], 128),
            pltpu.VMEM((2, 8) + tokens, BF16),
            pltpu.VMEM(tokens, BF16),
            pltpu.VMEM(tokens, BF16),
            pltpu.VMEM((8, 128, wide), BF16),
            pltpu.VMEM((8, 128, DV), BF16),
            pltpu.VMEM((4, 256, w_up.shape[1]), BF16),
            pltpu.VMEM((LENGTH, LENGTH), F32),
            pltpu.VMEM((4, 128, D), F32),
            pltpu.VMEM((2, 4) + tokens, BF16),
            pltpu.VMEM((2, 4) + tokens, BF16),
            pltpu.VMEM((2, 3) + tokens, BF16),
            pltpu.VMEM((2, 2, 64, D), BF16),
            pltpu.VMEM((2, 2) + tokens, BF16),
            dma((8,)),
            dma((4, number)),
            dma((4, number)),
            dma((2, len(GATHER))),
            dma((2, len(GATHER))),
            dma((2, 4)),
            dma((2, 4)),
            dma((2, 6)),
            dma((2, 6)),
        ],
        compiler_params=pltpu.CompilerParams(
            collective_id=0, has_side_effects=True, vmem_limit_bytes=63 * 1024 * 1024
        ),
    )(
        resid.reshape(tokens), mix_gain[None], cut(w_query), cut(w_key), cut(w_value), cut(w_gate),
        cut(w_output), decay_rate, mlp_gain[None], cut(w_up), cut(w_down),
    )
    return result.reshape(resid.shape)


def solution(mesh):
    placed = (
        P(("fs", "tp"), None),
        P(),
        P("fs", "tp"),
        P("fs", "tp"),
        P("fs", "tp"),
        P("fs", "tp"),
        P("tp", "fs"),
        P("tp"),
        P(),
        P("fs", "tp"),
        P("tp", "fs"),
    )
    return jax.shard_map(
        on_device, mesh=mesh, in_specs=placed, out_specs=P(("fs", "tp"), None), check_vma=False
    )
```

```python
import jax
import jax.numpy as jnp
from jax import lax
from jax.experimental import pallas as pl
from jax.experimental.pallas import tpu as pltpu
from jax.sharding import PartitionSpec as P

D = 2048
DK = 128
DV = 256
LENGTH = 512
RING = 4
EPS = 1e-06
MESH = pl.DeviceIdType.MESH
F32 = jnp.float32
BF16 = jnp.bfloat16

STEP = {"y+": (1, 0), "y-": (-1, 0), "z+": (0, 1), "z-": (0, -1)}


def near(d):
    return {0: 0, 1: 1, 2: 2, 3: -1}[d % RING]


def arrived(message):
    dy, dz, part, way = message
    return near(dy - STEP[way][0]), near(dz - STEP[way][1]), part, way


def onward(message):
    dy, dz, part, way = arrived(message)
    half = "0" if way[1] == "+" else "1"
    across = ("z+", "z-") if way[0] == "y" else ("y+", "y-")
    first = "A" if way[0] == "y" else "B"
    if part == "full":
        return [(dy, dz, "h" + half, way)] + [(dy, dz, first, w) for w in across]
    if part in ("h0", "h1"):
        return [(dy, dz, first + part, w) for w in across]
    if part in ("A", "B"):
        return [(dy, dz, part + "h" + half, way)]
    far = dy if part[0] == "A" else dz
    last = dz if part[0] == "A" else dy
    if far == 2 and last != 2 and part[-1] == half:
        return [(dy, dz, part, way)]
    return []


def plan():
    rounds = [[(0, 0, "full", w) for w in ("y+", "y-", "z+", "z-")]]
    while rounds[-1]:
        rounds.append([m for sent in rounds[-1] for m in onward(sent)])
    return rounds[:-1]


ROUNDS = plan()
MESSAGES = [m for sent in ROUNDS for m in sent]
NUMBER = {m: i for i, m in enumerate(MESSAGES)}

GATHER = (
    [(0, h, q, w) for h in (0, 1) for q in (0, 1) for w in ("x+", "x-")]
    + [(0, h, None, "d") for h in (0, 1)]
    + [(dx, h, q, "d") for dx in (-1, 1, 2) for h in (0, 1) for q in (0, 1)]
    + [(-1, h, 0, "x+") for h in (0, 1)]
    + [(1, h, 1, "x-") for h in (0, 1)]
)
GATHER_NUMBER = {m: i for i, m in enumerate(GATHER)}
TURN = {2: 0, 1: 1, -1: 2, 0: 3}


def kernel(
    resid, mix_gain, wq, wk, wv, wg, wo, rate, mlp_gain, wu, wd,
    out,
    w_in, w_out, w_up, w_down, xn, rbuf, after, proj, gated, hid, decay, kept,
    dout, din, sout, rin2, rin1,
    local_sem, w_send, w_recv, g_send, g_recv, d_send, d_recv, s_send, s_recv,
):
    fs, tp = lax.axis_index("fs"), lax.axis_index("tp")
    z, y, x, c = fs // RING, fs % RING, tp // 2, tp % 2

    def turn(v, d):
        return (v + d + RING) % RING

    device = {
        "y+": (z * RING + turn(y, 1), tp),
        "y-": (z * RING + turn(y, -1), tp),
        "z+": (turn(z, 1) * RING + y, tp),
        "z-": (turn(z, -1) * RING + y, tp),
        "x+": (fs, turn(x, 1) * 2 + c),
        "x-": (fs, turn(x, -1) * 2 + c),
        "d": (fs, x * 2 + 1 - c),
    }

    def remote(src, dst, send, recv, way):
        return pltpu.make_async_remote_copy(
            src_ref=src, dst_ref=dst, send_sem=send, recv_sem=recv,
            device_id=device[way], device_id_type=MESH,
        )

    def send(*args):
        remote(*args).start()

    weights = (w_in, w_out, w_up, w_down)

    def piece(t, dy, dz, part):
        ref = weights[t]
        f = turn(z, dz) * RING + turn(y, dy)
        if part == "full":
            return ref.at[f]
        if part in ("A", "B"):
            return ref.at[f, :, "AB".index(part)]
        if part in ("h0", "h1"):
            return ref.at[f, int(part[1])]
        return ref.at[f, int(part[2]), "AB".index(part[0])]

    def w_copy(t, message, place):
        dy, dz, part, way = place
        ref = piece(t, dy, dz, part)
        return (ref, ref, w_send.at[t], w_recv.at[t, NUMBER[message]], way)

    def w_first(t):
        for message in ROUNDS[0]:
            send(*w_copy(t, message, message))

    def pump(t, r):
        for message in ROUNDS[r - 1]:
            remote(*w_copy(t, message, arrived(message))).wait_recv()
            for following in onward(message):
                send(*w_copy(t, following, following))

    def g_copy(g, message, dx, core):
        h, q, way = message[1:]
        block = turn(x, dx) * 2 + core
        ref = xn.at[g, block, h] if q is None else xn.at[g, block, h, q]
        return (ref, ref, g_send.at[g], g_recv.at[g, GATHER_NUMBER[message]], way)

    def g_send_one(g, message):
        send(*g_copy(g, message, message[0], c))

    def g_wait(g, message):
        dx, h, q, way = message
        if way == "d":
            copy = g_copy(g, message, dx, 1 - c)
        else:
            copy = g_copy(g, message, near(dx - (1 if way == "x+" else -1)), c)
        remote(*copy).wait_recv()

    def g_first(g, h):
        g_send_one(g, (0, h, 0, "x+"))
        g_send_one(g, (0, h, 1, "x-"))
        g_send_one(g, (0, h, None, "d"))

    def g_second(g, h):
        g_send_one(g, (0, h, 1, "x+"))
        g_send_one(g, (0, h, 0, "x-"))

    def g_near(g, h):
        g_wait(g, (0, h, 0, "x+"))
        g_send_one(g, (-1, h, 0, "x+"))
        g_send_one(g, (-1, h, 0, "d"))
        g_wait(g, (0, h, 1, "x-"))
        g_send_one(g, (1, h, 1, "x-"))
        g_send_one(g, (1, h, 1, "d"))

    def g_rest(g, h):
        g_wait(g, (0, h, 1, "x+"))
        g_send_one(g, (-1, h, 1, "d"))
        g_wait(g, (0, h, 0, "x-"))
        g_send_one(g, (1, h, 0, "d"))

    def g_far(g, h):
        g_wait(g, (-1, h, 0, "x+"))
        g_send_one(g, (2, h, 0, "d"))
        g_wait(g, (1, h, 1, "x-"))
        g_send_one(g, (2, h, 1, "d"))

    def g_partner(g, h, dx):
        for q in (None,) if dx == 0 else (0, 1):
            g_wait(g, (dx, h, q, "d"))

    def rows16(count, body):
        def step(i, carry):
            body(pl.ds(pl.multiple_of(i * 16, 16), 16))
            return carry

        lax.fori_loop(0, count // 16, step, 0)

    def d_copy(g, k, h):
        return (dout.at[g, k, h], din.at[g, k, h], d_send.at[g], d_recv.at[g, k, h], "d")

    def s_copy(g, h, n):
        if n < 2:
            src, dst, way = sout.at[g, 0, h, n], rin2.at[g, h, n], ("x+", "x-")[n]
        elif n < 4:
            src, dst, way = sout.at[g, 1, h, n - 2], rin1.at[g, 0, h, n - 2], "x+"
        else:
            src, dst, way = sout.at[g, 2, h, n - 4], rin1.at[g, 1, h, n - 4], "x-"
        return (src, dst, s_send.at[g], s_recv.at[g, h, n], way)

    def partial(g, cases, lhs, weight):
        depth = weight.shape[1] * weight.shape[2] * weight.shape[3]

        def step(j, carry):
            w = jnp.concatenate([weight[4 * j + i].reshape(depth, 128) for i in range(4)], axis=1)
            rows = jnp.concatenate([block for case in cases for block in lhs(*case)], axis=0)
            o = jnp.dot(rows, w, preferred_element_type=F32)
            columns = pl.ds(pl.multiple_of(j * 512, 512), 512)
            for n, (dx, h) in enumerate(cases):
                mine = o[n * 128 : (n + 1) * 128]
                dout[g, TURN[dx], h, :, :, columns] = mine[:64].astype(BF16).reshape(2, 32, 512)
                kept[TURN[dx], h, :, :, columns] = mine[64:].reshape(2, 32, 512)
            return carry

        lax.fori_loop(0, 4, step, 0)
        for dx, h in cases:
            send(*d_copy(g, TURN[dx], h))

    def add_quarter(g, k, h, q, extra=False):
        def body(rows):
            total = kept[k, h, q, rows, :] + din[g, k, h, q, rows, :].astype(F32)
            if extra:
                total = total + rin2[g, h, q, rows, :].astype(F32)
            sout[g, k, h, q, rows, :] = total.astype(BF16)

        rows16(32, body)

    def d_wait(g, k, h):
        remote(*d_copy(g, k, h)).wait_recv()

    def s_wait(g, h, n):
        remote(*s_copy(g, h, n)).wait_recv()

    def combine_far(g, h):
        d_wait(g, 0, h)
        for q in (0, 1):
            add_quarter(g, 0, h, q)
            send(*s_copy(g, h, q))

    def combine_free(g, h):
        d_wait(g, 1, h)
        add_quarter(g, 1, h, 1)
        send(*s_copy(g, h, 3))
        d_wait(g, 2, h)
        add_quarter(g, 2, h, 0)
        send(*s_copy(g, h, 4))

    def combine_near(g, h):
        s_wait(g, h, 0)
        add_quarter(g, 1, h, 0, True)
        send(*s_copy(g, h, 2))
        s_wait(g, h, 1)
        add_quarter(g, 2, h, 1, True)
        send(*s_copy(g, h, 5))

    def combine_own(g, h):
        d_wait(g, 3, h)
        for n in (3, 4, 2, 5):
            s_wait(g, h, n)

    def sum_rows(g, h, q, rows):
        total = kept[3, h, q, rows, :] + din[g, 3, h, q, rows, :].astype(F32)
        return total + rin1[g, 0, h, q, rows, :].astype(F32) + rin1[g, 1, h, q, rows, :].astype(F32)

    def normed(values, gain):
        scale = lax.rsqrt(jnp.mean(values * values, axis=-1, keepdims=True) + EPS)
        return (values * scale * gain).astype(BF16)

    loads = []

    def load(src, dst):
        copy = pltpu.make_async_copy(src, dst, local_sem.at[len(loads)])
        copy.start()
        loads.append(copy)

    for src, low, wide in ((wq, 0, 128), (wk, 128, 128), (wv, 256, 256), (wg, 512, 256)):
        load(src, w_in.at[fs, :, :, :, low : low + wide])
    load(resid, rbuf)
    load(wo, w_out.at[fs])
    load(wu, w_up.at[fs])
    load(wd, w_down.at[fs])
    barrier = pltpu.get_barrier_semaphore()
    for way in device:
        pl.semaphore_signal(barrier, inc=1, device_id=device[way], device_id_type=MESH)
    for copy in loads[:5]:
        copy.wait()
    for h in (0, 1):
        for q in (0, 1):
            def first_norm(rows):
                xn[0, tp, h, q, rows, :] = normed(rbuf[h, q, rows, :].astype(F32), mix_gain[...])

            rows16(32, first_norm)
    pl.semaphore_wait(barrier, 7)
    w_first(0)
    g_first(0, 0)
    g_second(0, 0)
    g_first(0, 1)
    g_second(0, 1)
    loads[5].wait()
    w_first(1)

    r = rate[0]

    def decay_rows(i, carry):
        rows = pl.ds(pl.multiple_of(i * 64, 64), 64)
        t = lax.broadcasted_iota(jnp.int32, (64, LENGTH), 0) + i * 64
        s = lax.broadcasted_iota(jnp.int32, (64, LENGTH), 1)
        gap = (t - s).astype(F32)
        value = jnp.exp(-r * jnp.maximum(gap, 0.0)) * DK ** (-0.5)
        decay[rows, :] = jnp.where(gap >= 0.0, value, 0.0)
        return carry

    lax.fori_loop(0, LENGTH // 64, decay_rows, 0)

    def project(seq):
        def body(j, carry):
            columns = pl.ds(pl.multiple_of(j * 256, 256), 256)
            lhs = xn[0, pl.ds(4 * seq, 4)].reshape(512, D)
            rhs = w_in[:, :, :, :, columns].reshape(D, 256)
            o = jnp.dot(lhs, rhs, preferred_element_type=F32).astype(BF16)
            proj[pl.ds(4 * seq, 4), :, columns] = o.reshape(4, 128, 256)
            return carry

        lax.fori_loop(0, 3, body, 0)

    def retain(seq):
        for i in (0, 1):
            mine = pl.ds(seq * 4 + 2 * i, 2)
            upto = pl.ds(seq * 4, 2 * i + 2)
            wide = 256 * (i + 1)
            q = proj[mine, :, 0:128].reshape(256, DK)
            k = proj[upto, :, 128:256].reshape(wide, DK)
            v = proj[upto, :, 256:512].reshape(wide, DV)
            scores = lax.dot_general(q, k, (((1,), (1,)), ((), ())), preferred_element_type=F32)
            scores = (scores * decay[i * 256 : (i + 1) * 256, 0:wide]).astype(BF16)
            mixed = jnp.dot(scores, v, preferred_element_type=F32)
            mixed = mixed - jnp.mean(mixed, axis=-1, keepdims=True)
            spread = jnp.mean(mixed * mixed, axis=-1, keepdims=True)
            gate = proj[mine, :, 512:768].reshape(256, DV).astype(F32)
            value = gate / (1.0 + jnp.exp(-gate)) * (mixed * lax.rsqrt(spread + EPS))
            gated[mine] = value.astype(BF16).reshape(2, 2, 64, DV)

    def gated_rows(dx, h):
        first = turn(x, dx) * 2
        return gated[first + 1 - c, h], gated[first + c, h]

    def lift(cases):
        def body(j, carry):
            columns = pl.ds(pl.multiple_of(j * 256, 256), 256)
            lhs = jnp.concatenate(
                [
                    xn[1, turn(x, dx) * 2 + core, h].reshape(64, D)
                    for dx, h in cases
                    for core in (1 - c, c)
                ],
                axis=0,
            )
            rhs = w_up[:, :, :, :, columns].reshape(D, 256)
            o = jnp.maximum(jnp.dot(lhs, rhs, preferred_element_type=F32), 0.0)
            o = (o * o).astype(BF16)
            for n, (dx, h) in enumerate(cases):
                hid[TURN[dx], h, :, columns] = o[n * 128 : (n + 1) * 128]
            return carry

        lax.fori_loop(0, w_up.shape[4] // 256, body, 0)

    def hidden_rows(dx, h):
        return (hid[TURN[dx], h],)

    pump(0, 1)
    g_near(0, 0)
    g_rest(0, 0)
    pump(0, 2)
    g_near(0, 1)
    g_rest(0, 1)
    pump(0, 3)
    pump(1, 1)
    loads[6].wait()
    w_first(2)
    g_far(0, 0)
    pump(0, 4)
    g_far(0, 1)
    for h in (0, 1):
        for dx in (0, -1, 1, 2):
            g_partner(0, h, dx)
    other = 1 - x // 2
    project(other)
    pump(1, 2)
    retain(other)
    pump(1, 3)
    pump(2, 1)
    loads[7].wait()
    w_first(3)
    pump(1, 4)
    partial(0, ((2, 0), (2, 1)), gated_rows, w_out)
    combine_far(0, 0)
    combine_far(0, 1)
    project(1 - other)
    retain(1 - other)
    partial(0, ((1, 0), (-1, 0)), gated_rows, w_out)
    partial(0, ((1, 1), (-1, 1)), gated_rows, w_out)
    combine_free(0, 0)
    combine_near(0, 0)
    combine_free(0, 1)
    combine_near(0, 1)
    pump(2, 2)
    partial(0, ((0, 0), (0, 1)), gated_rows, w_out)
    pump(3, 1)

    def second_norm(h):
        for q in (0, 1):
            def body(rows):
                value = rbuf[h, q, rows, :].astype(F32) + sum_rows(0, h, q, rows)
                value = value.astype(BF16)
                after[h, q, rows, :] = value
                xn[1, tp, h, q, rows, :] = normed(value.astype(F32), mlp_gain[...])

            rows16(32, body)

    combine_own(0, 0)
    second_norm(0)
    g_first(1, 0)
    g_second(1, 0)
    pump(2, 3)
    combine_own(0, 1)
    second_norm(1)
    g_first(1, 1)
    g_near(1, 0)
    g_second(1, 1)
    g_rest(1, 0)
    pump(2, 4)
    pump(3, 2)

    g_partner(1, 0, 0)
    g_partner(1, 0, -1)
    g_partner(1, 0, 1)
    lift(((0, 0), (-1, 0), (1, 0)))
    g_near(1, 1)
    g_far(1, 0)
    g_partner(1, 0, 2)
    lift(((2, 0),))
    pump(3, 3)
    g_rest(1, 1)
    g_far(1, 1)
    pump(3, 4)
    partial(1, ((2, 0),), hidden_rows, w_down)
    combine_far(1, 0)
    partial(1, ((1, 0), (-1, 0)), hidden_rows, w_down)
    combine_free(1, 0)
    g_partner(1, 1, 2)
    lift(((2, 1),))
    partial(1, ((2, 1),), hidden_rows, w_down)
    combine_near(1, 0)
    combine_far(1, 1)
    g_partner(1, 1, 0)
    g_partner(1, 1, -1)
    g_partner(1, 1, 1)
    lift(((0, 1), (-1, 1), (1, 1)))
    partial(1, ((1, 1), (-1, 1)), hidden_rows, w_down)
    combine_free(1, 1)
    combine_near(1, 1)
    partial(1, ((0, 0), (0, 1)), hidden_rows, w_down)

    def finish(h):
        for q in (0, 1):
            def body(rows):
                total = after[h, q, rows, :].astype(F32) + sum_rows(1, h, q, rows)
                out[h, q, rows, :] = total.astype(BF16)

            rows16(32, body)

    combine_own(1, 0)
    finish(0)
    combine_own(1, 1)
    finish(1)
    for t in range(4):
        ref = weights[t].at[0:15]
        remote(ref, ref, w_send.at[t], w_recv.at[t, 0], "d").wait_send()
    for g in (0, 1):
        remote(xn.at[g, 0:7], xn.at[g, 0:7], g_send.at[g], g_recv.at[g, 0], "d").wait_send()
        remote(dout.at[g], din.at[g], d_send.at[g], d_recv.at[g, 0, 0], "d").wait_send()
        remote(sout.at[g], sout.at[g], s_send.at[g], s_recv.at[g, 0, 0], "d").wait_send()


def on_device(
    resid, mix_gain, w_query, w_key, w_value, w_gate, w_output, decay_rate, mlp_gain, w_up, w_down
):
    def cut(w):
        return w.reshape(2, 2, w.shape[0] // 4, w.shape[1])

    wide = w_query.shape[1] + w_key.shape[1] + w_value.shape[1] + w_gate.shape[1]
    count = RING * RING

    def held(rows, columns):
        return pltpu.VMEM((count, 2, 2, rows // 4, columns), BF16)

    dma = pltpu.SemaphoreType.DMA
    vmem = pl.BlockSpec(memory_space=pltpu.VMEM)
    hbm = pl.BlockSpec(memory_space=pl.ANY)
    tokens = (2, 2, 32, D)
    number = len(MESSAGES)
    result = pl.pallas_call(
        kernel,
        out_shape=jax.ShapeDtypeStruct(tokens, BF16),
        in_specs=[
            hbm, vmem, hbm, hbm, hbm, hbm, hbm,
            pl.BlockSpec(memory_space=pltpu.SMEM), vmem, hbm, hbm,
        ],
        out_specs=vmem,
        scratch_shapes=[
            held(128, wide),
            held(w_output.shape[0], 128),
            held(128, w_up.shape[1]),
            held(w_down.shape[0], 128),
            pltpu.VMEM((2, 8) + tokens, BF16),
            pltpu.VMEM(tokens, BF16),
            pltpu.VMEM(tokens, BF16),
            pltpu.VMEM((8, 128, wide), BF16),
            pltpu.VMEM((8, 2, 64, DV), BF16),
            pltpu.VMEM((4, 2, 128, w_up.shape[1]), BF16),
            pltpu.VMEM((LENGTH, LENGTH), F32),
            pltpu.VMEM((4,) + tokens, F32),
            pltpu.VMEM((2, 4) + tokens, BF16),
            pltpu.VMEM((2, 4) + tokens, BF16),
            pltpu.VMEM((2, 3) + tokens, BF16),
            pltpu.VMEM((2,) + tokens, BF16),
            pltpu.VMEM((2, 2) + tokens, BF16),
            dma((8,)),
            dma((4,)),
            dma((4, number)),
            dma((2,)),
            dma((2, len(GATHER))),
            dma((2,)),
            dma((2, 4, 2)),
            dma((2,)),
            dma((2, 2, 6)),
        ],
        compiler_params=pltpu.CompilerParams(
            collective_id=0, has_side_effects=True, vmem_limit_bytes=63 * 1024 * 1024
        ),
    )(
        resid.reshape(tokens), mix_gain[None], cut(w_query), cut(w_key), cut(w_value), cut(w_gate),
        cut(w_output), decay_rate, mlp_gain[None], cut(w_up), cut(w_down),
    )
    return result.reshape(resid.shape)


def solution(mesh):
    placed = (
        P(("fs", "tp"), None),
        P(),
        P("fs", "tp"),
        P("fs", "tp"),
        P("fs", "tp"),
        P("fs", "tp"),
        P("tp", "fs"),
        P("tp"),
        P(),
        P("fs", "tp"),
        P("tp", "fs"),
    )
    return jax.shard_map(
        on_device, mesh=mesh, in_specs=placed, out_specs=P(("fs", "tp"), None), check_vma=False
    )
```

```python
import jax
import jax.numpy as jnp
from jax import lax
from jax.experimental import pallas as pl
from jax.experimental.pallas import tpu as pltpu
from jax.sharding import PartitionSpec as P

D = 2048
DK = 128
DV = 256
LENGTH = 512
RING = 4
EPS = 1e-06
MESH = pl.DeviceIdType.MESH
F32 = jnp.float32
BF16 = jnp.bfloat16

STEP = {"y+": (1, 0), "y-": (-1, 0), "z+": (0, 1), "z-": (0, -1)}


def near(d):
    return {0: 0, 1: 1, 2: 2, 3: -1}[d % RING]


def arrived(message):
    dy, dz, part, way = message
    return near(dy - STEP[way][0]), near(dz - STEP[way][1]), part, way


def onward(message):
    dy, dz, part, way = arrived(message)
    half = "0" if way[1] == "+" else "1"
    along = way[0] == "y"
    across = ("z+", "z-") if along else ("y+", "y-")
    first = "A" if along else "B"
    if part == "full":
        return [(dy, dz, "h" + half, way)] + [(dy, dz, first, w) for w in across]
    if part in ("h0", "h1"):
        onto = [(dy, dz, part, way)] if (dy if along else dz) != 2 and part[1] == half else []
        return onto + [(dy, dz, first + part, w) for w in across]
    if part in ("A", "B"):
        return [(dy, dz, part + "h" + half, way)]
    if (dy if way[0] == "y" else dz) != 2 and part[-1] == half:
        return [(dy, dz, part, way)]
    return []


def plan(parts):
    messages = [(0, 0, part, way) for part in parts for way in ("y+", "y-", "z+", "z-")]
    for message in messages:
        messages += onward(message)
    return messages


MESSAGES = [plan(parts) for parts in (("h0", "h1"), ("full",), ("full",), ("h0", "h1"))]
PLACES = (
    (0, 0), (1, 0), (-1, 0), (0, 1), (0, -1), (2, 0), (0, 2), (1, 1),
    (1, -1), (-1, 1), (-1, -1), (2, 1), (2, -1), (1, 2), (-1, 2), (2, 2),
)

GATHER = (
    [(0, h, q, w) for h in (0, 1) for q in (0, 1) for w in ("x+", "x-")]
    + [(0, h, None, "d") for h in (0, 1)]
    + [(dx, h, q, "d") for dx in (-1, 1, 2) for h in (0, 1) for q in (0, 1)]
    + [(-1, h, 0, "x+") for h in (0, 1)]
    + [(1, h, 1, "x-") for h in (0, 1)]
)
TURN = {2: 0, 1: 1, -1: 2, 0: 3}

SCHEDULE = (
    ("s", "w", 0, 0), ("s", "w", 0, 5), ("s", "w", 0, 2), ("s", "w", 0, 7), ("s", "g", 0, 0), ("s", "g", 0, 3), ("s", "g", 0, 8),
    ("s", "g", 0, 9), ("decay",), ("r", "g", 0, 8), ("s", "w", 1, 0), ("s", "w", 1, 1), ("s", "w", 1, 2), ("s", "w", 1, 3),
    ("r", "g", 0, 9), ("s", "g", 0, 2), ("s", "g", 0, 1), ("s", "w", 0, 4), ("s", "w", 0, 1), ("s", "w", 0, 6), ("s", "w", 0, 3),
    ("r", "w", 0, 0), ("r", "w", 0, 5), ("r", "w", 0, 2), ("r", "w", 0, 7), ("r", "g", 0, 0), ("s", "g", 0, 10), ("r", "g", 0, 3),
    ("s", "g", 0, 15), ("s", "w", 0, 8), ("s", "w", 0, 20), ("s", "w", 0, 13), ("s", "w", 0, 25), ("s", "g", 0, 22), ("s", "g", 0, 24),
    ("r", "w", 1, 0), ("r", "w", 1, 1), ("r", "w", 1, 2), ("r", "w", 1, 3), ("r", "g", 0, 10), ("r", "g", 0, 15), ("s", "w", 1, 4),
    ("s", "w", 1, 7), ("s", "w", 1, 10), ("s", "w", 1, 13), ("r", "g", 0, 2), ("s", "g", 0, 11), ("r", "g", 0, 1), ("s", "g", 0, 14),
    ("r", "w", 0, 4), ("r", "w", 0, 1), ("r", "w", 0, 6), ("r", "w", 0, 3), ("s", "w", 0, 14), ("s", "w", 0, 27), ("s", "w", 0, 9),
    ("s", "w", 0, 22), ("s", "g", 0, 4), ("s", "g", 0, 7), ("r", "g", 0, 11), ("s", "w", 1, 11), ("s", "w", 1, 12), ("s", "w", 1, 5),
    ("s", "w", 1, 6), ("r", "g", 0, 14), ("r", "w", 0, 8), ("r", "w", 0, 20), ("r", "w", 0, 13), ("r", "w", 0, 25), ("s", "w", 1, 14),
    ("s", "w", 1, 15), ("s", "w", 1, 8), ("s", "w", 1, 9), ("r", "g", 0, 22), ("s", "g", 0, 18), ("r", "g", 0, 24), ("s", "g", 0, 19),
    ("r", "w", 1, 4), ("r", "w", 1, 7), ("r", "w", 1, 10), ("r", "w", 1, 13), ("s", "w", 0, 16), ("s", "w", 0, 24), ("s", "w", 0, 11),
    ("s", "w", 0, 19), ("s", "g", 0, 6), ("s", "g", 0, 5), ("r", "w", 0, 14), ("r", "w", 0, 27), ("r", "w", 0, 9), ("r", "w", 0, 22),
    ("s", "w", 0, 32), ("s", "w", 0, 42), ("s", "w", 0, 28), ("s", "w", 0, 38), ("r", "g", 0, 18), ("r", "g", 0, 19), ("r", "w", 1, 11),
    ("r", "w", 1, 12), ("r", "w", 1, 5), ("r", "w", 1, 6), ("s", "w", 1, 24), ("s", "w", 1, 29), ("s", "w", 1, 16), ("s", "w", 1, 21),
    ("r", "w", 1, 14), ("r", "w", 1, 15), ("r", "w", 1, 8), ("r", "w", 1, 9), ("s", "w", 0, 26), ("s", "w", 0, 15), ("s", "w", 0, 21),
    ("s", "w", 0, 10), ("r", "g", 0, 4), ("s", "g", 0, 12), ("r", "g", 0, 7), ("s", "g", 0, 17), ("s", "g", 0, 23), ("s", "g", 0, 25),
    ("r", "w", 0, 16), ("r", "w", 0, 24), ("r", "w", 0, 11), ("r", "w", 0, 19), ("s", "w", 0, 23), ("s", "w", 0, 17), ("s", "w", 0, 18),
    ("s", "w", 0, 12), ("r", "g", 0, 12), ("r", "g", 0, 17), ("r", "w", 0, 32), ("r", "w", 0, 42), ("r", "w", 0, 28), ("r", "w", 0, 38),
    ("s", "w", 0, 41), ("s", "w", 0, 33), ("s", "w", 0, 37), ("s", "w", 0, 29), ("r", "w", 1, 24), ("r", "w", 1, 29), ("r", "w", 1, 16),
    ("r", "w", 1, 21), ("r", "g", 0, 6), ("s", "g", 0, 13), ("r", "g", 0, 5), ("s", "g", 0, 16), ("s", "w", 1, 28), ("s", "w", 1, 25),
    ("s", "w", 1, 20), ("s", "w", 1, 17), ("r", "w", 0, 26), ("r", "w", 0, 15), ("r", "w", 0, 21), ("r", "w", 0, 10), ("s", "w", 0, 34),
    ("s", "w", 0, 43), ("s", "w", 0, 30), ("s", "w", 0, 39), ("r", "g", 0, 13), ("r", "w", 0, 23), ("r", "w", 0, 17), ("r", "w", 0, 18),
    ("r", "w", 0, 12), ("s", "w", 1, 26), ("s", "w", 1, 27), ("s", "w", 1, 18), ("s", "w", 1, 19), ("r", "g", 0, 16), ("s", "w", 1, 30),
    ("s", "w", 1, 31), ("s", "w", 1, 22), ("s", "w", 1, 23), ("s", "w", 0, 35), ("s", "w", 0, 40), ("s", "w", 0, 31), ("s", "w", 0, 36),
    ("r", "w", 0, 41), ("r", "w", 0, 33), ("r", "w", 0, 37), ("r", "w", 0, 29), ("r", "g", 0, 23), ("s", "g", 0, 20), ("r", "g", 0, 25),
    ("s", "g", 0, 21), ("r", "w", 1, 28), ("r", "w", 1, 25), ("r", "w", 1, 20), ("r", "w", 1, 17), ("s", "w", 0, 45), ("s", "w", 0, 47),
    ("s", "w", 0, 44), ("s", "w", 0, 46), ("r", "w", 0, 34), ("r", "w", 0, 43), ("r", "w", 0, 30), ("r", "w", 0, 39), ("r", "g", 0, 20),
    ("r", "w", 1, 26), ("r", "w", 1, 27), ("r", "w", 1, 18), ("r", "w", 1, 19), ("s", "w", 1, 34), ("s", "w", 1, 35), ("s", "w", 1, 32),
    ("s", "w", 1, 33), ("r", "g", 0, 21), ("r", "w", 1, 30), ("r", "w", 1, 31), ("r", "w", 1, 22), ("r", "w", 1, 23), ("s", "w", 2, 0),
    ("s", "w", 2, 1), ("s", "w", 2, 2), ("s", "w", 2, 3), ("r", "w", 0, 35), ("r", "w", 0, 40), ("r", "w", 0, 31), ("r", "w", 0, 36),
    ("r", "w", 0, 45), ("r", "w", 0, 47), ("r", "w", 0, 44), ("r", "w", 0, 46), ("project", 1), ("r", "w", 1, 34), ("r", "w", 1, 35),
    ("r", "w", 1, 32), ("r", "w", 1, 33), ("retain", 1), ("s", "w", 3, 0), ("s", "w", 3, 5), ("s", "w", 3, 2), ("s", "w", 3, 7),
    ("part", 0, ((2, 0), (2, 1)), 0), ("project", 0), ("r", "d", 0, 0, 0, 0), ("r", "d", 0, 0, 1, 0), ("far", 0, 0, 0), ("s", "s", 0, 0, 0, 0),
    ("s", "s", 0, 0, 0, 1), ("r", "w", 2, 0), ("r", "w", 2, 1), ("r", "w", 2, 2), ("r", "w", 2, 3), ("far", 0, 1, 0), ("s", "w", 2, 4),
    ("s", "w", 2, 7), ("s", "w", 2, 10), ("s", "w", 2, 13), ("retain", 0), ("part", 0, ((1, 0), (-1, 0)), 0), ("s", "s", 0, 1, 0, 0),
    ("s", "s", 0, 1, 0, 1), ("part", 0, ((1, 1), (-1, 1)), 0), ("s", "w", 2, 11), ("s", "w", 2, 12), ("s", "w", 2, 5), ("s", "w", 2, 6),
    ("part", 0, ((0, 0), (0, 1)), 0), ("r", "w", 3, 0), ("r", "w", 3, 5), ("r", "w", 3, 2), ("r", "w", 3, 7), ("r", "d", 0, 1, 0, 0),
    ("free", 0, 0, 0, 1), ("r", "d", 0, 2, 0, 0), ("free", 0, 0, 0, 2), ("r", "d", 0, 1, 1, 0), ("free", 0, 1, 0, 1), ("r", "s", 0, 0, 0, 0),
    ("r", "s", 0, 0, 0, 1), ("near", 0, 0, 0, 1), ("r", "d", 0, 2, 1, 0), ("near", 0, 0, 0, 2), ("free", 0, 1, 0, 2), ("s", "s", 0, 0, 0, 2),
    ("s", "s", 0, 0, 0, 5), ("r", "d", 0, 3, 0, 0), ("r", "w", 2, 4), ("r", "w", 2, 7), ("r", "w", 2, 10), ("r", "w", 2, 13),
    ("s", "w", 2, 14), ("s", "w", 2, 15), ("s", "w", 2, 8), ("s", "w", 2, 9), ("r", "d", 0, 3, 1, 0), ("r", "s", 0, 1, 0, 0),
    ("r", "s", 0, 1, 0, 1), ("near", 0, 1, 0, 1), ("near", 0, 1, 0, 2), ("s", "s", 0, 0, 0, 3), ("s", "s", 0, 0, 0, 4), ("r", "w", 2, 11),
    ("r", "w", 2, 12), ("r", "w", 2, 5), ("r", "w", 2, 6), ("s", "w", 2, 24), ("s", "w", 2, 29), ("s", "w", 2, 16), ("s", "w", 2, 21),
    ("s", "w", 2, 28), ("s", "w", 2, 25), ("s", "w", 2, 20), ("s", "w", 2, 17), ("r", "s", 0, 0, 0, 2), ("r", "s", 0, 0, 0, 5),
    ("s", "s", 0, 1, 0, 2), ("s", "s", 0, 1, 0, 5), ("r", "w", 2, 14), ("r", "w", 2, 15), ("r", "w", 2, 8), ("r", "w", 2, 9),
    ("s", "w", 2, 26), ("s", "w", 2, 27), ("s", "w", 2, 18), ("s", "w", 2, 19), ("r", "w", 2, 24), ("r", "w", 2, 29), ("r", "w", 2, 16),
    ("r", "w", 2, 21), ("s", "w", 2, 30), ("s", "w", 2, 31), ("s", "w", 2, 22), ("s", "w", 2, 23), ("r", "s", 0, 0, 0, 3),
    ("r", "s", 0, 0, 0, 4), ("s", "s", 0, 1, 0, 3), ("s", "s", 0, 1, 0, 4), ("norm2", 0), ("s", "g", 1, 8), ("r", "w", 2, 28),
    ("r", "w", 2, 25), ("r", "w", 2, 20), ("r", "w", 2, 17), ("s", "w", 2, 34), ("s", "w", 2, 35), ("s", "w", 2, 32), ("s", "w", 2, 33),
    ("r", "w", 2, 26), ("r", "w", 2, 27), ("r", "w", 2, 18), ("r", "w", 2, 19), ("r", "g", 1, 8), ("s", "w", 3, 4), ("s", "w", 3, 1),
    ("s", "w", 3, 6), ("s", "w", 3, 3), ("r", "s", 0, 1, 0, 2), ("r", "s", 0, 1, 0, 5), ("s", "g", 1, 0), ("s", "g", 1, 3), ("r", "w", 2, 30),
    ("r", "w", 2, 31), ("r", "w", 2, 22), ("r", "w", 2, 23), ("r", "w", 2, 34), ("r", "w", 2, 35), ("r", "w", 2, 32), ("r", "w", 2, 33),
    ("s", "w", 3, 8), ("s", "w", 3, 20), ("s", "w", 3, 13), ("s", "w", 3, 25), ("r", "s", 0, 1, 0, 3), ("r", "s", 0, 1, 0, 4),
    ("s", "g", 1, 2), ("s", "g", 1, 1), ("norm2", 1), ("s", "g", 1, 9), ("r", "w", 3, 4), ("r", "w", 3, 1), ("r", "w", 3, 6),
    ("r", "w", 3, 3), ("r", "g", 1, 9), ("s", "w", 3, 14), ("s", "w", 3, 27), ("s", "w", 3, 9), ("s", "w", 3, 22), ("r", "g", 1, 0),
    ("s", "g", 1, 10), ("r", "g", 1, 3), ("s", "g", 1, 15), ("s", "g", 1, 22), ("s", "g", 1, 24), ("s", "w", 3, 16), ("s", "w", 3, 24),
    ("s", "w", 3, 11), ("s", "w", 3, 19), ("r", "g", 1, 10), ("r", "g", 1, 15), ("r", "w", 3, 8), ("r", "w", 3, 20), ("r", "w", 3, 13),
    ("r", "w", 3, 25), ("s", "w", 3, 32), ("s", "w", 3, 42), ("s", "w", 3, 28), ("s", "w", 3, 38), ("r", "g", 1, 2), ("s", "g", 1, 11),
    ("r", "g", 1, 1), ("s", "g", 1, 14), ("s", "g", 1, 4), ("s", "g", 1, 7), ("r", "w", 3, 14), ("r", "w", 3, 27), ("r", "w", 3, 9),
    ("r", "w", 3, 22), ("s", "w", 3, 26), ("s", "w", 3, 15), ("s", "w", 3, 21), ("s", "w", 3, 10), ("r", "g", 1, 11), ("r", "g", 1, 14),
    ("s", "w", 3, 23), ("s", "w", 3, 17), ("s", "w", 3, 18), ("s", "w", 3, 12), ("s", "g", 1, 6), ("s", "g", 1, 5),
    ("lift", ((0, 0), (-1, 0), (1, 0))), ("s", "w", 3, 41), ("s", "w", 3, 33), ("s", "w", 3, 37), ("s", "w", 3, 29), ("r", "w", 3, 16),
    ("r", "w", 3, 24), ("r", "w", 3, 11), ("r", "w", 3, 19), ("r", "g", 1, 22), ("s", "g", 1, 18), ("r", "g", 1, 24), ("s", "g", 1, 19),
    ("r", "w", 3, 32), ("r", "w", 3, 42), ("r", "w", 3, 28), ("r", "w", 3, 38), ("r", "w", 3, 26), ("r", "w", 3, 15), ("r", "w", 3, 21),
    ("r", "w", 3, 10), ("s", "w", 3, 34), ("s", "w", 3, 43), ("s", "w", 3, 30), ("s", "w", 3, 39), ("r", "g", 1, 18), ("r", "g", 1, 4),
    ("s", "g", 1, 12), ("r", "g", 1, 7), ("s", "g", 1, 17), ("r", "g", 1, 19), ("s", "w", 3, 35), ("s", "w", 3, 40), ("s", "w", 3, 31),
    ("s", "w", 3, 36), ("s", "g", 1, 23), ("s", "g", 1, 25), ("lift", ((2, 0),)), ("r", "w", 3, 23), ("r", "w", 3, 17), ("r", "w", 3, 18),
    ("r", "w", 3, 12), ("r", "g", 1, 12), ("part", 1, ((2, 0),), 0), ("r", "g", 1, 17), ("s", "w", 3, 45), ("s", "w", 3, 47),
    ("s", "w", 3, 44), ("s", "w", 3, 46), ("part", 1, ((1, 0), (-1, 0)), 0), ("r", "w", 3, 41), ("r", "w", 3, 33), ("r", "w", 3, 37),
    ("r", "w", 3, 29), ("r", "g", 1, 6), ("s", "g", 1, 13), ("r", "g", 1, 5), ("s", "g", 1, 16), ("r", "d", 1, 0, 0, 0), ("far", 1, 0, 0),
    ("s", "s", 1, 0, 0, 0), ("s", "s", 1, 0, 0, 1), ("r", "w", 3, 34), ("r", "w", 3, 43), ("r", "w", 3, 30), ("r", "w", 3, 39),
    ("r", "d", 1, 1, 0, 0), ("free", 1, 0, 0, 1), ("r", "d", 1, 2, 0, 0), ("free", 1, 0, 0, 2), ("s", "s", 1, 0, 0, 3), ("s", "s", 1, 0, 0, 4),
    ("r", "g", 1, 13), ("r", "w", 3, 35), ("r", "w", 3, 40), ("r", "w", 3, 31), ("r", "w", 3, 36), ("r", "g", 1, 16),
    ("lift", ((0, 1), (-1, 1), (1, 1))), ("r", "g", 1, 23), ("s", "g", 1, 20), ("r", "g", 1, 25), ("s", "g", 1, 21), ("r", "w", 3, 45),
    ("r", "w", 3, 47), ("r", "w", 3, 44), ("r", "w", 3, 46), ("r", "s", 1, 0, 0, 0), ("r", "s", 1, 0, 0, 1), ("near", 1, 0, 0, 1),
    ("s", "s", 1, 0, 0, 2), ("near", 1, 0, 0, 2), ("s", "s", 1, 0, 0, 5), ("part", 1, ((2, 0),), 1), ("part", 1, ((1, 1), (-1, 1)), 0),
    ("r", "s", 1, 0, 0, 3), ("r", "s", 1, 0, 0, 4), ("r", "g", 1, 20), ("part", 1, ((1, 0), (-1, 0)), 1), ("r", "g", 1, 21),
    ("r", "d", 1, 0, 0, 1), ("far", 1, 0, 1), ("s", "s", 1, 0, 1, 0), ("s", "s", 1, 0, 1, 1), ("lift", ((2, 1),)), ("r", "d", 1, 1, 1, 0),
    ("r", "d", 1, 2, 1, 0), ("r", "s", 1, 0, 0, 2), ("r", "s", 1, 0, 0, 5), ("r", "d", 1, 1, 0, 1), ("free", 1, 1, 0, 1), ("s", "s", 1, 1, 0, 3),
    ("free", 1, 1, 0, 2), ("s", "s", 1, 1, 0, 4), ("free", 1, 0, 1, 1), ("part", 1, ((2, 1),), 0), ("r", "d", 1, 2, 0, 1), ("free", 1, 0, 1, 2),
    ("s", "s", 1, 0, 1, 3), ("s", "s", 1, 0, 1, 4), ("part", 1, ((2, 1),), 1), ("part", 1, ((1, 1), (-1, 1)), 1), ("r", "d", 1, 0, 1, 0),
    ("r", "s", 1, 0, 1, 0), ("r", "s", 1, 0, 1, 1), ("far", 1, 1, 0), ("near", 1, 0, 1, 1), ("near", 1, 0, 1, 2), ("s", "s", 1, 1, 0, 0),
    ("s", "s", 1, 1, 0, 1), ("part", 1, ((0, 0), (0, 1)), 0), ("r", "d", 1, 0, 1, 1), ("far", 1, 1, 1), ("s", "s", 1, 1, 1, 0),
    ("s", "s", 1, 1, 1, 1), ("part", 1, ((0, 0), (0, 1)), 1), ("r", "s", 1, 1, 0, 3), ("r", "s", 1, 1, 0, 4), ("r", "d", 1, 1, 1, 1),
    ("r", "d", 1, 2, 1, 1), ("free", 1, 1, 1, 1), ("free", 1, 1, 1, 2), ("r", "d", 1, 3, 0, 0), ("finish", 0, 0), ("r", "d", 1, 3, 1, 0),
    ("r", "s", 1, 0, 1, 3), ("r", "s", 1, 0, 1, 4), ("s", "s", 1, 0, 1, 2), ("s", "s", 1, 0, 1, 5), ("r", "d", 1, 3, 0, 1), ("r", "d", 1, 3, 1, 1),
    ("r", "s", 1, 1, 0, 0), ("near", 1, 1, 0, 1), ("r", "s", 1, 1, 0, 1), ("near", 1, 1, 0, 2), ("s", "s", 1, 1, 0, 2), ("s", "s", 1, 1, 0, 5),
    ("r", "s", 1, 1, 1, 0), ("near", 1, 1, 1, 1), ("r", "s", 1, 1, 1, 1), ("near", 1, 1, 1, 2), ("s", "s", 1, 1, 1, 2), ("s", "s", 1, 1, 1, 5),
    ("r", "s", 1, 0, 1, 2), ("r", "s", 1, 0, 1, 5), ("finish", 0, 1), ("s", "s", 1, 1, 1, 3), ("s", "s", 1, 1, 1, 4), ("r", "s", 1, 1, 0, 2),
    ("r", "s", 1, 1, 0, 5), ("finish", 1, 0), ("r", "s", 1, 1, 1, 2), ("r", "s", 1, 1, 1, 5), ("r", "s", 1, 1, 1, 3), ("r", "s", 1, 1, 1, 4),
    ("finish", 1, 1),
)


def kernel(
    resid, mix_gain, wq, wk, wv, wg, wo, rate, mlp_gain, wu, wd,
    out,
    w_in, w_out, w_up, w_down, xn, rbuf, after, proj, gated, hid, decay, kept,
    dout, din, sout, rin2, rin1,
    local_sem, w_send, w_recv, g_send, g_recv, d_send, d_recv, s_send, s_recv,
):
    fs, tp = lax.axis_index("fs"), lax.axis_index("tp")
    z, y, x, c = fs // RING, fs % RING, tp // 2, tp % 2

    def turn(v, d):
        return (v + d + RING) % RING

    device = {
        "y+": (z * RING + turn(y, 1), tp),
        "y-": (z * RING + turn(y, -1), tp),
        "z+": (turn(z, 1) * RING + y, tp),
        "z-": (turn(z, -1) * RING + y, tp),
        "x+": (fs, turn(x, 1) * 2 + c),
        "x-": (fs, turn(x, -1) * 2 + c),
        "d": (fs, x * 2 + 1 - c),
    }

    def remote(src, dst, send, recv, way):
        return pltpu.make_async_remote_copy(
            src_ref=src, dst_ref=dst, send_sem=send, recv_sem=recv,
            device_id=device[way], device_id_type=MESH,
        )

    def send(*args):
        remote(*args).start()

    weights = (w_in, w_out, w_up, w_down)

    def block(dy, dz):
        return turn(z, dz) * RING + turn(y, dy)

    def piece(t, dy, dz, part):
        ref = weights[t]
        f = block(dy, dz)
        if part == "full":
            return ref.at[f]
        if part in ("A", "B"):
            return ref.at[f, :, "AB".index(part)]
        if part in ("h0", "h1"):
            return ref.at[f, int(part[1])]
        return ref.at[f, int(part[2]), "AB".index(part[0])]

    def w_copy(t, n, place):
        dy, dz, part, way = place
        ref = piece(t, dy, dz, part)
        return (ref, ref, w_send.at[t], w_recv.at[t, n], way)

    def g_copy(g, n, dx, core):
        h, q, way = GATHER[n][1:]
        block = turn(x, dx) * 2 + core
        ref = xn.at[g, block, h] if q is None else xn.at[g, block, h, q]
        return (ref, ref, g_send.at[g], g_recv.at[g, n], way)

    def rows16(count, body):
        def step(i, carry):
            body(pl.ds(pl.multiple_of(i * 16, 16), 16))
            return carry

        lax.fori_loop(0, count // 16, step, 0)

    def of(ref, j, g):
        return ref if g == 0 else ref.at[:, pl.ds(j * 1024, 1024)]

    def d_copy(g, k, h, j):
        columns = slice(None) if g == 0 else pl.ds(j * 1024, 1024)
        return (
            dout.at[g, k, h, :, :, columns], din.at[g, k, h, :, :, columns],
            d_send.at[g], d_recv.at[g, k, h, j], "d",
        )

    def s_copy(g, h, j, n):
        if n < 2:
            src, dst, way = sout.at[g, 0, h, n], rin2.at[g, h, n], ("x+", "x-")[n]
        elif n < 4:
            src, dst, way = sout.at[g, 1, h, n - 2], rin1.at[g, 0, h, n - 2], "x+"
        else:
            src, dst, way = sout.at[g, 2, h, n - 4], rin1.at[g, 1, h, n - 4], "x-"
        return (of(src, j, g), of(dst, j, g), s_send.at[g], s_recv.at[g, h, j, n], way)

    def start(kind, *which):
        if kind == "w":
            t, n = which
            send(*w_copy(t, n, MESSAGES[t][n]))
        elif kind == "g":
            g, n = which
            send(*g_copy(g, n, GATHER[n][0], c))
        else:
            send(*s_copy(*which))

    def receive(kind, *which):
        if kind == "w":
            t, n = which
            copy = w_copy(t, n, arrived(MESSAGES[t][n]))
        elif kind == "g":
            g, n = which
            dx, way = GATHER[n][0], GATHER[n][3]
            if way == "d":
                copy = g_copy(g, n, dx, 1 - c)
            else:
                copy = g_copy(g, n, near(dx - (1 if way == "x+" else -1)), c)
        elif kind == "d":
            copy = d_copy(*which)
        else:
            copy = s_copy(*which)
        remote(*copy).wait_recv()

    def product(g, cases, lhs, w, columns):
        rows = jnp.concatenate([block for case in cases for block in lhs(*case)], axis=0)
        o = jnp.dot(rows, w, preferred_element_type=F32)
        for n, (dx, h) in enumerate(cases):
            mine = o[n * 128 : (n + 1) * 128]
            dout[g, TURN[dx], h, :, :, columns] = mine[:64].astype(BF16).reshape(2, 32, 512)
            kept[TURN[dx], h, :, :, columns] = mine[64:].reshape(2, 32, 512)

    def partial(g, cases, j):
        if g == 0:
            depth = wo.shape[0] * wo.shape[1] * wo.shape[2]

            def step(i, carry):
                w = [w_out[4 * i + n].reshape(depth, 128) for n in range(4)]
                columns = pl.ds(pl.multiple_of(i * 512, 512), 512)
                product(0, cases, gated_rows, jnp.concatenate(w, axis=1), columns)
                return carry

            lax.fori_loop(0, 4, step, 0)
        else:
            depth = wd.shape[0] * wd.shape[1] * wd.shape[2]
            for i in (2 * j, 2 * j + 1):
                w = [w_down[block(*PLACES[4 * i + n])].reshape(depth, 128) for n in range(4)]
                columns = slice(i * 512, (i + 1) * 512)
                product(1, cases, hidden_rows, jnp.concatenate(w, axis=1), columns)
        for dx, h in cases:
            send(*d_copy(g, TURN[dx], h, j))

    def add_quarter(g, k, h, j, q, extra=False):
        columns = slice(None) if g == 0 else slice(j * 1024, (j + 1) * 1024)

        def body(rows):
            total = kept[k, h, q, rows, columns] + din[g, k, h, q, rows, columns].astype(F32)
            if extra:
                total = total + rin2[g, h, q, rows, columns].astype(F32)
            sout[g, k, h, q, rows, columns] = total.astype(BF16)

        rows16(32, body)

    def add_far(g, h, j):
        for q in (0, 1):
            add_quarter(g, 0, h, j, q)

    def add_free(g, h, j, k):
        add_quarter(g, k, h, j, 1 if k == 1 else 0)

    def add_near(g, h, j, k):
        add_quarter(g, k, h, j, 0 if k == 1 else 1, True)

    def sum_rows(h, q, rows):
        total = kept[3, h, q, rows, :] + din[0, 3, h, q, rows, :].astype(F32)
        return total + rin1[0, 0, h, q, rows, :].astype(F32) + rin1[0, 1, h, q, rows, :].astype(F32)

    def normed(values, gain):
        scale = lax.rsqrt(jnp.mean(values * values, axis=-1, keepdims=True) + EPS)
        return (values * scale * gain).astype(BF16)

    loads = []

    def load(src, dst):
        copy = pltpu.make_async_copy(src, dst, local_sem.at[len(loads)])
        copy.start()
        loads.append(copy)

    for src, low, wide in ((wq, 0, 128), (wk, 128, 128), (wv, 256, 256), (wg, 512, 256)):
        load(src, w_in.at[fs, :, :, :, low : low + wide])
    load(resid, rbuf)
    load(wo, w_out.at[fs])
    load(wu, w_up.at[fs])
    load(wd, w_down.at[fs])
    barrier = pltpu.get_barrier_semaphore()
    for way in device:
        pl.semaphore_signal(barrier, inc=1, device_id=device[way], device_id_type=MESH)
    for copy in loads[:5]:
        copy.wait()
    for h in (0, 1):
        for q in (0, 1):
            def first_norm(rows):
                xn[0, tp, h, q, rows, :] = normed(rbuf[h, q, rows, :].astype(F32), mix_gain[...])

            rows16(32, first_norm)
    pl.semaphore_wait(barrier, 7)
    r = rate[0]

    def make_decay():
        def some_rows(i, carry):
            rows = pl.ds(pl.multiple_of(i * 64, 64), 64)
            t = lax.broadcasted_iota(jnp.int32, (64, LENGTH), 0) + i * 64
            s = lax.broadcasted_iota(jnp.int32, (64, LENGTH), 1)
            gap = (t - s).astype(F32)
            value = jnp.exp(-r * jnp.maximum(gap, 0.0)) * DK ** (-0.5)
            decay[rows, :] = jnp.where(gap >= 0.0, value, 0.0)
            return carry

        lax.fori_loop(0, LENGTH // 64, some_rows, 0)

    own = x // 2
    sequence = (own, 1 - own)

    def project(seq):
        def body(j, carry):
            columns = pl.ds(pl.multiple_of(j * 256, 256), 256)
            lhs = xn[0, pl.ds(4 * seq, 4)].reshape(512, D)
            rhs = w_in[:, :, :, :, columns].reshape(D, 256)
            o = jnp.dot(lhs, rhs, preferred_element_type=F32).astype(BF16)
            proj[pl.ds(4 * seq, 4), :, columns] = o.reshape(4, 128, 256)
            return carry

        lax.fori_loop(0, 3, body, 0)

    def retain(seq):
        for i in (0, 1):
            mine = pl.ds(seq * 4 + 2 * i, 2)
            upto = pl.ds(seq * 4, 2 * i + 2)
            wide = 256 * (i + 1)
            q = proj[mine, :, 0:128].reshape(256, DK)
            k = proj[upto, :, 128:256].reshape(wide, DK)
            v = proj[upto, :, 256:512].reshape(wide, DV)
            scores = lax.dot_general(q, k, (((1,), (1,)), ((), ())), preferred_element_type=F32)
            scores = (scores * decay[i * 256 : (i + 1) * 256, 0:wide]).astype(BF16)
            mixed = jnp.dot(scores, v, preferred_element_type=F32)
            mixed = mixed - jnp.mean(mixed, axis=-1, keepdims=True)
            spread = jnp.mean(mixed * mixed, axis=-1, keepdims=True)
            gate = proj[mine, :, 512:768].reshape(256, DV).astype(F32)
            value = gate / (1.0 + jnp.exp(-gate)) * (mixed * lax.rsqrt(spread + EPS))
            gated[mine] = value.astype(BF16).reshape(2, 2, 64, DV)

    def gated_rows(dx, h):
        first = turn(x, dx) * 2
        return gated[first + 1 - c, h], gated[first + c, h]

    def lift(cases):
        def body(j, carry):
            columns = pl.ds(pl.multiple_of(j * 256, 256), 256)
            lhs = jnp.concatenate(
                [
                    xn[1, turn(x, dx) * 2 + core, h].reshape(64, D)
                    for dx, h in cases
                    for core in (1 - c, c)
                ],
                axis=0,
            )
            rhs = w_up[:, :, :, :, columns].reshape(D, 256)
            o = jnp.maximum(jnp.dot(lhs, rhs, preferred_element_type=F32), 0.0)
            o = (o * o).astype(BF16)
            for n, (dx, h) in enumerate(cases):
                hid[TURN[dx], h, :, columns] = o[n * 128 : (n + 1) * 128]
            return carry

        lax.fori_loop(0, w_up.shape[4] // 256, body, 0)

    def hidden_rows(dx, h):
        return (hid[TURN[dx], h],)

    def second_norm(h):
        for q in (0, 1):
            def body(rows):
                value = rbuf[h, q, rows, :].astype(F32) + sum_rows(h, q, rows)
                value = value.astype(BF16)
                after[h, q, rows, :] = value
                xn[1, tp, h, q, rows, :] = normed(value.astype(F32), mlp_gain[...])

            rows16(32, body)

    def finish(h, j):
        for i in range(8 * j, 8 * j + 8):
            here = pl.ds(pl.multiple_of(block(*PLACES[i]) * 128, 128), 128)
            at = slice(i * 128, (i + 1) * 128)
            total = after[h, :, :, here].astype(F32) + kept[3, h, :, :, at]
            total = total + din[1, 3, h, :, :, at].astype(F32)
            total = total + rin1[1, 0, h, :, :, at].astype(F32) + rin1[1, 1, h, :, :, at].astype(F32)
            out[h, :, :, here] = total.astype(BF16)

    actions = {
        "s": start,
        "r": receive,
        "decay": make_decay,
        "project": lambda which: project(sequence[which]),
        "retain": lambda which: retain(sequence[which]),
        "part": partial,
        "far": add_far,
        "free": add_free,
        "near": add_near,
        "norm2": second_norm,
        "lift": lift,
        "finish": finish,
    }
    for copy in loads[5:]:
        copy.wait()
    for name, *which in SCHEDULE:
        actions[name](*which)
    for t in range(4):
        ref = weights[t].at[0:15]
        remote(ref, ref, w_send.at[t], w_recv.at[t, 0], "d").wait_send()
    for g in (0, 1):
        remote(xn.at[g, 0:7], xn.at[g, 0:7], g_send.at[g], g_recv.at[g, 0], "d").wait_send()
        remote(dout.at[g], din.at[g], d_send.at[g], d_recv.at[g, 0, 0, 0], "d").wait_send()
        remote(sout.at[g], sout.at[g], s_send.at[g], s_recv.at[g, 0, 0, 0], "d").wait_send()


def on_device(
    resid, mix_gain, w_query, w_key, w_value, w_gate, w_output, decay_rate, mlp_gain, w_up, w_down
):
    def cut(w):
        return w.reshape(2, 2, w.shape[0] // 4, w.shape[1])

    wide = w_query.shape[1] + w_key.shape[1] + w_value.shape[1] + w_gate.shape[1]
    count = RING * RING

    def held(rows, columns):
        return pltpu.VMEM((count, 2, 2, rows // 4, columns), BF16)

    dma = pltpu.SemaphoreType.DMA
    vmem = pl.BlockSpec(memory_space=pltpu.VMEM)
    hbm = pl.BlockSpec(memory_space=pl.ANY)
    tokens = (2, 2, 32, D)
    number = max(len(messages) for messages in MESSAGES)
    result = pl.pallas_call(
        kernel,
        out_shape=jax.ShapeDtypeStruct(tokens, BF16),
        in_specs=[
            hbm, vmem, hbm, hbm, hbm, hbm, hbm,
            pl.BlockSpec(memory_space=pltpu.SMEM), vmem, hbm, hbm,
        ],
        out_specs=vmem,
        scratch_shapes=[
            held(128, wide),
            held(w_output.shape[0], 128),
            held(128, w_up.shape[1]),
            held(w_down.shape[0], 128),
            pltpu.VMEM((2, 8) + tokens, BF16),
            pltpu.VMEM(tokens, BF16),
            pltpu.VMEM(tokens, BF16),
            pltpu.VMEM((8, 128, wide), BF16),
            pltpu.VMEM((8, 2, 64, DV), BF16),
            pltpu.VMEM((4, 2, 128, w_up.shape[1]), BF16),
            pltpu.VMEM((LENGTH, LENGTH), F32),
            pltpu.VMEM((4,) + tokens, F32),
            pltpu.VMEM((2, 4) + tokens, BF16),
            pltpu.VMEM((2, 4) + tokens, BF16),
            pltpu.VMEM((2, 3) + tokens, BF16),
            pltpu.VMEM((2,) + tokens, BF16),
            pltpu.VMEM((2, 2) + tokens, BF16),
            dma((8,)),
            dma((4,)),
            dma((4, number)),
            dma((2,)),
            dma((2, len(GATHER))),
            dma((2,)),
            dma((2, 4, 2, 2)),
            dma((2,)),
            dma((2, 2, 2, 6)),
        ],
        compiler_params=pltpu.CompilerParams(
            collective_id=0, has_side_effects=True, vmem_limit_bytes=63 * 1024 * 1024
        ),
    )(
        resid.reshape(tokens), mix_gain[None], cut(w_query), cut(w_key), cut(w_value), cut(w_gate),
        cut(w_output), decay_rate, mlp_gain[None], cut(w_up), cut(w_down),
    )
    return result.reshape(resid.shape)


def solution(mesh):
    placed = (
        P(("fs", "tp"), None),
        P(),
        P("fs", "tp"),
        P("fs", "tp"),
        P("fs", "tp"),
        P("fs", "tp"),
        P("tp", "fs"),
        P("tp"),
        P(),
        P("fs", "tp"),
        P("tp", "fs"),
    )
    return jax.shard_map(
        on_device, mesh=mesh, in_specs=placed, out_specs=P(("fs", "tp"), None), check_vma=False
    )
```

```python
import jax
import jax.numpy as jnp
from jax import lax
from jax.experimental import pallas as pl
from jax.experimental.pallas import tpu as pltpu
from jax.sharding import PartitionSpec as P

D = 2048
DK = 128
DV = 256
LENGTH = 512
RING = 4
EPS = 1e-06
MESH = pl.DeviceIdType.MESH
F32 = jnp.float32
BF16 = jnp.bfloat16

STEP = {"y+": (1, 0), "y-": (-1, 0), "z+": (0, 1), "z-": (0, -1)}


def near(d):
    return {0: 0, 1: 1, 2: 2, 3: -1}[d % RING]


def arrived(message):
    dy, dz, part, way = message
    return near(dy - STEP[way][0]), near(dz - STEP[way][1]), part, way


def onward(message):
    dy, dz, part, way = arrived(message)
    half = "0" if way[1] == "+" else "1"
    along = way[0] == "y"
    across = ("z+", "z-") if along else ("y+", "y-")
    first = "A" if along else "B"
    if part == "full":
        return [(dy, dz, "h" + half, way)] + [(dy, dz, first, w) for w in across]
    if part in ("h0", "h1"):
        onto = [(dy, dz, part, way)] if (dy if along else dz) != 2 and part[1] == half else []
        return onto + [(dy, dz, first + part, w) for w in across]
    if part in ("A", "B"):
        return [(dy, dz, part + "h" + half, way)]
    if (dy if way[0] == "y" else dz) != 2 and part[-1] == half:
        return [(dy, dz, part, way)]
    return []


def plan(parts):
    messages = [(0, 0, part, way) for part in parts for way in ("y+", "y-", "z+", "z-")]
    for message in messages:
        messages += onward(message)
    return messages


MESSAGES = [plan(parts) for parts in (("h0", "h1"), ("full",), ("full",), ("h0", "h1"))]
PLACES = (
    (0, 0), (1, 0), (-1, 0), (0, 1), (0, -1), (2, 0), (0, 2), (1, 1),
    (1, -1), (-1, 1), (-1, -1), (2, 1), (2, -1), (1, 2), (-1, 2), (2, 2),
)

GATHER = (
    [(0, h, q, w) for h in (0, 1) for q in (0, 1) for w in ("x+", "x-")]
    + [(0, h, None, "d") for h in (0, 1)]
    + [(dx, h, q, "d") for dx in (-1, 1, 2) for h in (0, 1) for q in (0, 1)]
    + [(-1, h, 0, "x+") for h in (0, 1)]
    + [(1, h, 1, "x-") for h in (0, 1)]
)
TURN = {2: 0, 1: 1, -1: 2, 0: 3}

S, R, W, G, C, X = range(6)
DECAY, PROJECT, RETAIN, PRODUCT, FAR, FREE, NEAR, NORM, LIFT, FINISH = range(6, 16)
SCHEDULE = (
    (S, W, 0, 0), (S, W, 0, 5), (S, W, 0, 2), (S, W, 0, 7), (S, G, 0, 0), (S, G, 0, 3), (S, G, 0, 8), (S, G, 0, 9),
    (DECAY,), (S, W, 1, 0), (S, W, 1, 1), (S, W, 1, 2), (S, W, 1, 3), (R, G, 0, 8), (S, G, 0, 2), (S, G, 0, 1),
    (R, G, 0, 9), (S, W, 0, 4), (S, W, 0, 1), (S, W, 0, 6), (S, W, 0, 3), (R, W, 0, 0), (R, W, 0, 5), (R, W, 0, 2),
    (R, W, 0, 7), (S, W, 0, 8), (S, W, 0, 20), (S, W, 0, 13), (S, W, 0, 25), (S, G, 0, 4), (S, G, 0, 7), (R, G, 0, 0),
    (S, G, 0, 10), (R, G, 0, 3), (S, G, 0, 15), (R, W, 1, 0), (R, W, 1, 1), (R, W, 1, 2), (R, W, 1, 3), (R, G, 0, 10),
    (S, W, 1, 4), (S, W, 1, 7), (S, W, 1, 10), (S, W, 1, 13), (R, G, 0, 15), (S, W, 0, 14), (S, W, 0, 27),
    (S, W, 0, 9), (S, W, 0, 22), (S, G, 0, 22), (S, G, 0, 24), (R, G, 0, 2), (S, G, 0, 11), (R, G, 0, 1),
    (S, G, 0, 14), (R, W, 0, 4), (R, W, 0, 1), (R, W, 0, 6), (R, W, 0, 3), (S, W, 1, 11), (S, W, 1, 12), (S, W, 1, 5),
    (S, W, 1, 6), (S, W, 1, 14), (S, W, 1, 15), (S, W, 1, 8), (S, W, 1, 9), (R, G, 0, 11), (R, G, 0, 14),
    (S, W, 0, 16), (S, W, 0, 24), (S, W, 0, 11), (S, W, 0, 19), (R, W, 0, 8), (R, W, 0, 20), (R, W, 0, 13),
    (R, W, 0, 25), (S, G, 0, 6), (S, G, 0, 5), (R, G, 0, 4), (S, G, 0, 12), (R, G, 0, 7), (S, G, 0, 17), (R, W, 1, 4),
    (R, W, 1, 7), (R, W, 1, 10), (R, W, 1, 13), (S, W, 0, 32), (S, W, 0, 42), (S, W, 0, 28), (S, W, 0, 38),
    (R, W, 0, 14), (R, W, 0, 27), (R, W, 0, 9), (R, W, 0, 22), (S, W, 1, 24), (S, W, 1, 29), (S, W, 1, 16),
    (S, W, 1, 21), (R, G, 0, 12), (S, W, 0, 26), (S, W, 0, 15), (S, W, 0, 21), (S, W, 0, 10), (R, G, 0, 17),
    (R, W, 1, 11), (R, W, 1, 12), (R, W, 1, 5), (R, W, 1, 6), (S, G, 0, 23), (S, G, 0, 25), (R, W, 1, 14),
    (R, W, 1, 15), (R, W, 1, 8), (R, W, 1, 9), (S, W, 0, 23), (S, W, 0, 17), (S, W, 0, 18), (S, W, 0, 12),
    (R, G, 0, 22), (S, G, 0, 18), (R, G, 0, 24), (S, G, 0, 19), (R, W, 0, 16), (R, W, 0, 24), (R, W, 0, 11),
    (R, W, 0, 19), (S, W, 0, 41), (S, W, 0, 33), (S, W, 0, 37), (S, W, 0, 29), (R, G, 0, 18), (R, G, 0, 19),
    (R, W, 0, 32), (R, W, 0, 42), (R, W, 0, 28), (R, W, 0, 38), (S, W, 1, 28), (S, W, 1, 25), (S, W, 1, 20),
    (S, W, 1, 17), (R, W, 1, 24), (R, W, 1, 29), (R, W, 1, 16), (R, W, 1, 21), (S, W, 0, 34), (S, W, 0, 43),
    (S, W, 0, 30), (S, W, 0, 39), (R, G, 0, 6), (S, G, 0, 13), (R, G, 0, 5), (S, G, 0, 16), (R, W, 0, 26),
    (R, W, 0, 15), (R, W, 0, 21), (R, W, 0, 10), (S, W, 1, 26), (S, W, 1, 27), (S, W, 1, 18), (S, W, 1, 19),
    (S, W, 1, 30), (S, W, 1, 31), (S, W, 1, 22), (S, W, 1, 23), (S, W, 0, 35), (S, W, 0, 40), (S, W, 0, 31),
    (S, W, 0, 36), (R, G, 0, 13), (R, W, 0, 23), (R, W, 0, 17), (R, W, 0, 18), (R, W, 0, 12), (R, G, 0, 16),
    (S, W, 0, 45), (S, W, 0, 47), (S, W, 0, 44), (S, W, 0, 46), (R, W, 0, 41), (R, W, 0, 33), (R, W, 0, 37),
    (R, W, 0, 29), (R, G, 0, 23), (S, G, 0, 20), (R, G, 0, 25), (S, G, 0, 21), (R, W, 1, 28), (R, W, 1, 25),
    (R, W, 1, 20), (R, W, 1, 17), (S, W, 1, 34), (S, W, 1, 35), (S, W, 1, 32), (S, W, 1, 33), (S, W, 2, 0),
    (S, W, 2, 1), (S, W, 2, 2), (S, W, 2, 3), (R, W, 0, 34), (R, W, 0, 43), (R, W, 0, 30), (R, W, 0, 39),
    (R, G, 0, 20), (R, W, 1, 26), (R, W, 1, 27), (R, W, 1, 18), (R, W, 1, 19), (R, G, 0, 21), (R, W, 1, 30),
    (R, W, 1, 31), (R, W, 1, 22), (R, W, 1, 23), (R, W, 0, 35), (R, W, 0, 40), (R, W, 0, 31), (R, W, 0, 36),
    (R, W, 0, 45), (R, W, 0, 47), (R, W, 0, 44), (R, W, 0, 46), (PROJECT, 1, 0), (R, W, 1, 34), (R, W, 1, 35),
    (R, W, 1, 32), (R, W, 1, 33), (PROJECT, 1, 1), (PROJECT, 1, 2), (S, W, 3, 0), (S, W, 3, 5), (S, W, 3, 2),
    (S, W, 3, 7), (RETAIN, 1), (PRODUCT, 0, ((2, 0), (2, 1)), 0), (PROJECT, 0, 0), (PROJECT, 0, 1), (S, W, 3, 4),
    (S, W, 3, 1), (S, W, 3, 6), (S, W, 3, 3), (PROJECT, 0, 2), (R, C, 0, 0, 0, 0), (R, C, 0, 0, 1, 0), (FAR, 0, 0, 0),
    (S, X, 0, 0, 0, 0), (S, X, 0, 0, 0, 1), (R, W, 2, 0), (R, W, 2, 1), (R, W, 2, 2), (R, W, 2, 3), (FAR, 0, 1, 0),
    (RETAIN, 0), (PRODUCT, 0, ((1, 0), (-1, 0)), 0), (S, W, 2, 4), (S, W, 2, 7), (S, W, 2, 10), (S, W, 2, 13),
    (S, X, 0, 1, 0, 0), (S, X, 0, 1, 0, 1), (PRODUCT, 0, ((1, 1), (-1, 1)), 0), (PRODUCT, 0, ((0, 0), (0, 1)), 0),
    (R, W, 3, 0), (R, W, 3, 5), (R, W, 3, 2), (R, W, 3, 7), (R, C, 0, 1, 0, 0), (FREE, 0, 0, 0, 1),
    (R, C, 0, 2, 0, 0), (FREE, 0, 0, 0, 2), (R, C, 0, 1, 1, 0), (FREE, 0, 1, 0, 1), (S, X, 0, 0, 0, 3),
    (S, X, 0, 0, 0, 4), (S, W, 2, 11), (S, W, 2, 12), (S, W, 2, 5), (S, W, 2, 6), (R, C, 0, 2, 1, 0),
    (FREE, 0, 1, 0, 2), (R, X, 0, 0, 0, 0), (R, X, 0, 0, 0, 1), (NEAR, 0, 0, 0, 1), (NEAR, 0, 0, 0, 2),
    (R, C, 0, 3, 0, 0), (R, W, 3, 4), (R, W, 3, 1), (R, W, 3, 6), (R, W, 3, 3), (R, C, 0, 3, 1, 0),
    (S, X, 0, 0, 0, 2), (S, X, 0, 0, 0, 5), (S, W, 2, 14), (S, W, 2, 15), (S, W, 2, 8), (S, W, 2, 9),
    (R, X, 0, 1, 0, 0), (R, X, 0, 1, 0, 1), (NEAR, 0, 1, 0, 1), (NEAR, 0, 1, 0, 2), (R, W, 2, 4), (R, W, 2, 7),
    (R, W, 2, 10), (R, W, 2, 13), (S, X, 0, 1, 0, 2), (S, X, 0, 1, 0, 5), (S, W, 2, 24), (S, W, 2, 29), (S, W, 2, 16),
    (S, W, 2, 21), (R, X, 0, 0, 0, 3), (R, X, 0, 0, 0, 4), (R, W, 2, 11), (R, W, 2, 12), (R, W, 2, 5), (R, W, 2, 6),
    (S, W, 2, 28), (S, W, 2, 25), (S, W, 2, 20), (S, W, 2, 17), (S, X, 0, 1, 0, 3), (S, X, 0, 1, 0, 4), (S, W, 2, 26),
    (S, W, 2, 27), (S, W, 2, 18), (S, W, 2, 19), (R, X, 0, 0, 0, 2), (R, X, 0, 0, 0, 5), (NORM, 0), (S, G, 1, 8),
    (R, W, 2, 14), (R, W, 2, 15), (R, W, 2, 8), (R, W, 2, 9), (S, W, 2, 30), (S, W, 2, 31), (S, W, 2, 22),
    (S, W, 2, 23), (R, W, 2, 24), (R, W, 2, 29), (R, W, 2, 16), (R, W, 2, 21), (S, G, 1, 0), (S, G, 1, 3),
    (R, G, 1, 8), (S, W, 2, 34), (S, W, 2, 35), (S, W, 2, 32), (S, W, 2, 33), (R, X, 0, 1, 0, 2), (R, X, 0, 1, 0, 5),
    (R, W, 2, 28), (R, W, 2, 25), (R, W, 2, 20), (R, W, 2, 17), (S, W, 3, 8), (S, W, 3, 20), (S, W, 3, 13),
    (S, W, 3, 25), (R, W, 2, 26), (R, W, 2, 27), (R, W, 2, 18), (R, W, 2, 19), (S, G, 1, 2), (S, G, 1, 1),
    (R, X, 0, 1, 0, 3), (R, X, 0, 1, 0, 4), (NORM, 1), (S, G, 1, 9), (R, W, 2, 30), (R, W, 2, 31), (R, W, 2, 22),
    (R, W, 2, 23), (S, W, 3, 14), (S, W, 3, 27), (S, W, 3, 9), (S, W, 3, 22), (R, W, 2, 34), (R, W, 2, 35),
    (R, W, 2, 32), (R, W, 2, 33), (S, G, 1, 4), (S, G, 1, 7), (R, G, 1, 9), (S, W, 3, 16), (S, W, 3, 24),
    (S, W, 3, 11), (S, W, 3, 19), (R, G, 1, 0), (S, G, 1, 10), (R, G, 1, 3), (S, G, 1, 15), (S, W, 3, 26),
    (S, W, 3, 15), (S, W, 3, 21), (S, W, 3, 10), (R, G, 1, 10), (R, G, 1, 15), (R, W, 3, 8), (R, W, 3, 20),
    (R, W, 3, 13), (R, W, 3, 25), (S, G, 1, 22), (S, G, 1, 24), (S, W, 3, 32), (S, W, 3, 42), (S, W, 3, 28),
    (S, W, 3, 38), (R, G, 1, 2), (S, G, 1, 11), (R, G, 1, 1), (S, G, 1, 14), (R, W, 3, 14), (R, W, 3, 27),
    (R, W, 3, 9), (R, W, 3, 22), (S, W, 3, 23), (S, W, 3, 17), (S, W, 3, 18), (S, W, 3, 12), (R, G, 1, 11),
    (R, G, 1, 14), (S, W, 3, 41), (S, W, 3, 33), (S, W, 3, 37), (S, W, 3, 29), (S, G, 1, 6), (S, G, 1, 5),
    (LIFT, ((0, 0), (-1, 0), (1, 0)), 0), (R, W, 3, 16), (R, W, 3, 24), (R, W, 3, 11), (R, W, 3, 19), (R, G, 1, 4),
    (S, G, 1, 12), (R, G, 1, 7), (S, G, 1, 17), (S, W, 3, 34), (S, W, 3, 43), (S, W, 3, 30), (S, W, 3, 39),
    (LIFT, ((0, 0), (-1, 0), (1, 0)), 1), (R, W, 3, 26), (R, W, 3, 15), (R, W, 3, 21), (R, W, 3, 10), (R, G, 1, 12),
    (R, W, 3, 32), (R, W, 3, 42), (R, W, 3, 28), (R, W, 3, 38), (R, G, 1, 17), (S, G, 1, 23), (S, G, 1, 25),
    (S, W, 3, 35), (S, W, 3, 40), (S, W, 3, 31), (S, W, 3, 36), (R, G, 1, 22), (S, G, 1, 18), (R, G, 1, 24),
    (S, G, 1, 19), (R, W, 3, 23), (R, W, 3, 17), (R, W, 3, 18), (R, W, 3, 12), (S, W, 3, 45), (S, W, 3, 47),
    (S, W, 3, 44), (S, W, 3, 46), (PRODUCT, 1, ((1, 0), (-1, 0)), 0), (R, G, 1, 18), (R, G, 1, 19),
    (LIFT, ((2, 0),), 0), (R, W, 3, 41), (R, W, 3, 33), (R, W, 3, 37), (R, W, 3, 29), (LIFT, ((2, 0),), 1),
    (R, C, 1, 1, 0, 0), (R, C, 1, 2, 0, 0), (R, G, 1, 6), (S, G, 1, 13), (R, G, 1, 5), (S, G, 1, 16),
    (FREE, 1, 0, 0, 1), (S, X, 1, 0, 0, 3), (FREE, 1, 0, 0, 2), (S, X, 1, 0, 0, 4), (R, W, 3, 34), (R, W, 3, 43),
    (R, W, 3, 30), (R, W, 3, 39), (PRODUCT, 1, ((2, 0),), 0), (R, G, 1, 13), (R, W, 3, 35), (R, W, 3, 40),
    (R, W, 3, 31), (R, W, 3, 36), (R, G, 1, 16), (LIFT, ((0, 1), (-1, 1), (1, 1)), 0), (R, C, 1, 0, 0, 0),
    (R, G, 1, 23), (S, G, 1, 20), (R, G, 1, 25), (S, G, 1, 21), (FAR, 1, 0, 0), (S, X, 1, 0, 0, 0),
    (S, X, 1, 0, 0, 1), (R, W, 3, 45), (R, W, 3, 47), (R, W, 3, 44), (R, W, 3, 46), (PRODUCT, 1, ((2, 0),), 1),
    (PRODUCT, 1, ((1, 0), (-1, 0)), 1), (R, X, 1, 0, 0, 3), (R, X, 1, 0, 0, 4), (R, G, 1, 20),
    (LIFT, ((0, 1), (-1, 1), (1, 1)), 1), (R, G, 1, 21), (R, C, 1, 0, 0, 1), (FAR, 1, 0, 1), (S, X, 1, 0, 1, 0),
    (S, X, 1, 0, 1, 1), (LIFT, ((2, 1),), 0), (R, C, 1, 1, 0, 1), (R, C, 1, 2, 0, 1), (FREE, 1, 0, 1, 1),
    (S, X, 1, 0, 1, 3), (FREE, 1, 0, 1, 2), (S, X, 1, 0, 1, 4), (LIFT, ((2, 1),), 1), (R, X, 1, 0, 0, 0),
    (R, X, 1, 0, 0, 1), (NEAR, 1, 0, 0, 1), (NEAR, 1, 0, 0, 2), (S, X, 1, 0, 0, 2), (S, X, 1, 0, 0, 5),
    (PRODUCT, 1, ((2, 1),), 0), (PRODUCT, 1, ((2, 1),), 1), (PRODUCT, 1, ((1, 1), (-1, 1)), 0), (R, C, 1, 0, 1, 0),
    (FAR, 1, 1, 0), (S, X, 1, 1, 0, 0), (S, X, 1, 1, 0, 1), (PRODUCT, 1, ((1, 1), (-1, 1)), 1), (R, X, 1, 0, 1, 0),
    (R, X, 1, 0, 1, 1), (R, C, 1, 0, 1, 1), (FAR, 1, 1, 1), (S, X, 1, 1, 1, 0), (S, X, 1, 1, 1, 1),
    (NEAR, 1, 0, 1, 1), (NEAR, 1, 0, 1, 2), (PRODUCT, 1, ((0, 0), (0, 1)), 0), (R, C, 1, 1, 1, 0), (R, C, 1, 2, 1, 0),
    (R, X, 1, 0, 1, 3), (R, X, 1, 0, 1, 4), (FREE, 1, 1, 0, 1), (FREE, 1, 1, 0, 2), (S, X, 1, 0, 1, 2),
    (S, X, 1, 0, 1, 5), (PRODUCT, 1, ((0, 0), (0, 1)), 1), (R, C, 1, 1, 1, 1), (R, C, 1, 2, 1, 1), (FREE, 1, 1, 1, 1),
    (FREE, 1, 1, 1, 2), (R, X, 1, 0, 0, 2), (R, X, 1, 0, 0, 5), (R, C, 1, 3, 0, 0), (FINISH, 0, 0),
    (R, C, 1, 3, 1, 0), (S, X, 1, 1, 0, 3), (S, X, 1, 1, 0, 4), (R, C, 1, 3, 0, 1), (R, X, 1, 1, 0, 0),
    (R, X, 1, 1, 0, 1), (NEAR, 1, 1, 0, 1), (NEAR, 1, 1, 0, 2), (R, C, 1, 3, 1, 1), (S, X, 1, 1, 0, 2),
    (S, X, 1, 1, 0, 5), (R, X, 1, 1, 1, 0), (R, X, 1, 1, 1, 1), (NEAR, 1, 1, 1, 1), (NEAR, 1, 1, 1, 2),
    (S, X, 1, 1, 1, 2), (S, X, 1, 1, 1, 5), (R, X, 1, 0, 1, 2), (R, X, 1, 0, 1, 5), (FINISH, 0, 1),
    (S, X, 1, 1, 1, 3), (S, X, 1, 1, 1, 4), (R, X, 1, 1, 0, 3), (R, X, 1, 1, 0, 4), (R, X, 1, 1, 0, 2),
    (R, X, 1, 1, 0, 5), (FINISH, 1, 0), (R, X, 1, 1, 1, 2), (R, X, 1, 1, 1, 5), (R, X, 1, 1, 1, 3),
    (R, X, 1, 1, 1, 4), (FINISH, 1, 1),
)


def way_of(key):
    if key[0] == W:
        return MESSAGES[key[1]][key[2]][3]
    if key[0] == G:
        return GATHER[key[2]][3]
    if key[0] == C:
        return "d"
    return ("x+", "x-", "x+", "x+", "x-", "x-")[key[4]]


def share():
    sent, waited = {}, {}
    for i, (name, *which) in enumerate(SCHEDULE):
        if name == S:
            sent[tuple(which)] = i
        elif name == R:
            waited[tuple(which)] = i
        elif name == PRODUCT:
            g, cases, j = which
            for dx, h in cases:
                sent[(C, g, TURN[dx], h, j)] = i
    back = {"x+": "x-", "x-": "x+", "y+": "y-", "y-": "y+", "z+": "z-", "z-": "z+", "d": "d"}
    last, place = [], {}
    for key in sorted(sent, key=lambda k: (sent[k], k)):
        toward = [k for k in sent if way_of(k) == back[way_of(key)] and waited[k] < sent[key]]
        heard = max([sent[k] for k in toward], default=-1)
        free = [(at, n) for n, at in enumerate(last) if at < heard]
        if free:
            n = max(free)[1]
            last[n] = waited[key]
        else:
            n = len(last)
            last.append(waited[key])
        place[key] = n
    return place, len(last)


SEMAPHORE, SEMAPHORES = share()


def kernel(
    resid, mix_gain, wq, wk, wv, wg, wo, rate, mlp_gain, wu, wd,
    out,
    w_in, w_out, w_up, w_down, xn, rbuf, after, proj, gated, hid, decay, kept,
    dout, din, sout, rin2, rin1,
    local_sem, w_send, g_send, d_send, s_send, recv,
):
    fs, tp = lax.axis_index("fs"), lax.axis_index("tp")
    z, y, x, c = fs // RING, fs % RING, tp // 2, tp % 2

    def turn(v, d):
        return (v + d + RING) % RING

    device = {
        "y+": (z * RING + turn(y, 1), tp),
        "y-": (z * RING + turn(y, -1), tp),
        "z+": (turn(z, 1) * RING + y, tp),
        "z-": (turn(z, -1) * RING + y, tp),
        "x+": (fs, turn(x, 1) * 2 + c),
        "x-": (fs, turn(x, -1) * 2 + c),
        "d": (fs, x * 2 + 1 - c),
    }

    def remote(src, dst, send, recv, way):
        return pltpu.make_async_remote_copy(
            src_ref=src, dst_ref=dst, send_sem=send, recv_sem=recv,
            device_id=device[way], device_id_type=MESH,
        )

    def send(*args):
        remote(*args).start()

    weights = (w_in, w_out, w_up, w_down)

    def block(dy, dz):
        return turn(z, dz) * RING + turn(y, dy)

    def piece(t, dy, dz, part):
        ref = weights[t]
        f = block(dy, dz)
        if part == "full":
            return ref.at[f]
        if part in ("A", "B"):
            return ref.at[f, :, "AB".index(part)]
        if part in ("h0", "h1"):
            return ref.at[f, int(part[1])]
        return ref.at[f, int(part[2]), "AB".index(part[0])]

    def w_copy(t, n, place):
        dy, dz, part, way = place
        ref = piece(t, dy, dz, part)
        return (ref, ref, w_send.at[t], recv.at[SEMAPHORE[W, t, n]], way)

    def g_copy(g, n, dx, core):
        h, q, way = GATHER[n][1:]
        block = turn(x, dx) * 2 + core
        ref = xn.at[g, block, h] if q is None else xn.at[g, block, h, q]
        return (ref, ref, g_send.at[g], recv.at[SEMAPHORE[G, g, n]], way)

    def rows16(count, body):
        def step(i, carry):
            body(pl.ds(pl.multiple_of(i * 16, 16), 16))
            return carry

        lax.fori_loop(0, count // 16, step, 0)

    def of(ref, j, g):
        return ref if g == 0 else ref.at[:, pl.ds(j * 1024, 1024)]

    def d_copy(g, k, h, j):
        columns = slice(None) if g == 0 else pl.ds(j * 1024, 1024)
        return (
            dout.at[g, k, h, :, :, columns], din.at[g, k, h, :, :, columns],
            d_send.at[g], recv.at[SEMAPHORE[C, g, k, h, j]], "d",
        )

    def s_copy(g, h, j, n):
        if n < 2:
            src, dst, way = sout.at[g, 0, h, n], rin2.at[g, h, n], ("x+", "x-")[n]
        elif n < 4:
            src, dst, way = sout.at[g, 1, h, n - 2], rin1.at[g, 0, h, n - 2], "x+"
        else:
            src, dst, way = sout.at[g, 2, h, n - 4], rin1.at[g, 1, h, n - 4], "x-"
        return (of(src, j, g), of(dst, j, g), s_send.at[g], recv.at[SEMAPHORE[X, g, h, j, n]], way)

    def start(kind, *which):
        if kind == W:
            t, n = which
            send(*w_copy(t, n, MESSAGES[t][n]))
        elif kind == G:
            g, n = which
            send(*g_copy(g, n, GATHER[n][0], c))
        else:
            send(*s_copy(*which))

    def receive(kind, *which):
        if kind == W:
            t, n = which
            copy = w_copy(t, n, arrived(MESSAGES[t][n]))
        elif kind == G:
            g, n = which
            dx, way = GATHER[n][0], GATHER[n][3]
            if way == "d":
                copy = g_copy(g, n, dx, 1 - c)
            else:
                copy = g_copy(g, n, near(dx - (1 if way == "x+" else -1)), c)
        elif kind == C:
            copy = d_copy(*which)
        else:
            copy = s_copy(*which)
        remote(*copy).wait_recv()

    def product(g, cases, lhs, w, columns):
        rows = jnp.concatenate([block for case in cases for block in lhs(*case)], axis=0)
        o = jnp.dot(rows, w, preferred_element_type=F32)
        for n, (dx, h) in enumerate(cases):
            mine = o[n * 128 : (n + 1) * 128]
            dout[g, TURN[dx], h, :, :, columns] = mine[:64].astype(BF16).reshape(2, 32, 512)
            kept[TURN[dx], h, :, :, columns] = mine[64:].reshape(2, 32, 512)

    def partial(g, cases, j):
        if g == 0:
            depth = wo.shape[0] * wo.shape[1] * wo.shape[2]

            def step(i, carry):
                w = [w_out[4 * i + n].reshape(depth, 128) for n in range(4)]
                columns = pl.ds(pl.multiple_of(i * 512, 512), 512)
                product(0, cases, gated_rows, jnp.concatenate(w, axis=1), columns)
                return carry

            lax.fori_loop(0, 4, step, 0)
        else:
            depth = wd.shape[0] * wd.shape[1] * wd.shape[2]
            for i in (2 * j, 2 * j + 1):
                w = [w_down[block(*PLACES[4 * i + n])].reshape(depth, 128) for n in range(4)]
                columns = slice(i * 512, (i + 1) * 512)
                product(1, cases, hidden_rows, jnp.concatenate(w, axis=1), columns)
        for dx, h in cases:
            send(*d_copy(g, TURN[dx], h, j))

    def add_quarter(g, k, h, j, q, extra=False):
        columns = slice(None) if g == 0 else slice(j * 1024, (j + 1) * 1024)

        def body(rows):
            total = kept[k, h, q, rows, columns] + din[g, k, h, q, rows, columns].astype(F32)
            if extra:
                total = total + rin2[g, h, q, rows, columns].astype(F32)
            sout[g, k, h, q, rows, columns] = total.astype(BF16)

        rows16(32, body)

    def add_far(g, h, j):
        for q in (0, 1):
            add_quarter(g, 0, h, j, q)

    def add_free(g, h, j, k):
        add_quarter(g, k, h, j, 1 if k == 1 else 0)

    def add_near(g, h, j, k):
        add_quarter(g, k, h, j, 0 if k == 1 else 1, True)

    def sum_rows(h, q, rows):
        total = kept[3, h, q, rows, :] + din[0, 3, h, q, rows, :].astype(F32)
        return total + rin1[0, 0, h, q, rows, :].astype(F32) + rin1[0, 1, h, q, rows, :].astype(F32)

    def normed(values, gain):
        scale = lax.rsqrt(jnp.mean(values * values, axis=-1, keepdims=True) + EPS)
        return (values * scale * gain).astype(BF16)

    loads = []

    def load(src, dst):
        copy = pltpu.make_async_copy(src, dst, local_sem.at[len(loads)])
        copy.start()
        return copy

    for src, low, wide in ((wq, 0, 128), (wk, 128, 128), (wv, 256, 256), (wg, 512, 256)):
        load(src, w_in.at[fs, :, :, :, low : low + wide])
    loads.append(pltpu.make_async_copy(w_in.at[fs], w_in.at[fs], local_sem.at[0]))
    for src, dst in ((resid, rbuf), (wo, w_out.at[fs]), (wu, w_up.at[fs]), (wd, w_down.at[fs])):
        loads.append(load(src, dst))
    barrier = pltpu.get_barrier_semaphore()
    for way in device:
        pl.semaphore_signal(barrier, inc=1, device_id=device[way], device_id_type=MESH)
    for copy in loads[:2]:
        copy.wait()
    for h in (0, 1):
        for q in (0, 1):
            def first_norm(rows):
                xn[0, tp, h, q, rows, :] = normed(rbuf[h, q, rows, :].astype(F32), mix_gain[...])

            rows16(32, first_norm)
    pl.semaphore_wait(barrier, 7)
    r = rate[0]

    def make_decay():
        def some_rows(i, carry):
            rows = pl.ds(pl.multiple_of(i * 64, 64), 64)
            t = lax.broadcasted_iota(jnp.int32, (64, LENGTH), 0) + i * 64
            s = lax.broadcasted_iota(jnp.int32, (64, LENGTH), 1)
            gap = (t - s).astype(F32)
            value = jnp.exp(-r * jnp.maximum(gap, 0.0)) * DK ** (-0.5)
            decay[rows, :] = jnp.where(gap >= 0.0, value, 0.0)
            return carry

        lax.fori_loop(0, LENGTH // 64, some_rows, 0)

    own = x // 2
    sequence = (own, 1 - own)

    def project(seq, j):
        columns = slice(j * 256, (j + 1) * 256)
        lhs = xn[0, pl.ds(4 * seq, 4)].reshape(512, D)
        rhs = w_in[:, :, :, :, columns].reshape(D, 256)
        o = jnp.dot(lhs, rhs, preferred_element_type=F32).astype(BF16)
        proj[pl.ds(4 * seq, 4), :, columns] = o.reshape(4, 128, 256)

    def retain(seq):
        for i in (0, 1):
            mine = pl.ds(seq * 4 + 2 * i, 2)
            upto = pl.ds(seq * 4, 2 * i + 2)
            wide = 256 * (i + 1)
            q = proj[mine, :, 0:128].reshape(256, DK)
            k = proj[upto, :, 128:256].reshape(wide, DK)
            v = proj[upto, :, 256:512].reshape(wide, DV)
            scores = lax.dot_general(q, k, (((1,), (1,)), ((), ())), preferred_element_type=F32)
            scores = (scores * decay[i * 256 : (i + 1) * 256, 0:wide]).astype(BF16)
            mixed = jnp.dot(scores, v, preferred_element_type=F32)
            mixed = mixed - jnp.mean(mixed, axis=-1, keepdims=True)
            spread = jnp.mean(mixed * mixed, axis=-1, keepdims=True)
            gate = proj[mine, :, 512:768].reshape(256, DV).astype(F32)
            value = gate / (1.0 + jnp.exp(-gate)) * (mixed * lax.rsqrt(spread + EPS))
            gated[mine] = value.astype(BF16).reshape(2, 2, 64, DV)

    def gated_rows(dx, h):
        first = turn(x, dx) * 2
        return gated[first + 1 - c, h], gated[first + c, h]

    def lift(cases, half):
        def body(j, carry):
            columns = pl.ds(pl.multiple_of(j * 256, 256), 256)
            lhs = jnp.concatenate(
                [
                    xn[1, turn(x, dx) * 2 + core, h].reshape(64, D)
                    for dx, h in cases
                    for core in (1 - c, c)
                ],
                axis=0,
            )
            rhs = w_up[:, :, :, :, columns].reshape(D, 256)
            o = jnp.maximum(jnp.dot(lhs, rhs, preferred_element_type=F32), 0.0)
            o = (o * o).astype(BF16)
            for n, (dx, h) in enumerate(cases):
                hid[TURN[dx], h, :, columns] = o[n * 128 : (n + 1) * 128]
            return carry

        count = w_up.shape[4] // 512
        lax.fori_loop(half * count, (half + 1) * count, body, 0)

    def hidden_rows(dx, h):
        return (hid[TURN[dx], h],)

    def second_norm(h):
        for q in (0, 1):
            def body(rows):
                value = rbuf[h, q, rows, :].astype(F32) + sum_rows(h, q, rows)
                value = value.astype(BF16)
                after[h, q, rows, :] = value
                xn[1, tp, h, q, rows, :] = normed(value.astype(F32), mlp_gain[...])

            rows16(32, body)

    def finish(h, j):
        for i in range(8 * j, 8 * j + 8):
            here = pl.ds(pl.multiple_of(block(*PLACES[i]) * 128, 128), 128)
            at = slice(i * 128, (i + 1) * 128)
            total = after[h, :, :, here].astype(F32) + kept[3, h, :, :, at]
            total = total + din[1, 3, h, :, :, at].astype(F32)
            total = total + rin1[1, 0, h, :, :, at].astype(F32) + rin1[1, 1, h, :, :, at].astype(F32)
            out[h, :, :, here] = total.astype(BF16)

    actions = {
        S: start,
        R: receive,
        DECAY: make_decay,
        PROJECT: lambda which, j: project(sequence[which], j),
        RETAIN: lambda which: retain(sequence[which]),
        PRODUCT: partial,
        FAR: add_far,
        FREE: add_free,
        NEAR: add_near,
        NORM: second_norm,
        LIFT: lift,
        FINISH: finish,
    }
    for copy in loads[2:]:
        copy.wait()
    for name, *which in SCHEDULE:
        actions[name](*which)
    for t in range(4):
        ref = weights[t].at[0:15]
        remote(ref, ref, w_send.at[t], recv.at[0], "d").wait_send()
    for g in (0, 1):
        remote(xn.at[g, 0:7], xn.at[g, 0:7], g_send.at[g], recv.at[0], "d").wait_send()
        remote(dout.at[g], din.at[g], d_send.at[g], recv.at[0], "d").wait_send()
        remote(sout.at[g], sout.at[g], s_send.at[g], recv.at[0], "d").wait_send()


def on_device(
    resid, mix_gain, w_query, w_key, w_value, w_gate, w_output, decay_rate, mlp_gain, w_up, w_down
):
    def cut(w):
        return w.reshape(2, 2, w.shape[0] // 4, w.shape[1])

    wide = w_query.shape[1] + w_key.shape[1] + w_value.shape[1] + w_gate.shape[1]
    count = RING * RING

    def held(rows, columns):
        return pltpu.VMEM((count, 2, 2, rows // 4, columns), BF16)

    dma = pltpu.SemaphoreType.DMA
    vmem = pl.BlockSpec(memory_space=pltpu.VMEM)
    hbm = pl.BlockSpec(memory_space=pltpu.HBM)
    tokens = (2, 2, 32, D)
    result = pl.pallas_call(
        kernel,
        out_shape=pltpu.VMEM(tokens, BF16),
        in_specs=[
            hbm, vmem, hbm, hbm, hbm, hbm, hbm,
            pl.BlockSpec(memory_space=pltpu.SMEM), vmem, hbm, hbm,
        ],
        out_specs=vmem,
        scratch_shapes=[
            held(128, wide),
            held(w_output.shape[0], 128),
            held(128, w_up.shape[1]),
            held(w_down.shape[0], 128),
            pltpu.VMEM((2, 8) + tokens, BF16),
            pltpu.VMEM(tokens, BF16),
            pltpu.VMEM(tokens, BF16),
            pltpu.VMEM((8, 128, wide), BF16),
            pltpu.VMEM((8, 2, 64, DV), BF16),
            pltpu.VMEM((4, 2, 128, w_up.shape[1]), BF16),
            pltpu.VMEM((LENGTH, LENGTH), F32),
            pltpu.VMEM((4,) + tokens, F32),
            pltpu.VMEM((2, 4) + tokens, BF16),
            pltpu.VMEM((2, 4) + tokens, BF16),
            pltpu.VMEM((2, 3) + tokens, BF16),
            pltpu.VMEM((2,) + tokens, BF16),
            pltpu.VMEM((2, 2) + tokens, BF16),
            dma((5,)),
            dma((4,)),
            dma((2,)),
            dma((2,)),
            dma((2,)),
            dma((SEMAPHORES,)),
        ],
        compiler_params=pltpu.CompilerParams(
            collective_id=0, has_side_effects=True, vmem_limit_bytes=66060288
        ),
    )(
        resid.reshape(tokens), mix_gain[None], cut(w_query), cut(w_key), cut(w_value), cut(w_gate),
        cut(w_output), decay_rate, mlp_gain[None], cut(w_up), cut(w_down),
    )
    return result.reshape(resid.shape)


def solution(mesh):
    placed = (
        P(("fs", "tp"), None),
        P(),
        P("fs", "tp"),
        P("fs", "tp"),
        P("fs", "tp"),
        P("fs", "tp"),
        P("tp", "fs"),
        P("tp"),
        P(),
        P("fs", "tp"),
        P("tp", "fs"),
    )
    return jax.shard_map(
        on_device, mesh=mesh, in_specs=placed, out_specs=P(("fs", "tp"), None), check_vma=False
    )
```

```python
import jax
import jax.numpy as jnp
from jax import lax
from jax.experimental import pallas as pl
from jax.experimental.pallas import tpu as pltpu
from jax.sharding import PartitionSpec as P

D = 2048
DK = 128
DV = 256
LENGTH = 512
RING = 4
EPS = 1e-06
MESH = pl.DeviceIdType.MESH
F32 = jnp.float32
BF16 = jnp.bfloat16

STEP = {"y+": (1, 0), "y-": (-1, 0), "z+": (0, 1), "z-": (0, -1)}


def near(d):
    return {0: 0, 1: 1, 2: 2, 3: -1}[d % RING]


def arrived(message):
    dy, dz, part, way = message
    return near(dy - STEP[way][0]), near(dz - STEP[way][1]), part, way


def onward(message):
    dy, dz, part, way = arrived(message)
    half = "0" if way[1] == "+" else "1"
    along = way[0] == "y"
    across = ("z+", "z-") if along else ("y+", "y-")
    first = "A" if along else "B"
    if part == "full":
        return [(dy, dz, "h" + half, way)] + [(dy, dz, first, w) for w in across]
    if part in ("h0", "h1"):
        onto = [(dy, dz, part, way)] if (dy if along else dz) != 2 and part[1] == half else []
        return onto + [(dy, dz, first + part, w) for w in across]
    if part in ("A", "B"):
        return [(dy, dz, part + "h" + half, way)]
    if (dy if way[0] == "y" else dz) != 2 and part[-1] == half:
        return [(dy, dz, part, way)]
    return []


def plan(parts):
    messages = [(0, 0, part, way) for part in parts for way in ("y+", "y-", "z+", "z-")]
    for message in messages:
        messages += onward(message)
    return messages


MESSAGES = [plan(parts) for parts in (("h0", "h1"), ("full",), ("full",), ("full",))]
PLACES = (
    (0, 0), (1, 0), (-1, 0), (0, 1), (0, -1), (2, 0), (0, 2), (1, 1),
    (1, -1), (-1, 1), (-1, -1), (2, 1), (2, -1), (1, 2), (-1, 2), (2, 2),
)

GATHER = (
    [(0, h, q, w) for h in (0, 1) for q in (0, 1) for w in ("x+", "x-")]
    + [(0, h, None, "d") for h in (0, 1)]
    + [(dx, h, q, "d") for dx in (-1, 1, 2) for h in (0, 1) for q in (0, 1)]
    + [(-1, h, 0, "x+") for h in (0, 1)]
    + [(1, h, 1, "x-") for h in (0, 1)]
)
TURN = {2: 0, 1: 1, -1: 2, 0: 3}

S, R, W, G, C, X = range(6)
DECAY, PROJECT, RETAIN, PRODUCT, FAR, FREE, NEAR, NORM, LIFT, FINISH = range(6, 16)
SCHEDULE = (
    (S, W, 0, 0), (S, W, 1, 1), (S, W, 0, 5), (S, W, 0, 2), (S, W, 1, 3), (S, W, 0, 7), (S, G, 0, 0), (S, G, 0, 3),
    (S, G, 0, 8), (S, G, 0, 9), (DECAY,), (S, W, 1, 0), (S, W, 1, 2), (R, G, 0, 8), (S, W, 0, 4), (S, W, 0, 1),
    (S, W, 0, 6), (S, W, 0, 3), (R, G, 0, 9), (S, G, 0, 2), (S, G, 0, 1), (R, W, 1, 1), (R, W, 1, 3), (S, W, 1, 14),
    (S, W, 1, 7), (S, W, 1, 8), (S, W, 1, 13), (R, W, 0, 0), (R, W, 0, 2), (S, W, 0, 8), (S, W, 1, 15), (S, W, 0, 13),
    (S, W, 1, 9), (R, G, 0, 0), (S, G, 0, 10), (R, G, 0, 3), (S, G, 0, 15), (S, G, 0, 22), (S, G, 0, 24),
    (S, W, 0, 15), (S, W, 0, 10), (R, W, 0, 5), (R, W, 0, 7), (R, W, 1, 0), (R, W, 1, 2), (S, W, 0, 20),
    (S, W, 0, 25), (R, G, 0, 10), (S, W, 1, 4), (S, W, 1, 10), (R, G, 0, 15), (S, W, 1, 11), (S, W, 1, 5),
    (R, W, 0, 4), (R, W, 0, 1), (R, W, 0, 6), (R, W, 0, 3), (R, G, 0, 2), (S, G, 0, 11), (R, G, 0, 1), (S, G, 0, 14),
    (S, G, 0, 4), (S, G, 0, 7), (S, W, 0, 16), (S, W, 0, 11), (S, W, 0, 27), (S, W, 1, 6), (R, W, 1, 14),
    (R, W, 1, 7), (R, W, 1, 8), (R, W, 1, 13), (S, W, 0, 14), (S, W, 0, 9), (S, W, 0, 22), (R, G, 0, 11),
    (R, W, 1, 15), (R, W, 1, 9), (S, W, 1, 12), (R, G, 0, 14), (S, W, 1, 30), (S, W, 0, 24), (S, W, 0, 18),
    (S, W, 1, 21), (R, W, 0, 15), (R, W, 0, 10), (S, W, 0, 26), (S, W, 0, 12), (R, W, 0, 8), (R, W, 0, 13),
    (R, G, 0, 22), (S, G, 0, 18), (R, G, 0, 24), (S, G, 0, 19), (S, G, 0, 6), (S, G, 0, 5), (S, W, 1, 29),
    (S, W, 0, 28), (R, W, 1, 4), (R, W, 1, 10), (S, W, 1, 24), (S, W, 1, 25), (S, W, 0, 19), (S, W, 0, 32),
    (S, W, 0, 33), (R, G, 0, 18), (R, W, 1, 11), (R, W, 1, 5), (S, W, 1, 18), (R, G, 0, 19), (R, W, 0, 20),
    (R, W, 0, 25), (S, W, 1, 16), (S, W, 0, 38), (S, W, 0, 23), (S, W, 0, 42), (S, W, 0, 37), (R, W, 0, 16),
    (R, W, 0, 11), (R, W, 1, 6), (R, G, 0, 4), (S, G, 0, 12), (R, G, 0, 7), (S, G, 0, 17), (R, W, 0, 27),
    (S, G, 0, 23), (S, G, 0, 25), (S, W, 1, 19), (S, W, 0, 35), (S, W, 1, 31), (S, W, 0, 31), (S, W, 1, 23),
    (R, W, 0, 14), (R, W, 0, 9), (R, W, 0, 22), (R, W, 1, 12), (S, W, 1, 27), (S, W, 0, 39), (R, W, 1, 30),
    (R, W, 1, 21), (S, W, 0, 17), (R, G, 0, 12), (S, W, 0, 34), (S, W, 0, 30), (R, G, 0, 17), (R, W, 0, 24),
    (R, W, 0, 18), (S, W, 1, 33), (R, W, 1, 29), (R, W, 0, 26), (R, W, 0, 12), (S, W, 0, 40), (S, W, 0, 29),
    (R, W, 1, 25), (R, W, 1, 24), (S, W, 1, 34), (S, W, 0, 21), (R, W, 0, 28), (R, G, 0, 6), (S, G, 0, 13),
    (R, G, 0, 5), (S, G, 0, 16), (S, W, 1, 28), (R, W, 1, 18), (R, W, 0, 19), (S, W, 0, 41), (S, W, 1, 35),
    (S, W, 0, 36), (R, W, 0, 33), (R, W, 1, 16), (R, W, 0, 32), (S, W, 0, 43), (S, W, 0, 44), (R, G, 0, 13),
    (R, W, 0, 38), (S, W, 0, 45), (S, W, 0, 46), (R, G, 0, 16), (R, W, 0, 42), (R, W, 0, 37), (R, W, 0, 23),
    (R, W, 1, 19), (S, W, 0, 47), (S, W, 1, 32), (R, W, 1, 31), (R, W, 1, 23), (S, W, 1, 22), (R, W, 1, 27),
    (S, W, 1, 26), (S, W, 1, 20), (S, W, 1, 17), (R, W, 0, 31), (R, W, 0, 35), (R, G, 0, 23), (S, G, 0, 20),
    (R, G, 0, 25), (S, G, 0, 21), (S, W, 2, 0), (S, W, 2, 1), (S, W, 2, 2), (S, W, 2, 3), (R, W, 0, 39),
    (R, W, 0, 17), (R, W, 1, 33), (R, W, 0, 30), (R, W, 0, 34), (R, G, 0, 20), (R, W, 1, 34), (R, G, 0, 21),
    (R, W, 0, 40), (R, W, 0, 29), (R, W, 1, 28), (R, W, 1, 35), (R, W, 0, 21), (R, W, 0, 41), (R, W, 0, 36),
    (R, W, 0, 43), (PROJECT, 1, 0), (R, W, 0, 44), (R, W, 1, 32), (R, W, 1, 22), (R, W, 0, 45), (R, W, 0, 46),
    (R, W, 0, 47), (R, W, 1, 20), (R, W, 1, 26), (R, W, 1, 17), (PROJECT, 1, 1), (S, W, 3, 0), (S, W, 3, 1),
    (S, W, 3, 2), (S, W, 3, 3), (RETAIN, 1), (PRODUCT, 0, ((2, 0), (2, 1)), 0), (PRODUCT, 0, ((2, 0), (2, 1)), 1),
    (PROJECT, 0, 0), (R, C, 0, 0, 0, 0), (R, C, 0, 0, 1, 0), (R, C, 0, 0, 0, 1), (R, C, 0, 0, 1, 1), (FAR, 0, 0, 0),
    (S, X, 0, 0, 0, 0), (S, X, 0, 0, 0, 1), (FAR, 0, 1, 0), (FAR, 0, 0, 1), (FAR, 0, 1, 1), (PROJECT, 0, 1),
    (R, W, 2, 1), (R, W, 2, 2), (R, W, 2, 0), (R, W, 2, 3), (S, X, 0, 1, 0, 0), (S, X, 0, 1, 0, 1), (RETAIN, 0),
    (S, W, 2, 4), (S, W, 2, 12), (S, W, 2, 8), (S, W, 2, 13), (PRODUCT, 0, ((1, 0), (-1, 0)), 0), (S, X, 0, 0, 1, 0),
    (S, X, 0, 0, 1, 1), (PRODUCT, 0, ((1, 1), (-1, 1)), 0), (PRODUCT, 0, ((1, 0), (-1, 0)), 1),
    (PRODUCT, 0, ((1, 1), (-1, 1)), 1), (S, X, 0, 1, 1, 0), (S, X, 0, 1, 1, 1), (PRODUCT, 0, ((0, 0), (0, 1)), 0),
    (R, C, 0, 1, 0, 0), (R, X, 0, 0, 0, 0), (R, X, 0, 0, 0, 1), (R, C, 0, 2, 0, 0), (FREE, 0, 0, 0, 1),
    (FREE, 0, 0, 0, 2), (NEAR, 0, 0, 0, 1), (NEAR, 0, 0, 0, 2), (PRODUCT, 0, ((0, 0), (0, 1)), 1), (R, C, 0, 1, 1, 0),
    (R, C, 0, 2, 1, 0), (FREE, 0, 1, 0, 1), (FREE, 0, 1, 0, 2), (R, C, 0, 1, 0, 1), (FREE, 0, 0, 1, 1),
    (R, C, 0, 2, 0, 1), (FREE, 0, 0, 1, 2), (S, W, 2, 14), (S, W, 2, 7), (S, W, 2, 10), (S, W, 2, 6),
    (R, C, 0, 1, 1, 1), (FREE, 0, 1, 1, 1), (R, X, 0, 1, 0, 0), (R, X, 0, 1, 0, 1), (NEAR, 0, 1, 0, 1),
    (S, X, 0, 0, 0, 2), (S, X, 0, 0, 0, 5), (NEAR, 0, 1, 0, 2), (R, C, 0, 2, 1, 1), (FREE, 0, 1, 1, 2),
    (R, C, 0, 3, 0, 0), (R, C, 0, 3, 1, 0), (R, W, 3, 0), (R, W, 3, 1), (R, W, 3, 2), (R, W, 3, 3),
    (R, C, 0, 3, 0, 1), (R, C, 0, 3, 1, 1), (R, X, 0, 0, 1, 0), (R, X, 0, 0, 1, 1), (NEAR, 0, 0, 1, 1),
    (S, X, 0, 0, 1, 2), (S, X, 0, 0, 0, 4), (NEAR, 0, 0, 1, 2), (S, W, 2, 11), (S, W, 2, 15), (S, W, 2, 5),
    (S, W, 2, 9), (R, X, 0, 1, 1, 0), (R, X, 0, 1, 1, 1), (NEAR, 0, 1, 1, 1), (S, X, 0, 0, 0, 3), (S, X, 0, 0, 1, 5),
    (NEAR, 0, 1, 1, 2), (R, W, 2, 4), (R, W, 2, 12), (R, W, 2, 8), (R, W, 2, 13), (R, X, 0, 0, 0, 2),
    (R, X, 0, 0, 0, 5), (S, X, 0, 0, 1, 3), (S, X, 0, 0, 1, 4), (S, W, 2, 28), (S, W, 2, 29), (S, W, 2, 16),
    (S, W, 2, 17), (R, X, 0, 0, 1, 2), (R, X, 0, 0, 0, 4), (S, X, 0, 1, 0, 2), (S, X, 0, 1, 0, 5), (R, W, 2, 14),
    (R, W, 2, 7), (R, W, 2, 10), (R, W, 2, 6), (S, W, 2, 24), (S, W, 2, 25), (S, W, 2, 22), (S, W, 2, 21),
    (R, X, 0, 0, 0, 3), (R, X, 0, 0, 1, 5), (S, X, 0, 1, 1, 2), (S, X, 0, 1, 1, 5), (S, W, 2, 30), (S, W, 2, 27),
    (S, W, 2, 20), (S, W, 2, 19), (R, X, 0, 0, 1, 3), (R, X, 0, 0, 1, 4), (S, X, 0, 1, 0, 3), (S, X, 0, 1, 0, 4),
    (NORM, 0), (S, G, 1, 8), (R, W, 2, 11), (R, W, 2, 15), (R, W, 2, 5), (R, W, 2, 9), (S, W, 2, 26), (S, W, 2, 31),
    (S, W, 2, 18), (S, W, 2, 23), (R, X, 0, 1, 0, 2), (R, X, 0, 1, 0, 5), (S, X, 0, 1, 1, 3), (S, X, 0, 1, 1, 4),
    (R, G, 1, 8), (R, W, 2, 28), (R, W, 2, 29), (R, W, 2, 16), (R, W, 2, 17), (S, W, 3, 4), (S, W, 2, 35),
    (S, W, 2, 32), (S, W, 3, 13), (R, X, 0, 1, 1, 2), (R, X, 0, 1, 1, 5), (S, G, 1, 0), (S, G, 1, 3), (R, W, 2, 24),
    (R, W, 2, 25), (R, W, 2, 22), (R, W, 2, 21), (S, W, 3, 7), (S, W, 3, 10), (R, X, 0, 1, 0, 3), (R, X, 0, 1, 0, 4),
    (R, W, 2, 30), (R, W, 2, 27), (R, W, 2, 20), (R, W, 2, 19), (S, W, 2, 34), (S, W, 2, 33), (R, X, 0, 1, 1, 3),
    (R, X, 0, 1, 1, 4), (S, G, 1, 2), (S, G, 1, 1), (NORM, 1), (S, G, 1, 9), (R, W, 2, 26), (R, W, 2, 31),
    (R, W, 2, 18), (R, W, 2, 23), (S, W, 3, 11), (S, W, 3, 15), (S, W, 3, 8), (S, W, 3, 9), (R, G, 1, 9),
    (R, W, 2, 35), (R, W, 2, 32), (R, G, 1, 0), (S, G, 1, 10), (R, G, 1, 3), (S, G, 1, 15), (S, G, 1, 22),
    (S, G, 1, 24), (R, W, 3, 4), (R, W, 3, 13), (S, W, 3, 14), (S, W, 3, 29), (S, W, 3, 16), (S, W, 3, 6),
    (R, G, 1, 10), (R, G, 1, 15), (R, W, 3, 7), (R, W, 3, 10), (R, W, 2, 34), (R, W, 2, 33), (S, W, 3, 12),
    (S, W, 3, 5), (R, G, 1, 2), (S, G, 1, 11), (R, G, 1, 1), (S, G, 1, 14), (S, G, 1, 4), (S, G, 1, 7), (S, W, 3, 24),
    (S, W, 3, 21), (R, G, 1, 11), (R, G, 1, 14), (S, W, 3, 28), (S, W, 3, 25), (S, W, 3, 20), (S, W, 3, 17),
    (S, G, 1, 6), (S, G, 1, 5), (LIFT, ((0, 0), (-1, 0), (1, 0)), 0), (R, W, 3, 11), (R, W, 3, 15), (R, W, 3, 8),
    (R, W, 3, 9), (R, G, 1, 22), (S, G, 1, 18), (R, G, 1, 24), (S, G, 1, 19), (S, W, 3, 26), (S, W, 3, 31),
    (S, W, 3, 22), (S, W, 3, 23), (LIFT, ((0, 0), (-1, 0), (1, 0)), 1), (R, W, 3, 29), (R, W, 3, 16),
    (PRODUCT, 1, ((1, 0), (-1, 0)), 0), (R, G, 1, 18), (R, G, 1, 19), (S, W, 3, 35), (S, W, 3, 32),
    (LIFT, ((2, 0),), 0), (R, W, 3, 14), (S, W, 3, 30), (R, W, 3, 6), (S, W, 3, 19), (LIFT, ((2, 0),), 1),
    (R, G, 1, 4), (S, G, 1, 23), (S, G, 1, 12), (R, G, 1, 7), (S, G, 1, 25), (S, G, 1, 17), (R, C, 1, 1, 0, 0),
    (FREE, 1, 0, 0, 1), (PRODUCT, 1, ((2, 0),), 0), (R, C, 1, 2, 0, 0), (R, W, 3, 12), (R, W, 3, 5), (R, W, 3, 24),
    (R, W, 3, 21), (S, W, 3, 34), (S, W, 3, 27), (S, W, 3, 18), (S, W, 3, 33), (FREE, 1, 0, 0, 2), (R, G, 1, 12),
    (R, G, 1, 17), (R, W, 3, 28), (R, W, 3, 25), (R, W, 3, 20), (R, W, 3, 17), (R, C, 1, 0, 0, 0), (FAR, 1, 0, 0),
    (R, G, 1, 6), (S, G, 1, 13), (R, G, 1, 5), (S, G, 1, 16), (S, X, 1, 0, 0, 0), (S, X, 1, 0, 0, 1), (R, W, 3, 26),
    (R, W, 3, 31), (R, W, 3, 22), (R, W, 3, 23), (R, G, 1, 13), (R, G, 1, 16), (S, X, 1, 0, 0, 3), (S, X, 1, 0, 0, 4),
    (LIFT, ((0, 1), (-1, 1), (1, 1)), 0), (R, W, 3, 35), (R, W, 3, 32), (R, W, 3, 30), (R, W, 3, 19),
    (LIFT, ((0, 1), (-1, 1), (1, 1)), 1), (R, G, 1, 23), (S, G, 1, 20), (R, G, 1, 25), (S, G, 1, 21), (R, W, 3, 34),
    (R, W, 3, 27), (R, W, 3, 18), (R, W, 3, 33), (PRODUCT, 1, ((2, 0),), 1), (R, X, 1, 0, 0, 0), (R, X, 1, 0, 0, 1),
    (NEAR, 1, 0, 0, 1), (S, X, 1, 0, 0, 2), (NEAR, 1, 0, 0, 2), (S, X, 1, 0, 0, 5),
    (PRODUCT, 1, ((1, 1), (-1, 1)), 0), (PRODUCT, 1, ((1, 0), (-1, 0)), 1), (R, G, 1, 20), (R, G, 1, 21),
    (R, X, 1, 0, 0, 3), (R, X, 1, 0, 0, 4), (R, C, 1, 0, 0, 1), (FAR, 1, 0, 1), (S, X, 1, 0, 1, 0),
    (S, X, 1, 0, 1, 1), (LIFT, ((2, 1),), 0), (R, C, 1, 1, 1, 0), (FREE, 1, 1, 0, 1), (S, X, 1, 1, 0, 3),
    (LIFT, ((2, 1),), 1), (R, C, 1, 2, 1, 0), (R, C, 1, 1, 0, 1), (FREE, 1, 1, 0, 2), (S, X, 1, 1, 0, 4),
    (FREE, 1, 0, 1, 1), (PRODUCT, 1, ((2, 1),), 0), (R, C, 1, 2, 0, 1), (FREE, 1, 0, 1, 2),
    (PRODUCT, 1, ((2, 1),), 1), (R, X, 1, 0, 0, 2), (R, X, 1, 0, 0, 5), (S, X, 1, 0, 1, 3), (S, X, 1, 0, 1, 4),
    (PRODUCT, 1, ((1, 1), (-1, 1)), 1), (PRODUCT, 1, ((0, 0), (0, 1)), 0), (R, C, 1, 0, 1, 0), (R, X, 1, 0, 1, 0),
    (R, X, 1, 0, 1, 1), (R, C, 1, 0, 1, 1), (FAR, 1, 1, 0), (S, X, 1, 1, 0, 0), (S, X, 1, 1, 0, 1), (FAR, 1, 1, 1),
    (NEAR, 1, 0, 1, 1), (NEAR, 1, 0, 1, 2), (PRODUCT, 1, ((0, 0), (0, 1)), 1), (R, C, 1, 1, 1, 1), (R, C, 1, 2, 1, 1),
    (FREE, 1, 1, 1, 1), (FREE, 1, 1, 1, 2), (R, X, 1, 1, 0, 3), (S, X, 1, 1, 1, 0), (R, C, 1, 3, 0, 0),
    (S, X, 1, 1, 1, 1), (FINISH, 0, 0), (R, X, 1, 1, 0, 4), (R, C, 1, 3, 1, 0), (R, C, 1, 3, 0, 1),
    (R, C, 1, 3, 1, 1), (R, X, 1, 0, 1, 3), (S, X, 1, 0, 1, 2), (R, X, 1, 0, 1, 4), (S, X, 1, 0, 1, 5),
    (R, X, 1, 1, 0, 0), (NEAR, 1, 1, 0, 1), (S, X, 1, 1, 0, 2), (R, X, 1, 1, 0, 1), (NEAR, 1, 1, 0, 2),
    (S, X, 1, 1, 0, 5), (R, X, 1, 1, 1, 0), (NEAR, 1, 1, 1, 1), (S, X, 1, 1, 1, 2), (R, X, 1, 1, 1, 1),
    (NEAR, 1, 1, 1, 2), (S, X, 1, 1, 1, 5), (R, X, 1, 0, 1, 2), (S, X, 1, 1, 1, 3), (R, X, 1, 0, 1, 5),
    (S, X, 1, 1, 1, 4), (FINISH, 0, 1), (R, X, 1, 1, 0, 2), (R, X, 1, 1, 0, 5), (FINISH, 1, 0), (R, X, 1, 1, 1, 2),
    (R, X, 1, 1, 1, 5), (R, X, 1, 1, 1, 3), (R, X, 1, 1, 1, 4), (FINISH, 1, 1),
)


def way_of(key):
    if key[0] == W:
        return MESSAGES[key[1]][key[2]][3]
    if key[0] == G:
        return GATHER[key[2]][3]
    if key[0] == C:
        return "d"
    return ("x+", "x-", "x+", "x+", "x-", "x-")[key[4]]


def share():
    sent, waited = {}, {}
    for i, (name, *which) in enumerate(SCHEDULE):
        if name == S:
            sent[tuple(which)] = i
        elif name == R:
            waited[tuple(which)] = i
        elif name == PRODUCT:
            g, cases, j = which
            for dx, h in cases:
                sent[(C, g, TURN[dx], h, j)] = i
    back = {"x+": "x-", "x-": "x+", "y+": "y-", "y-": "y+", "z+": "z-", "z-": "z+", "d": "d"}
    last, place = [], {}
    for key in sorted(sent, key=lambda k: (sent[k], k)):
        toward = [k for k in sent if way_of(k) == back[way_of(key)] and waited[k] < sent[key]]
        heard = max([sent[k] for k in toward], default=-1)
        free = [(at, n) for n, at in enumerate(last) if at < heard]
        if free:
            n = max(free)[1]
            last[n] = waited[key]
        else:
            n = len(last)
            last.append(waited[key])
        place[key] = n
    return place, len(last)


SEMAPHORE, SEMAPHORES = share()


def kernel(
    resid, mix_gain, wq, wk, wv, wg, wo, rate, mlp_gain, wu, wd,
    out,
    w_in, w_out, w_up, w_down, xn, rbuf, after, proj, gated, hid, decay, begun, kept,
    dout, din, sout, rin2, rin1,
    local_sem, w_send, g_send, d_send, s_send, recv,
):
    fs, tp = lax.axis_index("fs"), lax.axis_index("tp")
    z, y, x, c = fs // RING, fs % RING, tp // 2, tp % 2

    def turn(v, d):
        return (v + d + RING) % RING

    device = {
        "y+": (z * RING + turn(y, 1), tp),
        "y-": (z * RING + turn(y, -1), tp),
        "z+": (turn(z, 1) * RING + y, tp),
        "z-": (turn(z, -1) * RING + y, tp),
        "x+": (fs, turn(x, 1) * 2 + c),
        "x-": (fs, turn(x, -1) * 2 + c),
        "d": (fs, x * 2 + 1 - c),
    }

    def remote(src, dst, send, recv, way):
        return pltpu.make_async_remote_copy(
            src_ref=src, dst_ref=dst, send_sem=send, recv_sem=recv,
            device_id=device[way], device_id_type=MESH,
        )

    def send(*args):
        remote(*args).start()

    weights = (w_in, w_out, w_up, w_down)

    def block(dy, dz):
        return turn(z, dz) * RING + turn(y, dy)

    def piece(t, dy, dz, part):
        ref = weights[t]
        f = block(dy, dz)
        if part == "full":
            return ref.at[f]
        if part in ("A", "B"):
            return ref.at[f, :, "AB".index(part)]
        if part in ("h0", "h1"):
            return ref.at[f, int(part[1])]
        return ref.at[f, int(part[2]), "AB".index(part[0])]

    def w_copy(t, n, place):
        dy, dz, part, way = place
        ref = piece(t, dy, dz, part)
        return (ref, ref, w_send.at[t], recv.at[SEMAPHORE[W, t, n]], way)

    def g_copy(g, n, dx, core):
        h, q, way = GATHER[n][1:]
        block = turn(x, dx) * 2 + core
        ref = xn.at[g, block, h] if q is None else xn.at[g, block, h, q]
        return (ref, ref, g_send.at[g], recv.at[SEMAPHORE[G, g, n]], way)

    def rows16(count, body):
        def step(i, carry):
            body(pl.ds(pl.multiple_of(i * 16, 16), 16))
            return carry

        lax.fori_loop(0, count // 16, step, 0)

    def of(ref, j):
        return ref.at[:, pl.ds(j * 1024, 1024)]

    def d_copy(g, k, h, j):
        columns = pl.ds(j * 1024, 1024)
        return (
            dout.at[g, k, h, :, :, columns], din.at[g, k, h, :, :, columns],
            d_send.at[g], recv.at[SEMAPHORE[C, g, k, h, j]], "d",
        )

    def s_copy(g, h, j, n):
        if n < 2:
            src, dst, way = sout.at[g, 0, h, n], rin2.at[g, h, n], ("x+", "x-")[n]
        elif n < 4:
            src, dst, way = sout.at[g, 1, h, n - 2], rin1.at[g, 0, h, n - 2], "x+"
        else:
            src, dst, way = sout.at[g, 2, h, n - 4], rin1.at[g, 1, h, n - 4], "x-"
        return (of(src, j), of(dst, j), s_send.at[g], recv.at[SEMAPHORE[X, g, h, j, n]], way)

    def start(kind, *which):
        if kind == W:
            t, n = which
            send(*w_copy(t, n, MESSAGES[t][n]))
        elif kind == G:
            g, n = which
            send(*g_copy(g, n, GATHER[n][0], c))
        else:
            send(*s_copy(*which))

    def receive(kind, *which):
        if kind == W:
            t, n = which
            copy = w_copy(t, n, arrived(MESSAGES[t][n]))
        elif kind == G:
            g, n = which
            dx, way = GATHER[n][0], GATHER[n][3]
            if way == "d":
                copy = g_copy(g, n, dx, 1 - c)
            else:
                copy = g_copy(g, n, near(dx - (1 if way == "x+" else -1)), c)
        elif kind == C:
            copy = d_copy(*which)
        else:
            copy = s_copy(*which)
        remote(*copy).wait_recv()

    def partial(g, cases, j):
        weight, lhs = ((w_out, gated_rows), (w_down, hidden_rows))[g]
        depth = weight.shape[1] * weight.shape[2] * weight.shape[3]
        for i in (2 * j, 2 * j + 1):
            w = [weight[block(*PLACES[4 * i + n])].reshape(depth, 128) for n in range(4)]
            rows = [some for case in cases for some in lhs(*case)]
            o = jnp.dot(
                jnp.concatenate(rows, axis=0), jnp.concatenate(w, axis=1), preferred_element_type=F32
            )
            columns = slice(i * 512, (i + 1) * 512)
            for n, (dx, h) in enumerate(cases):
                mine = o[n * 128 : (n + 1) * 128]
                dout[g, TURN[dx], h, :, :, columns] = mine[:64].astype(BF16).reshape(2, 32, 512)
                kept[TURN[dx], h, :, :, columns] = mine[64:].reshape(2, 32, 512)
        for dx, h in cases:
            send(*d_copy(g, TURN[dx], h, j))

    def add_quarter(g, k, h, j, q, extra=False):
        columns = slice(j * 1024, (j + 1) * 1024)

        def body(rows):
            total = kept[k, h, q, rows, columns] + din[g, k, h, q, rows, columns].astype(F32)
            if extra:
                total = total + rin2[g, h, q, rows, columns].astype(F32)
            sout[g, k, h, q, rows, columns] = total.astype(BF16)

        rows16(32, body)

    def add_far(g, h, j):
        for q in (0, 1):
            add_quarter(g, 0, h, j, q)

    def add_free(g, h, j, k):
        add_quarter(g, k, h, j, 1 if k == 1 else 0)

    def add_near(g, h, j, k):
        add_quarter(g, k, h, j, 0 if k == 1 else 1, True)

    def add_own(g, h, i, source, target):
        here = pl.ds(pl.multiple_of(block(*PLACES[i]) * 128, 128), 128)
        at = slice(i * 128, (i + 1) * 128)
        total = source[h, :, :, here].astype(F32) + kept[3, h, :, :, at]
        total = total + din[g, 3, h, :, :, at].astype(F32)
        total = total + rin1[g, 0, h, :, :, at].astype(F32) + rin1[g, 1, h, :, :, at].astype(F32)
        target[h, :, :, here] = total.astype(BF16)

    def normed(values, gain):
        scale = lax.rsqrt(jnp.mean(values * values, axis=-1, keepdims=True) + EPS)
        return (values * scale * gain).astype(BF16)

    loads = []

    def load(src, dst):
        copy = pltpu.make_async_copy(src, dst, local_sem.at[len(loads)])
        copy.start()
        return copy

    for src, low, wide in ((wq, 0, 128), (wk, 128, 128), (wv, 256, 256), (wg, 512, 256)):
        load(src, w_in.at[fs, :, :, :, low : low + wide])
    loads.append(pltpu.make_async_copy(w_in.at[fs], w_in.at[fs], local_sem.at[0]))
    for src, dst in ((resid, rbuf), (wo, w_out.at[fs]), (wu, w_up.at[fs]), (wd, w_down.at[fs])):
        loads.append(load(src, dst))
    barrier = pltpu.get_barrier_semaphore()
    for way in device:
        pl.semaphore_signal(barrier, inc=1, device_id=device[way], device_id_type=MESH)
    for copy in loads[:2]:
        copy.wait()
    for h in (0, 1):
        for q in (0, 1):
            def first_norm(rows):
                xn[0, tp, h, q, rows, :] = normed(rbuf[h, q, rows, :].astype(F32), mix_gain[...])

            rows16(32, first_norm)
    pl.semaphore_wait(barrier, 7)
    r = rate[0]

    def make_decay():
        def some_rows(i, carry):
            rows = pl.ds(pl.multiple_of(i * 64, 64), 64)
            t = lax.broadcasted_iota(jnp.int32, (64, LENGTH), 0) + i * 64
            s = lax.broadcasted_iota(jnp.int32, (64, LENGTH), 1)
            gap = (t - s).astype(F32)
            value = jnp.exp(-r * jnp.maximum(gap, 0.0)) * DK ** (-0.5)
            decay[rows, :] = jnp.where(gap >= 0.0, value, 0.0)
            return carry

        lax.fori_loop(0, LENGTH // 64, some_rows, 0)

    own = x // 2
    sequence = (own, 1 - own)

    def project(which, seq, part):
        blocks = [block(*place) for place in (PLACES[:12], PLACES[12:])[part]]

        def body(j, carry):
            columns = pl.ds(pl.multiple_of(j * 256, 256), 256)
            lhs = [
                xn[0, pl.ds(4 * seq, 4), :, :, :, pl.ds(pl.multiple_of(f * 128, 128), 128)].reshape(512, 128)
                for f in blocks
            ]
            rhs = [w_in[f, :, :, :, columns].reshape(128, 256) for f in blocks]
            o = jnp.dot(
                jnp.concatenate(lhs, axis=1), jnp.concatenate(rhs, axis=0), preferred_element_type=F32
            )
            if part == 0:
                begun[which, j] = o
            else:
                o = (begun[which, j] + o).astype(BF16)
                proj[pl.ds(4 * seq, 4), :, columns] = o.reshape(4, 128, 256)
            return carry

        lax.fori_loop(0, 3, body, 0)

    def retain(seq):
        for i in (0, 1):
            mine = pl.ds(seq * 4 + 2 * i, 2)
            upto = pl.ds(seq * 4, 2 * i + 2)
            wide = 256 * (i + 1)
            q = proj[mine, :, 0:128].reshape(256, DK)
            k = proj[upto, :, 128:256].reshape(wide, DK)
            v = proj[upto, :, 256:512].reshape(wide, DV)
            scores = lax.dot_general(q, k, (((1,), (1,)), ((), ())), preferred_element_type=F32)
            scores = (scores * decay[i * 256 : (i + 1) * 256, 0:wide]).astype(BF16)
            mixed = jnp.dot(scores, v, preferred_element_type=F32)
            mixed = mixed - jnp.mean(mixed, axis=-1, keepdims=True)
            spread = jnp.mean(mixed * mixed, axis=-1, keepdims=True)
            gate = proj[mine, :, 512:768].reshape(256, DV).astype(F32)
            value = gate / (1.0 + jnp.exp(-gate)) * (mixed * lax.rsqrt(spread + EPS))
            gated[mine] = value.astype(BF16).reshape(2, 2, 64, DV)

    def gated_rows(dx, h):
        first = turn(x, dx) * 2
        return gated[first + 1 - c, h], gated[first + c, h]

    def lift(cases, part):
        def body(j, carry):
            columns = pl.ds(pl.multiple_of(j * 256, 256), 256)
            lhs = jnp.concatenate(
                [
                    xn[1, turn(x, dx) * 2 + core, h].reshape(64, D)
                    for dx, h in cases
                    for core in (1 - c, c)
                ],
                axis=0,
            )
            rhs = w_up[:, :, :, :, columns].reshape(D, 256)
            o = jnp.maximum(jnp.dot(lhs, rhs, preferred_element_type=F32), 0.0)
            o = (o * o).astype(BF16)
            for n, (dx, h) in enumerate(cases):
                hid[TURN[dx], h, :, columns] = o[n * 128 : (n + 1) * 128]
            return carry

        count = w_up.shape[4] // 512
        lax.fori_loop(part * count, (part + 1) * count, body, 0)

    def hidden_rows(dx, h):
        return (hid[TURN[dx], h],)

    def second_norm(h):
        for i in range(16):
            add_own(0, h, i, rbuf, after)
        for q in (0, 1):
            def body(rows):
                xn[1, tp, h, q, rows, :] = normed(after[h, q, rows, :].astype(F32), mlp_gain[...])

            rows16(32, body)

    def finish(h, j):
        for i in range(8 * j, 8 * j + 8):
            add_own(1, h, i, after, out)

    actions = {
        S: start,
        R: receive,
        DECAY: make_decay,
        PROJECT: lambda which, part: project(which, sequence[which], part),
        RETAIN: lambda which: retain(sequence[which]),
        PRODUCT: partial,
        FAR: add_far,
        FREE: add_free,
        NEAR: add_near,
        NORM: second_norm,
        LIFT: lift,
        FINISH: finish,
    }
    for copy in loads[2:]:
        copy.wait()
    for name, *which in SCHEDULE:
        actions[name](*which)
    for t in range(4):
        ref = weights[t].at[0:15]
        remote(ref, ref, w_send.at[t], recv.at[0], "d").wait_send()
    for g in (0, 1):
        remote(xn.at[g, 0:7], xn.at[g, 0:7], g_send.at[g], recv.at[0], "d").wait_send()
        remote(dout.at[g], din.at[g], d_send.at[g], recv.at[0], "d").wait_send()
        remote(sout.at[g], sout.at[g], s_send.at[g], recv.at[0], "d").wait_send()


def on_device(
    resid, mix_gain, w_query, w_key, w_value, w_gate, w_output, decay_rate, mlp_gain, w_up, w_down
):
    def cut(w):
        return w.reshape(2, 2, w.shape[0] // 4, w.shape[1])

    wide = w_query.shape[1] + w_key.shape[1] + w_value.shape[1] + w_gate.shape[1]
    count = RING * RING

    def held(rows, columns):
        return pltpu.VMEM((count, 2, 2, rows // 4, columns), BF16)

    dma = pltpu.SemaphoreType.DMA
    vmem = pl.BlockSpec(memory_space=pltpu.VMEM)
    hbm = pl.BlockSpec(memory_space=pltpu.HBM)
    tokens = (2, 2, 32, D)
    result = pl.pallas_call(
        kernel,
        out_shape=pltpu.VMEM(tokens, BF16),
        in_specs=[
            hbm, vmem, hbm, hbm, hbm, hbm, hbm,
            pl.BlockSpec(memory_space=pltpu.SMEM), vmem, hbm, hbm,
        ],
        out_specs=vmem,
        scratch_shapes=[
            held(128, wide),
            held(w_output.shape[0], 128),
            held(128, w_up.shape[1]),
            held(w_down.shape[0], 128),
            pltpu.VMEM((2, 8) + tokens, BF16),
            pltpu.VMEM(tokens, BF16),
            pltpu.VMEM(tokens, BF16),
            pltpu.VMEM((8, 128, wide), BF16),
            pltpu.VMEM((8, 2, 64, DV), BF16),
            pltpu.VMEM((4, 2, 128, w_up.shape[1]), BF16),
            pltpu.VMEM((LENGTH, LENGTH), F32),
            pltpu.VMEM((2, wide // 256, LENGTH, 256), F32),
            pltpu.VMEM((4,) + tokens, F32),
            pltpu.VMEM((2, 4) + tokens, BF16),
            pltpu.VMEM((2, 4) + tokens, BF16),
            pltpu.VMEM((2, 3) + tokens, BF16),
            pltpu.VMEM((2,) + tokens, BF16),
            pltpu.VMEM((2, 2) + tokens, BF16),
            dma((5,)),
            dma((4,)),
            dma((2,)),
            dma((2,)),
            dma((2,)),
            dma((SEMAPHORES,)),
        ],
        compiler_params=pltpu.CompilerParams(
            collective_id=0, has_side_effects=True, vmem_limit_bytes=66060288
        ),
    )(
        resid.reshape(tokens), mix_gain[None], cut(w_query), cut(w_key), cut(w_value), cut(w_gate),
        cut(w_output), decay_rate, mlp_gain[None], cut(w_up), cut(w_down),
    )
    return result.reshape(resid.shape)


def solution(mesh):
    placed = (
        P(("fs", "tp"), None),
        P(),
        P("fs", "tp"),
        P("fs", "tp"),
        P("fs", "tp"),
        P("fs", "tp"),
        P("tp", "fs"),
        P("tp"),
        P(),
        P("fs", "tp"),
        P("tp", "fs"),
    )
    return jax.shard_map(
        on_device, mesh=mesh, in_specs=placed, out_specs=P(("fs", "tp"), None), check_vma=False
    )
```

```python
import jax
import jax.numpy as jnp
from jax import lax
from jax.experimental import pallas as pl
from jax.experimental.pallas import tpu as pltpu
from jax.sharding import PartitionSpec as P

D = 2048
DK = 128
DV = 256
LENGTH = 512
RING = 4
EPS = 1e-06
MESH = pl.DeviceIdType.MESH
F32 = jnp.float32
BF16 = jnp.bfloat16

STEP = {"y+": (1, 0), "y-": (-1, 0), "z+": (0, 1), "z-": (0, -1)}


def near(d):
    return {0: 0, 1: 1, 2: 2, 3: -1}[d % RING]


def arrived(message):
    dy, dz, part, way = message
    return near(dy - STEP[way][0]), near(dz - STEP[way][1]), part, way


def onward(message):
    dy, dz, part, way = arrived(message)
    half = "0" if way[1] == "+" else "1"
    along = way[0] == "y"
    across = ("z+", "z-") if along else ("y+", "y-")
    first = "A" if along else "B"
    if part == "full":
        return [(dy, dz, "h" + half, way)] + [(dy, dz, first, w) for w in across]
    if part in ("h0", "h1"):
        onto = [(dy, dz, part, way)] if (dy if along else dz) != 2 and part[1] == half else []
        return onto + [(dy, dz, first + part, w) for w in across]
    if part in ("A", "B"):
        return [(dy, dz, part + "h" + half, way)]
    if (dy if way[0] == "y" else dz) != 2 and part[-1] == half:
        return [(dy, dz, part, way)]
    return []


def plan(parts):
    messages = [(0, 0, part, way) for part in parts for way in ("y+", "y-", "z+", "z-")]
    for message in messages:
        messages += onward(message)
    return messages


MESSAGES = [plan(parts) for parts in (("h0", "h1"), ("full",), ("h0", "h1"), ("full",))]
PLACES = (
    (0, 0), (1, 0), (-1, 0), (0, 1), (0, -1), (2, 0), (0, 2), (1, 1),
    (1, -1), (-1, 1), (-1, -1), (2, 1), (2, -1), (1, 2), (-1, 2), (2, 2),
)

GATHER = (
    [(0, h, q, w) for h in (0, 1) for q in (0, 1) for w in ("x+", "x-")]
    + [(0, h, None, "d") for h in (0, 1)]
    + [(dx, h, q, "d") for dx in (-1, 1, 2) for h in (0, 1) for q in (0, 1)]
    + [(-1, h, 0, "x+") for h in (0, 1)]
    + [(1, h, 1, "x-") for h in (0, 1)]
)
TURN = {2: 0, 1: 1, -1: 2, 0: 3}

S, R, W, G, C, X = range(6)
DECAY, PROJECT, RETAIN, PRODUCT, FAR, FREE, NEAR, NORM, LIFT, FINISH = range(6, 16)
SCHEDULE = (
    (S, W, 0, 0), (S, W, 0, 5), (S, W, 0, 2), (S, W, 0, 7), (S, G, 0, 0), (S, G, 0, 3), (S, G, 0, 8), (S, G, 0, 9),
    (DECAY,), (S, W, 0, 4), (S, W, 0, 1), (S, W, 0, 6), (S, W, 0, 3), (R, G, 0, 8), (R, G, 0, 9), (S, G, 0, 2),
    (S, G, 0, 1), (S, W, 1, 0), (S, W, 1, 1), (S, W, 1, 2), (S, W, 1, 3), (R, W, 0, 0), (R, W, 0, 5), (R, W, 0, 2),
    (R, W, 0, 7), (S, W, 0, 8), (S, W, 0, 20), (S, W, 0, 13), (S, W, 0, 25), (S, G, 0, 4), (S, G, 0, 7), (R, G, 0, 0),
    (S, G, 0, 10), (R, G, 0, 3), (S, G, 0, 15), (R, G, 0, 10), (R, W, 0, 4), (R, W, 0, 1), (R, W, 0, 6), (R, W, 0, 3),
    (S, W, 0, 16), (S, W, 0, 24), (S, W, 0, 11), (S, W, 0, 22), (R, G, 0, 15), (S, G, 0, 22), (S, G, 0, 24),
    (S, W, 0, 14), (S, W, 0, 27), (S, W, 0, 9), (S, W, 0, 19), (R, G, 0, 2), (S, G, 0, 11), (R, G, 0, 1),
    (S, G, 0, 14), (R, W, 1, 0), (R, W, 1, 1), (R, W, 1, 2), (R, W, 1, 3), (S, W, 0, 26), (S, W, 0, 15),
    (S, W, 0, 21), (S, W, 0, 12), (R, G, 0, 11), (R, G, 0, 14), (S, W, 0, 23), (S, W, 0, 17), (S, W, 0, 18),
    (S, W, 0, 10), (R, W, 0, 8), (R, W, 0, 20), (R, W, 0, 13), (R, W, 0, 25), (S, G, 0, 6), (S, G, 0, 5),
    (R, G, 0, 4), (S, G, 0, 12), (R, G, 0, 7), (S, G, 0, 17), (S, W, 0, 32), (S, W, 0, 42), (S, W, 0, 28),
    (S, W, 0, 38), (R, W, 0, 16), (R, W, 0, 24), (R, W, 0, 11), (R, W, 0, 22), (S, W, 0, 41), (S, W, 0, 33),
    (S, W, 0, 31), (S, W, 0, 39), (R, G, 0, 12), (R, W, 0, 14), (R, W, 0, 27), (R, W, 0, 9), (R, W, 0, 19),
    (R, G, 0, 17), (S, W, 0, 35), (S, W, 0, 40), (S, W, 0, 37), (S, W, 0, 29), (R, W, 0, 26), (R, W, 0, 15),
    (R, W, 0, 21), (R, W, 0, 12), (S, G, 0, 23), (S, G, 0, 25), (R, G, 0, 22), (S, G, 0, 18), (R, G, 0, 24),
    (S, G, 0, 19), (S, W, 0, 34), (S, W, 0, 43), (S, W, 0, 30), (S, W, 0, 36), (R, W, 0, 23), (R, W, 0, 17),
    (R, W, 0, 18), (R, W, 0, 10), (R, G, 0, 18), (S, W, 1, 4), (S, W, 1, 7), (S, W, 1, 10), (S, W, 1, 13),
    (R, G, 0, 19), (R, W, 0, 32), (R, W, 0, 42), (R, W, 0, 28), (R, W, 0, 38), (S, W, 0, 45), (S, W, 0, 47),
    (S, W, 0, 44), (S, W, 0, 46), (R, W, 0, 41), (R, W, 0, 33), (R, W, 0, 31), (R, W, 0, 39), (R, G, 0, 6),
    (S, G, 0, 13), (R, G, 0, 5), (S, G, 0, 16), (S, W, 1, 14), (S, W, 1, 12), (S, W, 1, 8), (S, W, 1, 6),
    (R, W, 0, 35), (R, W, 0, 40), (R, W, 0, 37), (R, W, 0, 29), (S, W, 1, 11), (S, W, 1, 15), (S, W, 1, 5),
    (S, W, 1, 9), (R, G, 0, 13), (R, G, 0, 16), (S, W, 2, 0), (S, W, 2, 5), (S, W, 2, 2), (S, W, 2, 7), (R, W, 0, 34),
    (R, W, 0, 43), (R, W, 0, 30), (R, W, 0, 36), (PROJECT, 1, 0), (R, W, 1, 4), (R, W, 1, 7), (R, W, 1, 10),
    (R, W, 1, 13), (R, G, 0, 23), (S, G, 0, 20), (R, G, 0, 25), (S, G, 0, 21), (S, W, 1, 24), (S, W, 1, 29),
    (S, W, 1, 16), (S, W, 1, 21), (PROJECT, 0, 0), (R, W, 0, 45), (R, W, 0, 47), (R, W, 0, 44), (R, W, 0, 46),
    (R, G, 0, 20), (R, W, 1, 14), (R, W, 1, 12), (R, W, 1, 8), (R, W, 1, 6), (R, G, 0, 21), (S, W, 1, 28),
    (S, W, 1, 30), (S, W, 2, 4), (S, W, 1, 25), (S, W, 1, 27), (S, W, 2, 1), (S, W, 1, 22), (S, W, 1, 20),
    (S, W, 2, 6), (S, W, 1, 17), (S, W, 1, 19), (S, W, 2, 3), (PROJECT, 2, 0), (R, W, 1, 11), (R, W, 1, 15),
    (R, W, 1, 5), (R, W, 1, 9), (PROJECT, 1, 1), (RETAIN, 1), (PRODUCT, 0, ((2, 0), (2, 1)), 0), (S, W, 1, 26),
    (S, W, 1, 31), (S, W, 1, 18), (S, W, 1, 23), (PROJECT, 0, 1), (R, W, 2, 0), (R, W, 2, 5), (R, W, 2, 2),
    (R, W, 2, 7), (R, W, 1, 24), (R, W, 1, 29), (R, W, 1, 16), (R, W, 1, 21), (R, W, 1, 28), (R, W, 1, 25),
    (R, W, 1, 22), (R, W, 1, 17), (S, W, 1, 34), (S, W, 2, 8), (S, W, 1, 35), (S, W, 2, 20), (S, W, 1, 32),
    (S, W, 2, 13), (S, W, 1, 33), (S, W, 2, 25), (RETAIN, 0), (R, W, 1, 30), (R, W, 1, 27), (R, W, 1, 20),
    (R, W, 1, 19), (R, C, 0, 0, 0, 0), (R, C, 0, 0, 1, 0), (FAR, 0, 0, 0), (S, X, 0, 0, 0, 0), (S, X, 0, 0, 0, 1),
    (FAR, 0, 1, 0), (PRODUCT, 0, ((1, 0), (-1, 0)), 0), (PRODUCT, 0, ((1, 1), (-1, 1)), 0), (S, X, 0, 1, 0, 0),
    (S, X, 0, 1, 0, 1), (PRODUCT, 0, ((0, 0), (0, 1)), 0), (R, C, 0, 1, 0, 0), (FREE, 0, 0, 0, 1), (R, C, 0, 2, 0, 0),
    (FREE, 0, 0, 0, 2), (R, C, 0, 1, 1, 0), (FREE, 0, 1, 0, 1), (R, W, 2, 4), (R, W, 2, 1), (R, W, 2, 6),
    (R, W, 2, 3), (S, W, 2, 16), (S, W, 2, 27), (S, W, 3, 2), (S, W, 2, 19), (S, X, 0, 0, 0, 3), (S, X, 0, 0, 0, 4),
    (R, C, 0, 2, 1, 0), (FREE, 0, 1, 0, 2), (R, W, 1, 26), (R, W, 1, 31), (R, W, 1, 18), (R, W, 1, 23),
    (R, C, 0, 3, 0, 0), (R, W, 1, 34), (R, W, 1, 35), (R, W, 1, 32), (R, W, 1, 33), (PRODUCT, 0, ((2, 0), (2, 1)), 1),
    (R, C, 0, 3, 1, 0), (PRODUCT, 0, ((1, 0), (-1, 0)), 1), (S, W, 3, 0), (S, W, 2, 24), (S, W, 2, 22),
    (S, X, 0, 1, 0, 3), (S, X, 0, 1, 0, 4), (PRODUCT, 0, ((1, 1), (-1, 1)), 1), (PRODUCT, 0, ((0, 0), (0, 1)), 1),
    (R, X, 0, 0, 0, 0), (R, X, 0, 0, 0, 1), (NEAR, 0, 0, 0, 1), (NEAR, 0, 0, 0, 2), (R, C, 0, 0, 0, 1),
    (FAR, 0, 0, 1), (R, C, 0, 0, 1, 1), (FAR, 0, 1, 1), (S, W, 3, 1), (S, W, 3, 3), (R, C, 0, 1, 0, 1),
    (S, X, 0, 0, 1, 0), (S, X, 0, 0, 1, 1), (FREE, 0, 0, 1, 1), (R, C, 0, 2, 0, 1), (FREE, 0, 0, 1, 2),
    (R, X, 0, 1, 0, 0), (R, X, 0, 1, 0, 1), (NEAR, 0, 1, 0, 1), (NEAR, 0, 1, 0, 2), (R, C, 0, 1, 1, 1),
    (FREE, 0, 1, 1, 1), (R, W, 2, 8), (R, W, 2, 20), (R, W, 2, 13), (R, W, 2, 25), (R, C, 0, 2, 1, 1),
    (FREE, 0, 1, 1, 2), (R, C, 0, 3, 0, 1), (R, C, 0, 3, 1, 1), (S, X, 0, 1, 1, 0), (S, X, 0, 1, 1, 1),
    (R, X, 0, 0, 0, 3), (R, X, 0, 0, 0, 4), (R, W, 2, 16), (R, W, 2, 27), (R, W, 2, 19), (S, W, 2, 9),
    (S, X, 0, 0, 0, 2), (S, X, 0, 0, 0, 5), (R, X, 0, 1, 0, 3), (R, X, 0, 1, 0, 4), (R, W, 2, 24), (R, W, 2, 22),
    (S, W, 2, 32), (S, W, 2, 28), (S, X, 0, 0, 1, 3), (S, X, 0, 0, 1, 4), (R, X, 0, 0, 1, 0), (R, X, 0, 0, 1, 1),
    (NEAR, 0, 0, 1, 1), (NEAR, 0, 0, 1, 2), (S, W, 2, 14), (S, W, 2, 42), (S, W, 2, 11), (S, W, 2, 38),
    (S, X, 0, 0, 1, 2), (S, X, 0, 0, 1, 5), (R, X, 0, 1, 1, 0), (R, X, 0, 1, 1, 1), (NEAR, 0, 1, 1, 1),
    (NEAR, 0, 1, 1, 2), (R, W, 3, 2), (S, W, 2, 35), (S, W, 2, 15), (S, W, 2, 21), (S, W, 2, 29), (S, X, 0, 1, 0, 2),
    (S, X, 0, 1, 0, 5), (R, X, 0, 0, 0, 2), (R, X, 0, 0, 0, 5), (R, W, 3, 0), (R, W, 2, 9), (S, W, 2, 41),
    (S, W, 2, 43), (S, W, 2, 18), (S, W, 2, 10), (S, X, 0, 1, 1, 2), (S, X, 0, 1, 1, 5), (R, X, 0, 0, 1, 3),
    (R, X, 0, 0, 1, 4), (R, W, 2, 32), (R, W, 3, 1), (R, W, 3, 3), (R, W, 2, 28), (S, W, 3, 4), (S, W, 3, 7),
    (S, W, 2, 37), (S, W, 3, 13), (S, X, 0, 1, 1, 3), (S, X, 0, 1, 1, 4), (R, X, 0, 0, 1, 2), (R, X, 0, 0, 1, 5),
    (NORM, 0), (S, G, 1, 8), (R, W, 2, 14), (R, W, 2, 42), (R, W, 2, 11), (R, W, 2, 38), (S, W, 2, 31), (S, G, 1, 0),
    (S, G, 1, 3), (R, X, 0, 1, 0, 2), (R, X, 0, 1, 0, 5), (R, W, 2, 35), (R, W, 2, 15), (R, W, 2, 21), (R, W, 2, 29),
    (R, G, 1, 8), (S, W, 2, 34), (S, W, 2, 47), (S, W, 3, 10), (S, W, 2, 46), (R, X, 0, 1, 1, 2), (R, X, 0, 1, 1, 5),
    (R, W, 2, 41), (R, W, 2, 43), (R, W, 2, 18), (R, W, 2, 10), (S, W, 2, 45), (S, W, 2, 40), (S, W, 2, 36),
    (S, G, 1, 2), (S, G, 1, 1), (R, X, 0, 1, 1, 3), (R, X, 0, 1, 1, 4), (NORM, 1), (S, G, 1, 9), (R, W, 2, 37),
    (S, W, 2, 23), (S, W, 2, 33), (S, W, 2, 30), (S, W, 2, 39), (R, W, 3, 4), (R, W, 2, 31), (R, W, 3, 7),
    (R, W, 3, 13), (R, G, 1, 9), (S, W, 2, 26), (S, W, 2, 17), (S, W, 2, 44), (S, W, 2, 12), (S, G, 1, 4),
    (S, G, 1, 7), (R, G, 1, 0), (S, G, 1, 10), (R, G, 1, 3), (S, G, 1, 15), (R, W, 2, 34), (R, W, 2, 47),
    (R, W, 2, 46), (S, W, 3, 11), (S, W, 3, 15), (S, W, 3, 16), (S, W, 3, 9), (R, G, 1, 10), (R, G, 1, 15),
    (R, W, 2, 45), (R, W, 3, 10), (R, W, 2, 40), (R, W, 2, 36), (S, W, 3, 5), (S, G, 1, 22), (S, G, 1, 24),
    (R, G, 1, 2), (S, G, 1, 11), (R, G, 1, 1), (S, G, 1, 14), (R, W, 2, 23), (R, W, 2, 33), (R, W, 2, 30),
    (R, W, 2, 39), (S, W, 3, 24), (S, W, 3, 29), (S, W, 3, 21), (R, G, 1, 11), (R, G, 1, 14), (R, W, 2, 26),
    (R, W, 2, 17), (R, W, 2, 44), (R, W, 2, 12), (S, W, 3, 14), (S, W, 3, 12), (S, W, 3, 8), (S, W, 3, 6),
    (S, G, 1, 6), (S, G, 1, 5), (LIFT, ((0, 0), (-1, 0), (1, 0)), 0), (R, G, 1, 4), (S, G, 1, 12), (R, G, 1, 7),
    (S, G, 1, 17), (LIFT, ((0, 0), (-1, 0), (1, 0)), 1), (R, W, 3, 16), (R, G, 1, 12), (R, W, 3, 11), (R, W, 3, 15),
    (R, W, 3, 9), (PRODUCT, 1, ((1, 0), (-1, 0)), 0), (R, G, 1, 17), (S, W, 3, 26), (S, W, 3, 31), (S, W, 3, 32),
    (S, W, 3, 17), (S, G, 1, 23), (S, G, 1, 25), (R, G, 1, 22), (S, G, 1, 18), (R, G, 1, 24), (S, G, 1, 19),
    (R, W, 3, 24), (R, W, 3, 5), (R, W, 3, 29), (R, W, 3, 21), (R, C, 1, 1, 0, 0), (FREE, 1, 0, 0, 1), (S, W, 3, 34),
    (S, W, 3, 25), (S, W, 3, 18), (S, W, 3, 23), (R, C, 1, 2, 0, 0), (FREE, 1, 0, 0, 2), (R, G, 1, 18), (R, G, 1, 19),
    (LIFT, ((2, 0),), 0), (S, W, 3, 28), (S, W, 3, 35), (S, W, 3, 20), (S, W, 3, 33), (S, X, 1, 0, 0, 3),
    (S, X, 1, 0, 0, 4), (LIFT, ((2, 0),), 1), (R, G, 1, 6), (S, G, 1, 13), (R, G, 1, 5), (S, G, 1, 16), (R, W, 3, 14),
    (R, W, 3, 12), (R, W, 3, 8), (R, W, 3, 6), (PRODUCT, 1, ((2, 0),), 0), (S, W, 3, 30), (S, W, 3, 27),
    (S, W, 3, 22), (S, W, 3, 19), (R, G, 1, 13), (R, W, 3, 26), (R, W, 3, 31), (R, W, 3, 32), (R, W, 3, 17),
    (R, G, 1, 16), (LIFT, ((0, 1), (-1, 1), (1, 1)), 0), (R, C, 1, 0, 0, 0), (R, G, 1, 23), (S, G, 1, 20),
    (R, G, 1, 25), (S, G, 1, 21), (R, W, 3, 34), (R, W, 3, 25), (R, W, 3, 18), (R, W, 3, 23), (FAR, 1, 0, 0),
    (S, X, 1, 0, 0, 0), (S, X, 1, 0, 0, 1), (LIFT, ((0, 1), (-1, 1), (1, 1)), 1), (R, X, 1, 0, 0, 3),
    (R, X, 1, 0, 0, 4), (PRODUCT, 1, ((1, 1), (-1, 1)), 0), (R, G, 1, 20), (R, W, 3, 28), (R, W, 3, 35),
    (R, W, 3, 20), (R, W, 3, 33), (R, G, 1, 21), (LIFT, ((2, 1),), 0), (LIFT, ((2, 1),), 1), (R, W, 3, 30),
    (R, W, 3, 27), (R, W, 3, 22), (R, W, 3, 19), (R, C, 1, 1, 1, 0), (FREE, 1, 1, 0, 1), (S, X, 1, 1, 0, 3),
    (PRODUCT, 1, ((2, 1),), 0), (R, C, 1, 2, 1, 0), (FREE, 1, 1, 0, 2), (S, X, 1, 1, 0, 4),
    (PRODUCT, 1, ((2, 0),), 1), (R, X, 1, 0, 0, 0), (R, X, 1, 0, 0, 1), (NEAR, 1, 0, 0, 1), (NEAR, 1, 0, 0, 2),
    (S, X, 1, 0, 0, 2), (PRODUCT, 1, ((2, 1),), 1), (S, X, 1, 0, 0, 5), (PRODUCT, 1, ((1, 0), (-1, 0)), 1),
    (R, C, 1, 0, 1, 0), (FAR, 1, 1, 0), (S, X, 1, 1, 0, 0), (PRODUCT, 1, ((1, 1), (-1, 1)), 1), (R, C, 1, 0, 0, 1),
    (R, C, 1, 0, 1, 1), (S, X, 1, 1, 0, 1), (FAR, 1, 0, 1), (FAR, 1, 1, 1), (PRODUCT, 1, ((0, 0), (0, 1)), 0),
    (R, C, 1, 1, 0, 1), (R, C, 1, 2, 0, 1), (FREE, 1, 0, 1, 1), (FREE, 1, 0, 1, 2), (S, X, 1, 0, 1, 0),
    (S, X, 1, 0, 1, 1), (PRODUCT, 1, ((0, 0), (0, 1)), 1), (R, X, 1, 1, 0, 3), (R, C, 1, 1, 1, 1), (R, C, 1, 2, 1, 1),
    (FREE, 1, 1, 1, 1), (FREE, 1, 1, 1, 2), (R, X, 1, 1, 0, 4), (R, C, 1, 3, 0, 0), (S, X, 1, 1, 1, 0),
    (R, C, 1, 3, 1, 0), (R, X, 1, 0, 0, 2), (S, X, 1, 1, 1, 1), (R, C, 1, 3, 0, 1), (R, X, 1, 0, 0, 5),
    (FINISH, 0, 0), (R, C, 1, 3, 1, 1), (S, X, 1, 0, 1, 3), (R, X, 1, 1, 0, 0), (NEAR, 1, 1, 0, 1),
    (S, X, 1, 0, 1, 4), (R, X, 1, 1, 0, 1), (NEAR, 1, 1, 0, 2), (S, X, 1, 1, 0, 2), (R, X, 1, 0, 1, 0),
    (NEAR, 1, 0, 1, 1), (S, X, 1, 1, 0, 5), (R, X, 1, 0, 1, 1), (NEAR, 1, 0, 1, 2), (S, X, 1, 0, 1, 2),
    (R, X, 1, 1, 1, 0), (NEAR, 1, 1, 1, 1), (S, X, 1, 0, 1, 5), (R, X, 1, 1, 1, 1), (NEAR, 1, 1, 1, 2),
    (S, X, 1, 1, 1, 2), (R, X, 1, 0, 1, 3), (S, X, 1, 1, 1, 5), (R, X, 1, 0, 1, 4), (S, X, 1, 1, 1, 3),
    (R, X, 1, 1, 0, 2), (S, X, 1, 1, 1, 4), (R, X, 1, 1, 0, 5), (FINISH, 1, 0), (R, X, 1, 0, 1, 2),
    (R, X, 1, 0, 1, 5), (FINISH, 0, 1), (R, X, 1, 1, 1, 2), (R, X, 1, 1, 1, 5), (R, X, 1, 1, 1, 3),
    (R, X, 1, 1, 1, 4), (FINISH, 1, 1),
)


def way_of(key):
    if key[0] == W:
        return MESSAGES[key[1]][key[2]][3]
    if key[0] == G:
        return GATHER[key[2]][3]
    if key[0] == C:
        return "d"
    return ("x+", "x-", "x+", "x+", "x-", "x-")[key[4]]


def share():
    sent, waited = {}, {}
    for i, (name, *which) in enumerate(SCHEDULE):
        if name == S:
            sent[tuple(which)] = i
        elif name == R:
            waited[tuple(which)] = i
        elif name == PRODUCT:
            g, cases, j = which
            for dx, h in cases:
                sent[(C, g, TURN[dx], h, j)] = i
    back = {"x+": "x-", "x-": "x+", "y+": "y-", "y-": "y+", "z+": "z-", "z-": "z+", "d": "d"}
    last, place = [], {}
    for key in sorted(sent, key=lambda k: (sent[k], k)):
        toward = [k for k in sent if way_of(k) == back[way_of(key)] and waited[k] < sent[key]]
        heard = max([sent[k] for k in toward], default=-1)
        free = [(at, n) for n, at in enumerate(last) if at < heard]
        if free:
            n = max(free)[1]
            last[n] = waited[key]
        else:
            n = len(last)
            last.append(waited[key])
        place[key] = n
    return place, len(last)


SEMAPHORE, SEMAPHORES = share()


def kernel(
    resid, mix_gain_in, wq, wk, wv, wg, wo, rate, mlp_gain_in, wu, wd,
    out,
    w_in, w_out, w_up, w_down, xn, rbuf, after, proj, gated, hid, decay, begun, kept, mix_gain, mlp_gain,
    dout, din, sout, rin2, rin1,
    local_sem, w_send, g_send, d_send, s_send, recv,
):
    fs, tp = lax.axis_index("fs"), lax.axis_index("tp")
    z, y, x, c = fs // RING, fs % RING, tp // 2, tp % 2

    def turn(v, d):
        return (v + d + RING) % RING

    device = {
        "y+": (z * RING + turn(y, 1), tp),
        "y-": (z * RING + turn(y, -1), tp),
        "z+": (turn(z, 1) * RING + y, tp),
        "z-": (turn(z, -1) * RING + y, tp),
        "x+": (fs, turn(x, 1) * 2 + c),
        "x-": (fs, turn(x, -1) * 2 + c),
        "d": (fs, x * 2 + 1 - c),
    }

    def remote(src, dst, send, recv, way):
        return pltpu.make_async_remote_copy(
            src_ref=src, dst_ref=dst, send_sem=send, recv_sem=recv,
            device_id=device[way], device_id_type=MESH,
        )

    def send(*args):
        remote(*args).start()

    weights = (w_in, w_out, w_up, w_down)

    def block(dy, dz):
        return turn(z, dz) * RING + turn(y, dy)

    def piece(t, dy, dz, part):
        ref = weights[t]
        f = block(dy, dz)
        if part == "full":
            return ref.at[f]
        if part in ("A", "B"):
            return ref.at[f, :, "AB".index(part)]
        if part in ("h0", "h1"):
            return ref.at[f, int(part[1])]
        return ref.at[f, int(part[2]), "AB".index(part[0])]

    def w_copy(t, n, place):
        dy, dz, part, way = place
        ref = piece(t, dy, dz, part)
        return (ref, ref, w_send.at[t], recv.at[SEMAPHORE[W, t, n]], way)

    def g_copy(g, n, dx, core):
        h, q, way = GATHER[n][1:]
        block = turn(x, dx) * 2 + core
        ref = xn.at[g, block, h] if q is None else xn.at[g, block, h, q]
        return (ref, ref, g_send.at[g], recv.at[SEMAPHORE[G, g, n]], way)

    def rows16(count, body):
        def step(i, carry):
            body(pl.ds(pl.multiple_of(i * 16, 16), 16))
            return carry

        lax.fori_loop(0, count // 16, step, 0)

    def of(ref, j):
        return ref.at[:, pl.ds(j * 1024, 1024)]

    def d_copy(g, k, h, j):
        columns = pl.ds(j * 1024, 1024)
        return (
            dout.at[g, k, h, :, :, columns], din.at[g, k, h, :, :, columns],
            d_send.at[g], recv.at[SEMAPHORE[C, g, k, h, j]], "d",
        )

    def s_copy(g, h, j, n):
        if n < 2:
            src, dst, way = sout.at[g, 0, h, n], rin2.at[g, h, n], ("x+", "x-")[n]
        elif n < 4:
            src, dst, way = sout.at[g, 1, h, n - 2], rin1.at[g, 0, h, n - 2], "x+"
        else:
            src, dst, way = sout.at[g, 2, h, n - 4], rin1.at[g, 1, h, n - 4], "x-"
        return (of(src, j), of(dst, j), s_send.at[g], recv.at[SEMAPHORE[X, g, h, j, n]], way)

    def start(kind, *which):
        if kind == W:
            t, n = which
            send(*w_copy(t, n, MESSAGES[t][n]))
        elif kind == G:
            g, n = which
            send(*g_copy(g, n, GATHER[n][0], c))
        else:
            send(*s_copy(*which))

    def receive(kind, *which):
        if kind == W:
            t, n = which
            copy = w_copy(t, n, arrived(MESSAGES[t][n]))
        elif kind == G:
            g, n = which
            dx, way = GATHER[n][0], GATHER[n][3]
            if way == "d":
                copy = g_copy(g, n, dx, 1 - c)
            else:
                copy = g_copy(g, n, near(dx - (1 if way == "x+" else -1)), c)
        elif kind == C:
            copy = d_copy(*which)
        else:
            copy = s_copy(*which)
        remote(*copy).wait_recv()

    def partial(g, cases, j):
        weight, lhs = ((w_out, gated_rows), (w_down, hidden_rows))[g]
        depth = weight.shape[1] * weight.shape[2] * weight.shape[3]
        for i in (2 * j, 2 * j + 1):
            w = [weight[block(*PLACES[4 * i + n])].reshape(depth, 128) for n in range(4)]
            rows = [some for case in cases for some in lhs(*case)]
            o = jnp.dot(
                jnp.concatenate(rows, axis=0), jnp.concatenate(w, axis=1), preferred_element_type=F32
            )
            columns = slice(i * 512, (i + 1) * 512)
            for n, (dx, h) in enumerate(cases):
                mine = o[n * 128 : (n + 1) * 128]
                dout[g, TURN[dx], h, :, :, columns] = mine[:64].astype(BF16).reshape(2, 32, 512)
                kept[TURN[dx], h, :, :, columns] = mine[64:].reshape(2, 32, 512)
        for dx, h in cases:
            send(*d_copy(g, TURN[dx], h, j))

    def add_quarter(g, k, h, j, q, extra=False):
        columns = slice(j * 1024, (j + 1) * 1024)

        def body(rows):
            total = kept[k, h, q, rows, columns] + din[g, k, h, q, rows, columns].astype(F32)
            if extra:
                total = total + rin2[g, h, q, rows, columns].astype(F32)
            sout[g, k, h, q, rows, columns] = total.astype(BF16)

        rows16(32, body)

    def add_far(g, h, j):
        for q in (0, 1):
            add_quarter(g, 0, h, j, q)

    def add_free(g, h, j, k):
        add_quarter(g, k, h, j, 1 if k == 1 else 0)

    def add_near(g, h, j, k):
        add_quarter(g, k, h, j, 0 if k == 1 else 1, True)

    def add_own(g, h, i, source, target):
        here = pl.ds(pl.multiple_of(block(*PLACES[i]) * 128, 128), 128)
        at = slice(i * 128, (i + 1) * 128)
        total = source[h, :, :, here].astype(F32) + kept[3, h, :, :, at]
        total = total + din[g, 3, h, :, :, at].astype(F32)
        total = total + rin1[g, 0, h, :, :, at].astype(F32) + rin1[g, 1, h, :, :, at].astype(F32)
        target[h, :, :, here] = total.astype(BF16)

    def normed(values, gain):
        scale = lax.rsqrt(jnp.mean(values * values, axis=-1, keepdims=True) + EPS)
        return (values * scale * gain).astype(BF16)

    barrier = pltpu.get_barrier_semaphore()
    for way in device:
        pl.semaphore_signal(barrier, inc=1, device_id=device[way], device_id_type=MESH)
    loads = []

    def load(src, dst):
        copy = pltpu.make_async_copy(src, dst, local_sem.at[len(loads)])
        copy.start()
        return copy

    for src, low, wide in ((wq, 0, 128), (wk, 128, 128), (wv, 256, 256), (wg, 512, 256)):
        load(src, w_in.at[fs, :, :, :, low : low + wide])
    loads.append(pltpu.make_async_copy(w_in.at[fs], w_in.at[fs], local_sem.at[0]))
    loads.append(load(resid, rbuf))
    loads.append(load(mix_gain_in, mix_gain))
    loads.append(load(mlp_gain_in, mlp_gain))
    for src, dst in ((wo, w_out.at[fs]), (wu, w_up.at[fs]), (wd, w_down.at[fs])):
        loads.append(load(src, dst))
    for copy in loads[:4]:
        copy.wait()
    for h in (0, 1):
        for q in (0, 1):
            def first_norm(rows):
                xn[0, tp, h, q, rows, :] = normed(rbuf[h, q, rows, :].astype(F32), mix_gain[...])

            rows16(32, first_norm)
    pl.semaphore_wait(barrier, 7)
    r = rate[0]

    def make_decay():
        def some_rows(i, carry):
            rows = pl.ds(pl.multiple_of(i * 64, 64), 64)
            t = lax.broadcasted_iota(jnp.int32, (64, LENGTH), 0) + i * 64
            s = lax.broadcasted_iota(jnp.int32, (64, LENGTH), 1)
            gap = (t - s).astype(F32)
            value = jnp.exp(-r * jnp.maximum(gap, 0.0)) * DK ** (-0.5)
            decay[rows, :] = jnp.where(gap >= 0.0, value, 0.0)
            return carry

        lax.fori_loop(0, LENGTH // 64, some_rows, 0)

    own = x // 2
    sequence = (own, 1 - own)

    chips = ((2 * own, 2), (2 * (1 - own) + 1 - x % 2, 1), (turn(x, 2), 1))

    def project(which, part):
        blocks = [block(*place) for place in (PLACES[:12], PLACES[12:])[part]]
        first, count = chips[which] if part == 0 else (2 * sequence[which], 2)

        def body(j, carry):
            columns = pl.ds(pl.multiple_of(j * 256, 256), 256)
            lhs = [
                xn[0, pl.ds(2 * first, 2 * count), :, :, :, pl.ds(pl.multiple_of(f * 128, 128), 128)]
                .reshape(256 * count, 128)
                for f in blocks
            ]
            rhs = [w_in[f, :, :, :, columns].reshape(128, 256) for f in blocks]
            o = jnp.dot(
                jnp.concatenate(lhs, axis=1), jnp.concatenate(rhs, axis=0), preferred_element_type=F32
            ).reshape(count, 256, 256)
            if part == 0:
                begun[j, pl.ds(first, count)] = o
            else:
                o = (begun[j, pl.ds(first, count)] + o).astype(BF16)
                proj[pl.ds(2 * first, 2 * count), :, columns] = o.reshape(2 * count, 128, 256)
            return carry

        lax.fori_loop(0, 3, body, 0)

    def retain(seq):
        for i in (0, 1):
            mine = pl.ds(seq * 4 + 2 * i, 2)
            upto = pl.ds(seq * 4, 2 * i + 2)
            wide = 256 * (i + 1)
            q = proj[mine, :, 0:128].reshape(256, DK)
            k = proj[upto, :, 128:256].reshape(wide, DK)
            v = proj[upto, :, 256:512].reshape(wide, DV)
            scores = lax.dot_general(q, k, (((1,), (1,)), ((), ())), preferred_element_type=F32)
            scores = (scores * decay[i * 256 : (i + 1) * 256, 0:wide]).astype(BF16)
            mixed = jnp.dot(scores, v, preferred_element_type=F32)
            mixed = mixed - jnp.mean(mixed, axis=-1, keepdims=True)
            spread = jnp.mean(mixed * mixed, axis=-1, keepdims=True)
            gate = proj[mine, :, 512:768].reshape(256, DV).astype(F32)
            value = gate / (1.0 + jnp.exp(-gate)) * (mixed * lax.rsqrt(spread + EPS))
            gated[mine] = value.astype(BF16).reshape(2, 2, 64, DV)

    def gated_rows(dx, h):
        first = turn(x, dx) * 2
        return gated[first + 1 - c, h], gated[first + c, h]

    def lift(cases, part):
        def body(j, carry):
            columns = pl.ds(pl.multiple_of(j * 256, 256), 256)
            lhs = jnp.concatenate(
                [
                    xn[1, turn(x, dx) * 2 + core, h].reshape(64, D)
                    for dx, h in cases
                    for core in (1 - c, c)
                ],
                axis=0,
            )
            rhs = w_up[:, :, :, :, columns].reshape(D, 256)
            o = jnp.maximum(jnp.dot(lhs, rhs, preferred_element_type=F32), 0.0)
            o = (o * o).astype(BF16)
            for n, (dx, h) in enumerate(cases):
                hid[TURN[dx], h, :, columns] = o[n * 128 : (n + 1) * 128]
            return carry

        count = w_up.shape[4] // 512
        lax.fori_loop(part * count, (part + 1) * count, body, 0)

    def hidden_rows(dx, h):
        return (hid[TURN[dx], h],)

    def second_norm(h):
        for i in range(16):
            add_own(0, h, i, rbuf, after)
        for q in (0, 1):
            def body(rows):
                xn[1, tp, h, q, rows, :] = normed(after[h, q, rows, :].astype(F32), mlp_gain[...])

            rows16(32, body)

    def finish(h, j):
        for i in range(8 * j, 8 * j + 8):
            add_own(1, h, i, after, out)

    actions = {
        S: start,
        R: receive,
        DECAY: make_decay,
        PROJECT: project,
        RETAIN: lambda which: retain(sequence[which]),
        PRODUCT: partial,
        FAR: add_far,
        FREE: add_free,
        NEAR: add_near,
        NORM: second_norm,
        LIFT: lift,
        FINISH: finish,
    }
    for copy in loads[4:]:
        copy.wait()
    for name, *which in SCHEDULE:
        actions[name](*which)
    for t in range(4):
        ref = weights[t].at[0:15]
        remote(ref, ref, w_send.at[t], recv.at[0], "d").wait_send()
    for g in (0, 1):
        remote(xn.at[g, 0:7], xn.at[g, 0:7], g_send.at[g], recv.at[0], "d").wait_send()
        remote(dout.at[g], din.at[g], d_send.at[g], recv.at[0], "d").wait_send()
        remote(sout.at[g], sout.at[g], s_send.at[g], recv.at[0], "d").wait_send()


def on_device(
    resid, mix_gain, w_query, w_key, w_value, w_gate, w_output, decay_rate, mlp_gain, w_up, w_down
):
    def cut(w):
        return w.reshape(2, 2, w.shape[0] // 4, w.shape[1])

    wide = w_query.shape[1] + w_key.shape[1] + w_value.shape[1] + w_gate.shape[1]
    count = RING * RING

    def held(rows, columns):
        return pltpu.VMEM((count, 2, 2, rows // 4, columns), BF16)

    dma = pltpu.SemaphoreType.DMA
    vmem = pl.BlockSpec(memory_space=pltpu.VMEM)
    hbm = pl.BlockSpec(memory_space=pltpu.HBM)
    tokens = (2, 2, 32, D)
    result = pl.pallas_call(
        kernel,
        out_shape=pltpu.VMEM(tokens, BF16),
        in_specs=[
            hbm, hbm, hbm, hbm, hbm, hbm, hbm,
            pl.BlockSpec(memory_space=pltpu.SMEM), hbm, hbm, hbm,
        ],
        out_specs=vmem,
        scratch_shapes=[
            held(128, wide),
            held(w_output.shape[0], 128),
            held(128, w_up.shape[1]),
            held(w_down.shape[0], 128),
            pltpu.VMEM((2, 8) + tokens, BF16),
            pltpu.VMEM(tokens, BF16),
            pltpu.VMEM(tokens, BF16),
            pltpu.VMEM((8, 128, wide), BF16),
            pltpu.VMEM((8, 2, 64, DV), BF16),
            pltpu.VMEM((4, 2, 128, w_up.shape[1]), BF16),
            pltpu.VMEM((LENGTH, LENGTH), F32),
            pltpu.VMEM((wide // 256, 4, 256, 256), F32),
            pltpu.VMEM((4,) + tokens, F32),
            pltpu.VMEM((1, D), F32),
            pltpu.VMEM((1, D), F32),
            pltpu.VMEM((2, 4) + tokens, BF16),
            pltpu.VMEM((2, 4) + tokens, BF16),
            pltpu.VMEM((2, 3) + tokens, BF16),
            pltpu.VMEM((2,) + tokens, BF16),
            pltpu.VMEM((2, 2) + tokens, BF16),
            dma((8,)),
            dma((4,)),
            dma((2,)),
            dma((2,)),
            dma((2,)),
            dma((SEMAPHORES,)),
        ],
        compiler_params=pltpu.CompilerParams(
            collective_id=0, has_side_effects=True, vmem_limit_bytes=66060288
        ),
    )(
        resid.reshape(tokens), mix_gain[None], cut(w_query), cut(w_key), cut(w_value), cut(w_gate),
        cut(w_output), decay_rate, mlp_gain[None], cut(w_up), cut(w_down),
    )
    return result.reshape(resid.shape)


def solution(mesh):
    placed = (
        P(("fs", "tp"), None),
        P(),
        P("fs", "tp"),
        P("fs", "tp"),
        P("fs", "tp"),
        P("fs", "tp"),
        P("tp", "fs"),
        P("tp"),
        P(),
        P("fs", "tp"),
        P("tp", "fs"),
    )
    return jax.shard_map(
        on_device, mesh=mesh, in_specs=placed, out_specs=P(("fs", "tp"), None), check_vma=False
    )
```

```python
import jax
import jax.numpy as jnp
from jax import lax
from jax.experimental import pallas as pl
from jax.experimental.pallas import tpu as pltpu
from jax.sharding import PartitionSpec as P

D = 2048
DK = 128
DV = 256
LENGTH = 512
RING = 4
EPS = 1e-06
MESH = pl.DeviceIdType.MESH
F32 = jnp.float32
BF16 = jnp.bfloat16

STEP = {"y+": (1, 0), "y-": (-1, 0), "z+": (0, 1), "z-": (0, -1)}


def near(d):
    return {0: 0, 1: 1, 2: 2, 3: -1}[d % RING]


def arrived(message):
    dy, dz, part, way = message
    return near(dy - STEP[way][0]), near(dz - STEP[way][1]), part, way


def onward(message):
    dy, dz, part, way = arrived(message)
    half = "0" if way[1] == "+" else "1"
    along = way[0] == "y"
    across = ("z+", "z-") if along else ("y+", "y-")
    first = "A" if along else "B"
    if part == "full":
        return [(dy, dz, "h" + half, way)] + [(dy, dz, first, w) for w in across]
    if part in ("h0", "h1"):
        onto = [(dy, dz, part, way)] if (dy if along else dz) != 2 and part[1] == half else []
        return onto + [(dy, dz, first + part, w) for w in across]
    if part in ("A", "B"):
        return [(dy, dz, part + "h" + half, way)]
    if (dy if way[0] == "y" else dz) != 2 and part[-1] == half:
        return [(dy, dz, part, way)]
    return []


def plan(parts):
    messages = [(0, 0, part, way) for part in parts for way in ("y+", "y-", "z+", "z-")]
    for message in messages:
        messages += onward(message)
    return messages


MESSAGES = [plan(parts) for parts in (("h0", "h1"), ("full",), ("h0", "h1"), ("full",))]
PLACES = (
    (0, 0), (1, 0), (-1, 0), (0, 1), (0, -1), (2, 0), (0, 2), (1, 1),
    (1, -1), (-1, 1), (-1, -1), (2, 1), (2, -1), (1, 2), (-1, 2), (2, 2),
)

GATHER = (
    [(0, h, q, w) for h in (0, 1) for q in (0, 1) for w in ("x+", "x-")]
    + [(0, h, None, "d") for h in (0, 1)]
    + [(dx, h, q, "d") for dx in (-1, 1, 2) for h in (0, 1) for q in (0, 1)]
    + [(-1, h, 0, "x+") for h in (0, 1)]
    + [(1, h, 1, "x-") for h in (0, 1)]
)
TURN = {2: 0, 1: 1, -1: 2, 0: 3}

S, R, W, G, C, X = range(6)
DECAY, PROJECT, RETAIN, PRODUCT, FAR, FREE, NEAR, NORM, LIFT, FINISH = range(6, 16)
SCHEDULE = (
    (S, W, 0, 0), (S, W, 0, 5), (S, W, 0, 2), (S, W, 0, 7), (S, G, 0, 0), (S, G, 0, 3), (S, G, 0, 8), (S, G, 0, 9),
    (DECAY,), (S, W, 0, 4), (S, W, 0, 1), (S, W, 0, 6), (S, W, 0, 3), (R, G, 0, 8), (R, G, 0, 9), (S, G, 0, 2),
    (S, G, 0, 1), (S, W, 1, 0), (S, W, 1, 1), (S, W, 1, 2), (S, W, 1, 3), (R, W, 0, 0), (R, W, 0, 5), (R, W, 0, 2),
    (R, W, 0, 7), (S, W, 0, 8), (S, W, 0, 20), (S, W, 0, 13), (S, W, 0, 25), (S, G, 0, 4), (S, G, 0, 7), (R, G, 0, 0),
    (S, G, 0, 10), (R, G, 0, 3), (S, G, 0, 15), (R, G, 0, 10), (R, W, 0, 4), (R, W, 0, 1), (R, W, 0, 6), (R, W, 0, 3),
    (S, W, 0, 16), (S, W, 0, 24), (S, W, 0, 11), (S, W, 0, 22), (R, G, 0, 15), (S, G, 0, 22), (S, G, 0, 24),
    (S, W, 0, 14), (S, W, 0, 27), (S, W, 0, 9), (S, W, 0, 19), (R, G, 0, 2), (S, G, 0, 11), (R, G, 0, 1),
    (S, G, 0, 14), (R, W, 1, 0), (R, W, 1, 1), (R, W, 1, 2), (R, W, 1, 3), (S, W, 0, 26), (S, W, 0, 15),
    (S, W, 0, 21), (S, W, 0, 12), (R, G, 0, 11), (R, G, 0, 14), (S, W, 0, 23), (S, W, 0, 17), (S, W, 0, 18),
    (S, W, 0, 10), (R, W, 0, 8), (R, W, 0, 20), (R, W, 0, 13), (R, W, 0, 25), (S, G, 0, 6), (S, G, 0, 5),
    (R, G, 0, 4), (S, G, 0, 12), (R, G, 0, 7), (S, G, 0, 17), (S, W, 0, 32), (S, W, 0, 42), (S, W, 0, 28),
    (S, W, 0, 38), (R, W, 0, 16), (R, W, 0, 24), (R, W, 0, 11), (R, W, 0, 22), (S, W, 0, 41), (S, W, 0, 33),
    (S, W, 0, 31), (S, W, 0, 39), (R, G, 0, 12), (R, W, 0, 14), (R, W, 0, 27), (R, W, 0, 9), (R, W, 0, 19),
    (R, G, 0, 17), (S, W, 0, 35), (S, W, 0, 40), (S, W, 0, 37), (S, W, 0, 29), (R, W, 0, 26), (R, W, 0, 15),
    (R, W, 0, 21), (R, W, 0, 12), (S, G, 0, 23), (S, G, 0, 25), (R, G, 0, 22), (S, G, 0, 18), (R, G, 0, 24),
    (S, G, 0, 19), (S, W, 0, 34), (S, W, 0, 43), (S, W, 0, 30), (S, W, 0, 36), (R, W, 0, 23), (R, W, 0, 17),
    (R, W, 0, 18), (R, W, 0, 10), (R, G, 0, 18), (S, W, 1, 4), (S, W, 1, 7), (S, W, 1, 10), (S, W, 1, 13),
    (R, G, 0, 19), (R, W, 0, 32), (R, W, 0, 42), (R, W, 0, 28), (R, W, 0, 38), (S, W, 0, 45), (S, W, 0, 47),
    (S, W, 0, 44), (S, W, 0, 46), (R, W, 0, 41), (R, W, 0, 33), (R, W, 0, 31), (R, W, 0, 39), (R, G, 0, 6),
    (S, G, 0, 13), (R, G, 0, 5), (S, G, 0, 16), (S, W, 1, 14), (S, W, 1, 12), (S, W, 1, 8), (S, W, 1, 6),
    (R, W, 0, 35), (R, W, 0, 40), (R, W, 0, 37), (R, W, 0, 29), (S, W, 1, 11), (S, W, 1, 15), (S, W, 1, 5),
    (S, W, 1, 9), (R, G, 0, 13), (R, G, 0, 16), (S, W, 2, 0), (S, W, 2, 5), (S, W, 2, 2), (S, W, 2, 7), (R, W, 0, 34),
    (R, W, 0, 43), (R, W, 0, 30), (R, W, 0, 36), (PROJECT, 1, 0), (R, W, 1, 4), (R, W, 1, 7), (R, W, 1, 10),
    (R, W, 1, 13), (R, G, 0, 23), (S, G, 0, 20), (R, G, 0, 25), (S, G, 0, 21), (S, W, 1, 24), (S, W, 1, 29),
    (S, W, 1, 16), (S, W, 1, 21), (PROJECT, 0, 0), (R, W, 0, 45), (R, W, 0, 47), (R, W, 0, 44), (R, W, 0, 46),
    (R, G, 0, 20), (R, W, 1, 14), (R, W, 1, 12), (R, W, 1, 8), (R, W, 1, 6), (R, G, 0, 21), (S, W, 1, 28),
    (S, W, 1, 30), (S, W, 2, 4), (S, W, 1, 25), (S, W, 1, 27), (S, W, 2, 1), (S, W, 1, 22), (S, W, 1, 20),
    (S, W, 2, 6), (S, W, 1, 17), (S, W, 1, 19), (S, W, 2, 3), (PROJECT, 2, 0), (R, W, 1, 11), (R, W, 1, 15),
    (R, W, 1, 5), (R, W, 1, 9), (PROJECT, 1, 1), (RETAIN, 1), (PRODUCT, 0, ((2, 0), (2, 1)), 0), (S, W, 1, 26),
    (S, W, 1, 31), (S, W, 1, 18), (S, W, 1, 23), (PROJECT, 0, 1), (R, W, 2, 0), (R, W, 2, 5), (R, W, 2, 2),
    (R, W, 2, 7), (R, W, 1, 24), (R, W, 1, 29), (R, W, 1, 16), (R, W, 1, 21), (R, W, 1, 28), (R, W, 1, 25),
    (R, W, 1, 22), (R, W, 1, 17), (S, W, 1, 34), (S, W, 2, 8), (S, W, 1, 35), (S, W, 2, 20), (S, W, 1, 32),
    (S, W, 2, 13), (S, W, 1, 33), (S, W, 2, 25), (RETAIN, 0), (R, W, 1, 30), (R, W, 1, 27), (R, W, 1, 20),
    (R, W, 1, 19), (R, C, 0, 0, 0, 0), (R, C, 0, 0, 1, 0), (FAR, 0, 0, 0), (S, X, 0, 0, 0, 0), (S, X, 0, 0, 0, 1),
    (FAR, 0, 1, 0), (PRODUCT, 0, ((1, 0), (-1, 0)), 0), (PRODUCT, 0, ((1, 1), (-1, 1)), 0), (S, X, 0, 1, 0, 0),
    (S, X, 0, 1, 0, 1), (PRODUCT, 0, ((0, 0), (0, 1)), 0), (R, C, 0, 1, 0, 0), (FREE, 0, 0, 0, 1), (R, C, 0, 2, 0, 0),
    (FREE, 0, 0, 0, 2), (R, C, 0, 1, 1, 0), (FREE, 0, 1, 0, 1), (R, W, 2, 4), (R, W, 2, 1), (R, W, 2, 6),
    (R, W, 2, 3), (S, W, 2, 16), (S, W, 2, 27), (S, W, 3, 2), (S, W, 2, 19), (S, X, 0, 0, 0, 3), (S, X, 0, 0, 0, 4),
    (R, C, 0, 2, 1, 0), (FREE, 0, 1, 0, 2), (R, W, 1, 26), (R, W, 1, 31), (R, W, 1, 18), (R, W, 1, 23),
    (R, C, 0, 3, 0, 0), (R, W, 1, 34), (R, W, 1, 35), (R, W, 1, 32), (R, W, 1, 33), (PRODUCT, 0, ((2, 0), (2, 1)), 1),
    (R, C, 0, 3, 1, 0), (PRODUCT, 0, ((1, 0), (-1, 0)), 1), (S, W, 3, 0), (S, W, 2, 24), (S, W, 2, 22),
    (S, X, 0, 1, 0, 3), (S, X, 0, 1, 0, 4), (PRODUCT, 0, ((1, 1), (-1, 1)), 1), (PRODUCT, 0, ((0, 0), (0, 1)), 1),
    (R, X, 0, 0, 0, 0), (R, X, 0, 0, 0, 1), (NEAR, 0, 0, 0, 1), (NEAR, 0, 0, 0, 2), (R, C, 0, 0, 0, 1),
    (FAR, 0, 0, 1), (R, C, 0, 0, 1, 1), (FAR, 0, 1, 1), (S, W, 3, 1), (S, W, 3, 3), (R, C, 0, 1, 0, 1),
    (S, X, 0, 0, 1, 0), (S, X, 0, 0, 1, 1), (FREE, 0, 0, 1, 1), (R, C, 0, 2, 0, 1), (FREE, 0, 0, 1, 2),
    (R, X, 0, 1, 0, 0), (R, X, 0, 1, 0, 1), (NEAR, 0, 1, 0, 1), (NEAR, 0, 1, 0, 2), (R, C, 0, 1, 1, 1),
    (FREE, 0, 1, 1, 1), (R, W, 2, 8), (R, W, 2, 20), (R, W, 2, 13), (R, W, 2, 25), (R, C, 0, 2, 1, 1),
    (FREE, 0, 1, 1, 2), (R, C, 0, 3, 0, 1), (R, C, 0, 3, 1, 1), (S, X, 0, 1, 1, 0), (S, X, 0, 1, 1, 1),
    (R, X, 0, 0, 0, 3), (R, X, 0, 0, 0, 4), (R, W, 2, 16), (R, W, 2, 27), (R, W, 2, 19), (S, W, 2, 9),
    (S, X, 0, 0, 0, 2), (S, X, 0, 0, 0, 5), (R, X, 0, 1, 0, 3), (R, X, 0, 1, 0, 4), (R, W, 2, 24), (R, W, 2, 22),
    (S, W, 2, 32), (S, W, 2, 28), (S, X, 0, 0, 1, 3), (S, X, 0, 0, 1, 4), (R, X, 0, 0, 1, 0), (R, X, 0, 0, 1, 1),
    (NEAR, 0, 0, 1, 1), (NEAR, 0, 0, 1, 2), (S, W, 2, 14), (S, W, 2, 42), (S, W, 2, 11), (S, W, 2, 38),
    (S, X, 0, 0, 1, 2), (S, X, 0, 0, 1, 5), (R, X, 0, 1, 1, 0), (R, X, 0, 1, 1, 1), (NEAR, 0, 1, 1, 1),
    (NEAR, 0, 1, 1, 2), (R, W, 3, 2), (S, W, 2, 35), (S, W, 2, 15), (S, W, 2, 21), (S, W, 2, 29), (S, X, 0, 1, 0, 2),
    (S, X, 0, 1, 0, 5), (R, X, 0, 0, 0, 2), (R, X, 0, 0, 0, 5), (R, W, 3, 0), (R, W, 2, 9), (S, W, 2, 41),
    (S, W, 2, 43), (S, W, 2, 18), (S, W, 2, 10), (S, X, 0, 1, 1, 2), (S, X, 0, 1, 1, 5), (R, X, 0, 0, 1, 3),
    (R, X, 0, 0, 1, 4), (R, W, 2, 32), (R, W, 3, 1), (R, W, 3, 3), (R, W, 2, 28), (S, W, 3, 4), (S, W, 3, 7),
    (S, W, 2, 37), (S, W, 3, 13), (S, X, 0, 1, 1, 3), (S, X, 0, 1, 1, 4), (R, X, 0, 0, 1, 2), (R, X, 0, 0, 1, 5),
    (NORM, 0), (S, G, 1, 8), (R, W, 2, 14), (R, W, 2, 42), (R, W, 2, 11), (R, W, 2, 38), (S, W, 2, 31), (S, G, 1, 0),
    (S, G, 1, 3), (R, X, 0, 1, 0, 2), (R, X, 0, 1, 0, 5), (R, W, 2, 35), (R, W, 2, 15), (R, W, 2, 21), (R, W, 2, 29),
    (R, G, 1, 8), (S, W, 2, 34), (S, W, 2, 47), (S, W, 3, 10), (S, W, 2, 46), (R, X, 0, 1, 1, 2), (R, X, 0, 1, 1, 5),
    (R, W, 2, 41), (R, W, 2, 43), (R, W, 2, 18), (R, W, 2, 10), (S, W, 2, 45), (S, W, 2, 40), (S, W, 2, 36),
    (S, G, 1, 2), (S, G, 1, 1), (R, X, 0, 1, 1, 3), (R, X, 0, 1, 1, 4), (NORM, 1), (S, G, 1, 9), (R, W, 2, 37),
    (S, W, 2, 23), (S, W, 2, 33), (S, W, 2, 30), (S, W, 2, 39), (R, W, 3, 4), (R, W, 2, 31), (R, W, 3, 7),
    (R, W, 3, 13), (R, G, 1, 9), (S, W, 2, 26), (S, W, 2, 17), (S, W, 2, 44), (S, W, 2, 12), (S, G, 1, 4),
    (S, G, 1, 7), (R, G, 1, 0), (S, G, 1, 10), (R, G, 1, 3), (S, G, 1, 15), (R, W, 2, 34), (R, W, 2, 47),
    (R, W, 2, 46), (S, W, 3, 11), (S, W, 3, 15), (S, W, 3, 16), (S, W, 3, 9), (R, G, 1, 10), (R, G, 1, 15),
    (R, W, 2, 45), (R, W, 3, 10), (R, W, 2, 40), (R, W, 2, 36), (S, W, 3, 5), (S, G, 1, 22), (S, G, 1, 24),
    (R, G, 1, 2), (S, G, 1, 11), (R, G, 1, 1), (S, G, 1, 14), (R, W, 2, 23), (R, W, 2, 33), (R, W, 2, 30),
    (R, W, 2, 39), (S, W, 3, 24), (S, W, 3, 29), (S, W, 3, 21), (R, G, 1, 11), (R, G, 1, 14), (R, W, 2, 26),
    (R, W, 2, 17), (R, W, 2, 44), (R, W, 2, 12), (S, W, 3, 14), (S, W, 3, 12), (S, W, 3, 8), (S, W, 3, 6),
    (S, G, 1, 6), (S, G, 1, 5), (LIFT, ((0, 0), (-1, 0), (1, 0)), 0), (R, G, 1, 4), (S, G, 1, 12), (R, G, 1, 7),
    (S, G, 1, 17), (LIFT, ((0, 0), (-1, 0), (1, 0)), 1), (R, W, 3, 16), (R, G, 1, 12), (R, W, 3, 11), (R, W, 3, 15),
    (R, W, 3, 9), (PRODUCT, 1, ((1, 0), (-1, 0)), 0), (R, G, 1, 17), (S, W, 3, 26), (S, W, 3, 31), (S, W, 3, 32),
    (S, W, 3, 17), (S, G, 1, 23), (S, G, 1, 25), (R, G, 1, 22), (S, G, 1, 18), (R, G, 1, 24), (S, G, 1, 19),
    (R, W, 3, 24), (R, W, 3, 5), (R, W, 3, 29), (R, W, 3, 21), (R, C, 1, 1, 0, 0), (FREE, 1, 0, 0, 1), (S, W, 3, 34),
    (S, W, 3, 25), (S, W, 3, 18), (S, W, 3, 23), (R, C, 1, 2, 0, 0), (FREE, 1, 0, 0, 2), (R, G, 1, 18), (R, G, 1, 19),
    (LIFT, ((2, 0),), 0), (S, W, 3, 28), (S, W, 3, 35), (S, W, 3, 20), (S, W, 3, 33), (S, X, 1, 0, 0, 3),
    (S, X, 1, 0, 0, 4), (LIFT, ((2, 0),), 1), (R, G, 1, 6), (S, G, 1, 13), (R, G, 1, 5), (S, G, 1, 16), (R, W, 3, 14),
    (R, W, 3, 12), (R, W, 3, 8), (R, W, 3, 6), (PRODUCT, 1, ((2, 0),), 0), (S, W, 3, 30), (S, W, 3, 27),
    (S, W, 3, 22), (S, W, 3, 19), (R, G, 1, 13), (R, W, 3, 26), (R, W, 3, 31), (R, W, 3, 32), (R, W, 3, 17),
    (R, G, 1, 16), (LIFT, ((0, 1), (-1, 1), (1, 1)), 0), (R, C, 1, 0, 0, 0), (R, G, 1, 23), (S, G, 1, 20),
    (R, G, 1, 25), (S, G, 1, 21), (R, W, 3, 34), (R, W, 3, 25), (R, W, 3, 18), (R, W, 3, 23), (FAR, 1, 0, 0),
    (S, X, 1, 0, 0, 0), (S, X, 1, 0, 0, 1), (LIFT, ((0, 1), (-1, 1), (1, 1)), 1), (R, X, 1, 0, 0, 3),
    (R, X, 1, 0, 0, 4), (PRODUCT, 1, ((1, 1), (-1, 1)), 0), (R, G, 1, 20), (R, W, 3, 28), (R, W, 3, 35),
    (R, W, 3, 20), (R, W, 3, 33), (R, G, 1, 21), (LIFT, ((2, 1),), 0), (LIFT, ((2, 1),), 1), (R, W, 3, 30),
    (R, W, 3, 27), (R, W, 3, 22), (R, W, 3, 19), (R, C, 1, 1, 1, 0), (FREE, 1, 1, 0, 1), (S, X, 1, 1, 0, 3),
    (PRODUCT, 1, ((2, 1),), 0), (R, C, 1, 2, 1, 0), (FREE, 1, 1, 0, 2), (S, X, 1, 1, 0, 4),
    (PRODUCT, 1, ((2, 0),), 1), (R, X, 1, 0, 0, 0), (R, X, 1, 0, 0, 1), (NEAR, 1, 0, 0, 1), (NEAR, 1, 0, 0, 2),
    (S, X, 1, 0, 0, 2), (PRODUCT, 1, ((2, 1),), 1), (S, X, 1, 0, 0, 5), (PRODUCT, 1, ((1, 0), (-1, 0)), 1),
    (R, C, 1, 0, 1, 0), (FAR, 1, 1, 0), (S, X, 1, 1, 0, 0), (PRODUCT, 1, ((1, 1), (-1, 1)), 1), (R, C, 1, 0, 0, 1),
    (R, C, 1, 0, 1, 1), (S, X, 1, 1, 0, 1), (FAR, 1, 0, 1), (FAR, 1, 1, 1), (PRODUCT, 1, ((0, 0), (0, 1)), 0),
    (R, C, 1, 1, 0, 1), (R, C, 1, 2, 0, 1), (FREE, 1, 0, 1, 1), (FREE, 1, 0, 1, 2), (S, X, 1, 0, 1, 0),
    (S, X, 1, 0, 1, 1), (PRODUCT, 1, ((0, 0), (0, 1)), 1), (R, X, 1, 1, 0, 3), (R, C, 1, 1, 1, 1), (R, C, 1, 2, 1, 1),
    (FREE, 1, 1, 1, 1), (FREE, 1, 1, 1, 2), (R, X, 1, 1, 0, 4), (R, C, 1, 3, 0, 0), (S, X, 1, 1, 1, 0),
    (R, C, 1, 3, 1, 0), (R, X, 1, 0, 0, 2), (S, X, 1, 1, 1, 1), (R, C, 1, 3, 0, 1), (R, X, 1, 0, 0, 5),
    (FINISH, 0, 0), (R, C, 1, 3, 1, 1), (S, X, 1, 0, 1, 3), (R, X, 1, 1, 0, 0), (NEAR, 1, 1, 0, 1),
    (S, X, 1, 0, 1, 4), (R, X, 1, 1, 0, 1), (NEAR, 1, 1, 0, 2), (S, X, 1, 1, 0, 2), (R, X, 1, 0, 1, 0),
    (NEAR, 1, 0, 1, 1), (S, X, 1, 1, 0, 5), (R, X, 1, 0, 1, 1), (NEAR, 1, 0, 1, 2), (S, X, 1, 0, 1, 2),
    (R, X, 1, 1, 1, 0), (NEAR, 1, 1, 1, 1), (S, X, 1, 0, 1, 5), (R, X, 1, 1, 1, 1), (NEAR, 1, 1, 1, 2),
    (S, X, 1, 1, 1, 2), (R, X, 1, 0, 1, 3), (S, X, 1, 1, 1, 5), (R, X, 1, 0, 1, 4), (S, X, 1, 1, 1, 3),
    (R, X, 1, 1, 0, 2), (S, X, 1, 1, 1, 4), (R, X, 1, 1, 0, 5), (FINISH, 1, 0), (R, X, 1, 0, 1, 2),
    (R, X, 1, 0, 1, 5), (FINISH, 0, 1), (R, X, 1, 1, 1, 2), (R, X, 1, 1, 1, 5), (R, X, 1, 1, 1, 3),
    (R, X, 1, 1, 1, 4), (FINISH, 1, 1),
)


def way_of(key):
    if key[0] == W:
        return MESSAGES[key[1]][key[2]][3]
    if key[0] == G:
        return GATHER[key[2]][3]
    if key[0] == C:
        return "d"
    return ("x+", "x-", "x+", "x+", "x-", "x-")[key[4]]


def share():
    sent, waited = {}, {}
    for i, (name, *which) in enumerate(SCHEDULE):
        if name == S:
            sent[tuple(which)] = i
        elif name == R:
            waited[tuple(which)] = i
        elif name == PRODUCT:
            g, cases, j = which
            for dx, h in cases:
                sent[(C, g, TURN[dx], h, j)] = i
    back = {"x+": "x-", "x-": "x+", "y+": "y-", "y-": "y+", "z+": "z-", "z-": "z+", "d": "d"}
    last, place = [], {}
    for key in sorted(sent, key=lambda k: (sent[k], k)):
        toward = [k for k in sent if way_of(k) == back[way_of(key)] and waited[k] < sent[key]]
        heard = max([sent[k] for k in toward], default=-1)
        free = [(at, n) for n, at in enumerate(last) if at < heard]
        if free:
            n = max(free)[1]
            last[n] = waited[key]
        else:
            n = len(last)
            last.append(waited[key])
        place[key] = n
    return place, len(last)


SEMAPHORE, SEMAPHORES = share()


def kernel(
    resid, mix_gain_in, wq, wk, wv, wg, wo, rate_in, mlp_gain_in, wu, wd,
    out,
    w_in, w_out, w_up, w_down, xn, rbuf, after, proj, gated, hid, decay, begun, kept, mix_gain, mlp_gain, rate,
    dout, din, sout, rin2, rin1,
    local_sem, w_send, g_send, d_send, s_send, recv,
):
    fs, tp = lax.axis_index("fs"), lax.axis_index("tp")
    z, y, x, c = fs // RING, fs % RING, tp // 2, tp % 2

    def turn(v, d):
        return (v + d + RING) % RING

    device = {
        "y+": (z * RING + turn(y, 1), tp),
        "y-": (z * RING + turn(y, -1), tp),
        "z+": (turn(z, 1) * RING + y, tp),
        "z-": (turn(z, -1) * RING + y, tp),
        "x+": (fs, turn(x, 1) * 2 + c),
        "x-": (fs, turn(x, -1) * 2 + c),
        "d": (fs, x * 2 + 1 - c),
    }

    def remote(src, dst, send, recv, way):
        return pltpu.make_async_remote_copy(
            src_ref=src, dst_ref=dst, send_sem=send, recv_sem=recv,
            device_id=device[way], device_id_type=MESH,
        )

    def send(*args):
        remote(*args).start()

    weights = (w_in, w_out, w_up, w_down)

    def block(dy, dz):
        return turn(z, dz) * RING + turn(y, dy)

    def piece(t, dy, dz, part):
        ref = weights[t]
        f = block(dy, dz)
        if part == "full":
            return ref.at[f]
        if part in ("A", "B"):
            return ref.at[f, :, "AB".index(part)]
        if part in ("h0", "h1"):
            return ref.at[f, int(part[1])]
        return ref.at[f, int(part[2]), "AB".index(part[0])]

    def w_copy(t, n, place):
        dy, dz, part, way = place
        ref = piece(t, dy, dz, part)
        return (ref, ref, w_send.at[t], recv.at[SEMAPHORE[W, t, n]], way)

    def g_copy(g, n, dx, core):
        h, q, way = GATHER[n][1:]
        block = turn(x, dx) * 2 + core
        ref = xn.at[g, block, h] if q is None else xn.at[g, block, h, q]
        return (ref, ref, g_send.at[g], recv.at[SEMAPHORE[G, g, n]], way)

    def rows16(count, body):
        def step(i, carry):
            body(pl.ds(pl.multiple_of(i * 16, 16), 16))
            return carry

        lax.fori_loop(0, count // 16, step, 0)

    def of(ref, j):
        return ref.at[:, pl.ds(j * 1024, 1024)]

    def d_copy(g, k, h, j):
        columns = pl.ds(j * 1024, 1024)
        return (
            dout.at[g, k, h, :, :, columns], din.at[g, k, h, :, :, columns],
            d_send.at[g], recv.at[SEMAPHORE[C, g, k, h, j]], "d",
        )

    def s_copy(g, h, j, n):
        if n < 2:
            src, dst, way = sout.at[g, 0, h, n], rin2.at[g, h, n], ("x+", "x-")[n]
        elif n < 4:
            src, dst, way = sout.at[g, 1, h, n - 2], rin1.at[g, 0, h, n - 2], "x+"
        else:
            src, dst, way = sout.at[g, 2, h, n - 4], rin1.at[g, 1, h, n - 4], "x-"
        return (of(src, j), of(dst, j), s_send.at[g], recv.at[SEMAPHORE[X, g, h, j, n]], way)

    def start(kind, *which):
        if kind == W:
            t, n = which
            send(*w_copy(t, n, MESSAGES[t][n]))
        elif kind == G:
            g, n = which
            send(*g_copy(g, n, GATHER[n][0], c))
        else:
            send(*s_copy(*which))

    def receive(kind, *which):
        if kind == W:
            t, n = which
            copy = w_copy(t, n, arrived(MESSAGES[t][n]))
        elif kind == G:
            g, n = which
            dx, way = GATHER[n][0], GATHER[n][3]
            if way == "d":
                copy = g_copy(g, n, dx, 1 - c)
            else:
                copy = g_copy(g, n, near(dx - (1 if way == "x+" else -1)), c)
        elif kind == C:
            copy = d_copy(*which)
        else:
            copy = s_copy(*which)
        remote(*copy).wait_recv()

    def partial(g, cases, j):
        weight, lhs = ((w_out, gated_rows), (w_down, hidden_rows))[g]
        depth = weight.shape[1] * weight.shape[2] * weight.shape[3]
        for i in (2 * j, 2 * j + 1):
            w = [weight[block(*PLACES[4 * i + n])].reshape(depth, 128) for n in range(4)]
            rows = [some for case in cases for some in lhs(*case)]
            o = jnp.dot(
                jnp.concatenate(rows, axis=0), jnp.concatenate(w, axis=1), preferred_element_type=F32
            )
            columns = slice(i * 512, (i + 1) * 512)
            for n, (dx, h) in enumerate(cases):
                mine = o[n * 128 : (n + 1) * 128]
                dout[g, TURN[dx], h, :, :, columns] = mine[:64].astype(BF16).reshape(2, 32, 512)
                kept[TURN[dx], h, :, :, columns] = mine[64:].reshape(2, 32, 512)
        for dx, h in cases:
            send(*d_copy(g, TURN[dx], h, j))

    def add_quarter(g, k, h, j, q, extra=False):
        columns = slice(j * 1024, (j + 1) * 1024)

        def body(rows):
            total = kept[k, h, q, rows, columns] + din[g, k, h, q, rows, columns].astype(F32)
            if extra:
                total = total + rin2[g, h, q, rows, columns].astype(F32)
            sout[g, k, h, q, rows, columns] = total.astype(BF16)

        rows16(32, body)

    def add_far(g, h, j):
        for q in (0, 1):
            add_quarter(g, 0, h, j, q)

    def add_free(g, h, j, k):
        add_quarter(g, k, h, j, 1 if k == 1 else 0)

    def add_near(g, h, j, k):
        add_quarter(g, k, h, j, 0 if k == 1 else 1, True)

    def add_own(g, h, i, source, target):
        here = pl.ds(pl.multiple_of(block(*PLACES[i]) * 128, 128), 128)
        at = slice(i * 128, (i + 1) * 128)
        total = source[h, :, :, here].astype(F32) + kept[3, h, :, :, at]
        total = total + din[g, 3, h, :, :, at].astype(F32)
        total = total + rin1[g, 0, h, :, :, at].astype(F32) + rin1[g, 1, h, :, :, at].astype(F32)
        target[h, :, :, here] = total.astype(BF16)

    def normed(values, gain):
        scale = lax.rsqrt(jnp.mean(values * values, axis=-1, keepdims=True) + EPS)
        return (values * scale * gain).astype(BF16)

    barrier = pltpu.get_barrier_semaphore()
    for way in device:
        pl.semaphore_signal(barrier, inc=1, device_id=device[way], device_id_type=MESH)
    loads = []

    def load(src, dst):
        copy = pltpu.make_async_copy(src, dst, local_sem.at[len(loads)])
        copy.start()
        return copy

    for src, low, wide in ((wq, 0, 128), (wk, 128, 128), (wv, 256, 256), (wg, 512, 256)):
        load(src, w_in.at[fs, :, :, :, low : low + wide])
    loads.append(pltpu.make_async_copy(w_in.at[fs], w_in.at[fs], local_sem.at[0]))
    loads.append(load(resid, rbuf))
    loads.append(load(mix_gain_in, mix_gain))
    loads.append(load(mlp_gain_in, mlp_gain))
    loads.append(load(rate_in, rate))
    for src, dst in ((wo, w_out.at[fs]), (wu, w_up.at[fs]), (wd, w_down.at[fs])):
        loads.append(load(src, dst))
    for copy in loads[:5]:
        copy.wait()
    for h in (0, 1):
        for q in (0, 1):
            def first_norm(rows):
                xn[0, tp, h, q, rows, :] = normed(rbuf[h, q, rows, :].astype(F32), mix_gain[...])

            rows16(32, first_norm)
    pl.semaphore_wait(barrier, 7)
    r = rate[0]

    def make_decay():
        def some_rows(i, carry):
            rows = pl.ds(pl.multiple_of(i * 64, 64), 64)
            t = lax.broadcasted_iota(jnp.int32, (64, LENGTH), 0) + i * 64
            s = lax.broadcasted_iota(jnp.int32, (64, LENGTH), 1)
            gap = (t - s).astype(F32)
            value = jnp.exp(-r * jnp.maximum(gap, 0.0)) * DK ** (-0.5)
            decay[rows, :] = jnp.where(gap >= 0.0, value, 0.0)
            return carry

        lax.fori_loop(0, LENGTH // 64, some_rows, 0)

    own = x // 2
    sequence = (own, 1 - own)

    chips = ((2 * own, 2), (2 * (1 - own) + 1 - x % 2, 1), (turn(x, 2), 1))

    def project(which, part):
        blocks = [block(*place) for place in (PLACES[:12], PLACES[12:])[part]]
        first, count = chips[which] if part == 0 else (2 * sequence[which], 2)

        def body(j, carry):
            columns = pl.ds(pl.multiple_of(j * 256, 256), 256)
            lhs = [
                xn[0, pl.ds(2 * first, 2 * count), :, :, :, pl.ds(pl.multiple_of(f * 128, 128), 128)]
                .reshape(256 * count, 128)
                for f in blocks
            ]
            rhs = [w_in[f, :, :, :, columns].reshape(128, 256) for f in blocks]
            o = jnp.dot(
                jnp.concatenate(lhs, axis=1), jnp.concatenate(rhs, axis=0), preferred_element_type=F32
            ).reshape(count, 256, 256)
            if part == 0:
                begun[j, pl.ds(first, count)] = o
            else:
                o = (begun[j, pl.ds(first, count)] + o).astype(BF16)
                proj[pl.ds(2 * first, 2 * count), :, columns] = o.reshape(2 * count, 128, 256)
            return carry

        lax.fori_loop(0, 3, body, 0)

    def retain(seq):
        for i in (0, 1):
            mine = pl.ds(seq * 4 + 2 * i, 2)
            upto = pl.ds(seq * 4, 2 * i + 2)
            wide = 256 * (i + 1)
            q = proj[mine, :, 0:128].reshape(256, DK)
            k = proj[upto, :, 128:256].reshape(wide, DK)
            v = proj[upto, :, 256:512].reshape(wide, DV)
            scores = lax.dot_general(q, k, (((1,), (1,)), ((), ())), preferred_element_type=F32)
            scores = (scores * decay[i * 256 : (i + 1) * 256, 0:wide]).astype(BF16)
            mixed = jnp.dot(scores, v, preferred_element_type=F32)
            mixed = mixed - jnp.mean(mixed, axis=-1, keepdims=True)
            spread = jnp.mean(mixed * mixed, axis=-1, keepdims=True)
            gate = proj[mine, :, 512:768].reshape(256, DV).astype(F32)
            value = gate / (1.0 + jnp.exp(-gate)) * (mixed * lax.rsqrt(spread + EPS))
            gated[mine] = value.astype(BF16).reshape(2, 2, 64, DV)

    def gated_rows(dx, h):
        first = turn(x, dx) * 2
        return gated[first + 1 - c, h], gated[first + c, h]

    def lift(cases, part):
        def body(j, carry):
            columns = pl.ds(pl.multiple_of(j * 256, 256), 256)
            lhs = jnp.concatenate(
                [
                    xn[1, turn(x, dx) * 2 + core, h].reshape(64, D)
                    for dx, h in cases
                    for core in (1 - c, c)
                ],
                axis=0,
            )
            rhs = w_up[:, :, :, :, columns].reshape(D, 256)
            o = jnp.maximum(jnp.dot(lhs, rhs, preferred_element_type=F32), 0.0)
            o = (o * o).astype(BF16)
            for n, (dx, h) in enumerate(cases):
                hid[TURN[dx], h, :, columns] = o[n * 128 : (n + 1) * 128]
            return carry

        count = w_up.shape[4] // 512
        lax.fori_loop(part * count, (part + 1) * count, body, 0)

    def hidden_rows(dx, h):
        return (hid[TURN[dx], h],)

    def second_norm(h):
        for i in range(16):
            add_own(0, h, i, rbuf, after)
        for q in (0, 1):
            def body(rows):
                xn[1, tp, h, q, rows, :] = normed(after[h, q, rows, :].astype(F32), mlp_gain[...])

            rows16(32, body)

    def finish(h, j):
        for i in range(8 * j, 8 * j + 8):
            add_own(1, h, i, after, out)

    actions = {
        S: start,
        R: receive,
        DECAY: make_decay,
        PROJECT: project,
        RETAIN: lambda which: retain(sequence[which]),
        PRODUCT: partial,
        FAR: add_far,
        FREE: add_free,
        NEAR: add_near,
        NORM: second_norm,
        LIFT: lift,
        FINISH: finish,
    }
    for copy in loads[5:]:
        copy.wait()
    for name, *which in SCHEDULE:
        actions[name](*which)
    for t in range(4):
        ref = weights[t].at[0:15]
        remote(ref, ref, w_send.at[t], recv.at[0], "d").wait_send()
    for g in (0, 1):
        remote(xn.at[g, 0:7], xn.at[g, 0:7], g_send.at[g], recv.at[0], "d").wait_send()
        remote(dout.at[g], din.at[g], d_send.at[g], recv.at[0], "d").wait_send()
        remote(sout.at[g], sout.at[g], s_send.at[g], recv.at[0], "d").wait_send()


def on_device(
    resid, mix_gain, w_query, w_key, w_value, w_gate, w_output, decay_rate, mlp_gain, w_up, w_down
):
    def cut(w):
        return w.reshape(2, 2, w.shape[0] // 4, w.shape[1])

    wide = w_query.shape[1] + w_key.shape[1] + w_value.shape[1] + w_gate.shape[1]
    count = RING * RING

    def held(rows, columns):
        return pltpu.VMEM((count, 2, 2, rows // 4, columns), BF16)

    dma = pltpu.SemaphoreType.DMA
    vmem = pl.BlockSpec(memory_space=pltpu.VMEM)
    hbm = pl.BlockSpec(memory_space=pltpu.HBM)
    tokens = (2, 2, 32, D)
    result = pl.pallas_call(
        kernel,
        out_shape=pltpu.VMEM(tokens, BF16),
        in_specs=[
            hbm, hbm, hbm, hbm, hbm, hbm, hbm,
            hbm, hbm, hbm, hbm,
        ],
        out_specs=vmem,
        scratch_shapes=[
            held(128, wide),
            held(w_output.shape[0], 128),
            held(128, w_up.shape[1]),
            held(w_down.shape[0], 128),
            pltpu.VMEM((2, 8) + tokens, BF16),
            pltpu.VMEM(tokens, BF16),
            pltpu.VMEM(tokens, BF16),
            pltpu.VMEM((8, 128, wide), BF16),
            pltpu.VMEM((8, 2, 64, DV), BF16),
            pltpu.VMEM((4, 2, 128, w_up.shape[1]), BF16),
            pltpu.VMEM((LENGTH, LENGTH), F32),
            pltpu.VMEM((wide // 256, 4, 256, 256), F32),
            pltpu.VMEM((4,) + tokens, F32),
            pltpu.VMEM((1, D), F32),
            pltpu.VMEM((1, D), F32),
            pltpu.SMEM((1,), F32),
            pltpu.VMEM((2, 4) + tokens, BF16),
            pltpu.VMEM((2, 4) + tokens, BF16),
            pltpu.VMEM((2, 3) + tokens, BF16),
            pltpu.VMEM((2,) + tokens, BF16),
            pltpu.VMEM((2, 2) + tokens, BF16),
            dma((8,)),
            dma((4,)),
            dma((2,)),
            dma((2,)),
            dma((2,)),
            dma((SEMAPHORES,)),
        ],
        compiler_params=pltpu.CompilerParams(
            collective_id=0, has_side_effects=True, vmem_limit_bytes=66060288
        ),
    )(
        resid.reshape(tokens), mix_gain[None], cut(w_query), cut(w_key), cut(w_value), cut(w_gate),
        cut(w_output), decay_rate, mlp_gain[None], cut(w_up), cut(w_down),
    )
    return result.reshape(resid.shape)


def solution(mesh):
    placed = (
        P(("fs", "tp"), None),
        P(),
        P("fs", "tp"),
        P("fs", "tp"),
        P("fs", "tp"),
        P("fs", "tp"),
        P("tp", "fs"),
        P("tp"),
        P(),
        P("fs", "tp"),
        P("tp", "fs"),
    )
    return jax.shard_map(
        on_device, mesh=mesh, in_specs=placed, out_specs=P(("fs", "tp"), None), check_vma=False
    )
```
